128 devices in a mesh: sp: 16 (over z, x), tp: 8 (over y, core).
Axes of the slice: x: 4, y: 4, z: 4, core: 2. Of those that a mesh axis runs over, the one named last changes fastest.
Arguments:
- queries: bfloat16 [8192, 2048], P('sp', 'tp'), may hold values from -4.5 to 4.5
- keys: bfloat16 [8192, 2048], P('sp', 'tp'), may hold values from -4.5 to 4.5
- values: bfloat16 [8192, 2048], P('sp', 'tp'), may hold values from -6 to 6
- forget_logits: float32 [8192, 16], P('sp', 'tp'), may hold values from -1 to 20
- layer_input: bfloat16 [8192, 4096], P('sp', 'tp'), may hold values from -0.09375 to 0.09375
- out_grad: bfloat16 [8192, 2048], P('sp', 'tp'), may hold values from -6 to 6
Outputs:
- query_grad: float32 [8192, 2048], P('sp', 'tp')
- key_grad: float32 [8192, 2048], P('sp', 'tp')
- value_grad: float32 [8192, 2048], P('sp', 'tp')
- weight_grad: float32 [4096, 2048], P('sp', 'tp')
The draws below stay inside these ranges and needn't reach their ends.
All inputs are finite; a program needn't handle non-finite values.
Results may differ from the reference program's by a relative error of at most 0.04.
Values may be sent and summed in bfloat16 or wider, within the bound.
No kernel may reach another device: no remote copies, remote signals or barrier semaphores. Data moves between devices by JAX's collectives and lax.ppermute only.
A program may use at most 64 MiB of HBM per device.

```python
import math
import jax
import jax.numpy as jnp
from jax import lax

DMODEL = 4096
HEADS = 16
HEAD = 128
TOK_DEV = 512
TOKENS = 8192


def drawn_pair(key):
    full_shape = (TOKENS, HEADS * HEAD)
    query_rows = jnp.clip(jax.random.normal(jax.random.fold_in(key, 101), full_shape, jnp.float32), -4.5, 4.5)
    key_rows = jnp.clip(jax.random.normal(jax.random.fold_in(key, 102), full_shape, jnp.float32), -4.5, 4.5)
    return (query_rows, key_rows)


def draw_queries(key, part):
    return drawn_pair(key)[0].astype(jnp.bfloat16)


def draw_keys(key, part):
    return drawn_pair(key)[1].astype(jnp.bfloat16)


def draw_forget_logits(key, part):
    ranks = jax.random.permutation(jax.random.fold_in(key, 201), HEADS)
    quick = ranks < HEADS // 2
    levels = jax.random.uniform(jax.random.fold_in(key, 202), (HEADS,), jnp.float32, -0.5, 0.5)
    base_level = jnp.where(quick, math.log(80.0), math.log(TOKENS) + 1.0) + levels
    span_rows = max(TOK_DEV // 2, 1)
    shifts = jax.random.uniform(jax.random.fold_in(key, 203), (TOKENS // span_rows + 1, 1), jnp.float32, -0.9, 0.9)
    span_shift = jnp.repeat(shifts, span_rows, axis=0)[:TOKENS]
    noise = jnp.clip(jax.random.normal(jax.random.fold_in(key, 204), (TOKENS, HEADS), jnp.float32), -3.0, 3.0)
    return base_level[None, :] + span_shift + noise


def raised(values, own_key, source, target, parts, factor):
    def block_of(position):
        return (jnp.arange(values.shape[position]) // (values.shape[position] // parts)).reshape((-1,) + (1,) * (values.ndim - 1 - position))

    one_side = jax.random.permutation(own_key, parts)[block_of(target)]
    other_side = (block_of(target) + parts // 2) % parts
    return jnp.where((block_of(source) == one_side) | (block_of(source) == other_side), factor * values, values)


def level_of(key, shape, cuts, smallest, top_value):
    factor_of = 1.0
    for axis_at, shards_of in cuts:
        heights = jax.random.uniform(jax.random.fold_in(jax.random.fold_in(key, 6), axis_at), (shards_of,), jnp.float32, smallest / len(cuts), top_value / len(cuts))
        factor_of = factor_of * jnp.repeat(jnp.exp(heights), shape[axis_at] // shards_of).reshape((-1,) + (1,) * (len(shape) - 1 - axis_at))
    return factor_of


def gaussian(own_key, extent, spread, bound, cuts=(), kind=jnp.bfloat16):
    drawn = spread * jax.random.normal(own_key, extent, jnp.float32)
    if cuts:
        drawn = drawn * level_of(own_key, extent, cuts, -0.22, 0.18)
    return jnp.clip(drawn, -bound, bound).astype(kind)


def heavy_noise(key, extent, width, reach, pieces, heavy, kind=jnp.bfloat16):
    entries = width * jax.random.normal(key, extent, jnp.float32)
    if pieces:
        entries = entries * level_of(key, extent, pieces, -0.22, 0.18)
    return jnp.clip(raised(entries, jax.random.fold_in(key, 3), *heavy), -reach, reach).astype(kind)


def setup_inputs(seed: int = 0) -> dict:
    key_list = jax.random.split(jax.random.key(seed), 7)
    return {
        "queries": draw_queries(jax.random.fold_in(key_list[6], 71), 0),
        "keys": draw_keys(jax.random.fold_in(key_list[6], 71), 0),
        "values": gaussian(key_list[2], (TOKENS, HEADS * HEAD), 1.0, 6.0, ((0, 16), (1, 8))),
        "forget_logits": draw_forget_logits(jax.random.fold_in(key_list[6], 71), 0),
        "layer_input": heavy_noise(key_list[4], (TOKENS, DMODEL), TOKENS ** -0.5, 0.09375, ((0, 16), (1, 8)), (0, 1, 16, 2.0)),
        "out_grad": heavy_noise(key_list[5], (TOKENS, HEADS * HEAD), 1.0, 6.0, ((0, 16), (1, 8)), (0, 1, 16, 2.0)),
    }


def query_block(row_count):
    block_size = row_count
    while block_size > 512 and block_size % 2 == 0:
        block_size //= 2
    return block_size


def reference(queries, keys, values, forget_logits, layer_input, out_grad):
    row_count = queries.shape[0]
    head_total = queries.shape[1] // HEAD
    score_scale = HEAD ** -0.5
    gate_sums = jnp.cumsum(jax.nn.log_sigmoid(forget_logits), axis=0)
    positions = jnp.arange(row_count, dtype=jnp.int32)
    block_size = query_block(row_count)
    block_count = row_count // block_size

    def by_head(array):
        return array.reshape(row_count, head_total, HEAD).transpose(1, 0, 2)

    def one_head(inputs):
        head_query, head_key, head_value, head_grad, head_gates = inputs

        def one_block(carry, number):
            key_total, value_total = carry
            begin_at = number * block_size
            query_rows = lax.dynamic_slice_in_dim(head_query, begin_at, block_size, 0)
            grad_rows = lax.dynamic_slice_in_dim(head_grad, begin_at, block_size, 0)
            gate_rows = lax.dynamic_slice_in_dim(head_gates, begin_at, block_size, 0)
            scores = jnp.dot(query_rows, head_key.T, preferred_element_type=jnp.float32) * score_scale
            scores = scores + gate_rows[:, None] - head_gates[None, :]
            query_pos = begin_at + jnp.arange(block_size, dtype=jnp.int32)
            visible = positions[None, :] <= query_pos[:, None]
            row_max = jnp.max(jnp.where(visible, scores, -1.0e30), axis=1)
            weights = jnp.where(visible, jnp.exp(scores - row_max[:, None]), 0.0)
            weight_sum = jnp.sum(weights, axis=1)
            mixed = jnp.dot(weights.astype(jnp.bfloat16), head_value, preferred_element_type=jnp.float32)
            attended = (mixed / weight_sum[:, None]).astype(jnp.bfloat16)
            log_sums = row_max + jnp.log(weight_sum)
            row_terms = jnp.sum(attended.astype(jnp.float32) * grad_rows.astype(jnp.float32), axis=1)
            probs = jnp.where(visible, jnp.exp(scores - log_sums[:, None]), 0.0)
            prob_grads = jnp.dot(grad_rows, head_value.T, preferred_element_type=jnp.float32)
            score_grads = (probs * (prob_grads - row_terms[:, None])).astype(jnp.bfloat16)
            query_part = score_scale * jnp.dot(score_grads, head_key, preferred_element_type=jnp.float32)
            key_total = key_total + score_scale * jnp.dot(score_grads.T, query_rows, preferred_element_type=jnp.float32)
            value_total = value_total + jnp.dot(probs.astype(jnp.bfloat16).T, grad_rows, preferred_element_type=jnp.float32)
            return (key_total, value_total), query_part

        zeros_head = jnp.zeros((row_count, HEAD), jnp.float32)
        (key_total, value_total), query_parts = lax.scan(one_block, (zeros_head, zeros_head), jnp.arange(block_count, dtype=jnp.int32))
        return query_parts.reshape(row_count, HEAD), key_total, value_total

    query_heads, key_heads, value_heads = lax.map(one_head, (by_head(queries), by_head(keys), by_head(values), by_head(out_grad), gate_sums.T))

    def back_rows(array):
        return array.transpose(1, 0, 2).reshape(row_count, head_total * HEAD)

    query_grad = back_rows(query_heads)
    weight_grad = jnp.dot(layer_input.T, query_grad.astype(jnp.bfloat16), preferred_element_type=jnp.float32)
    return query_grad, back_rows(key_heads), back_rows(value_heads), weight_grad
```

```python
import functools
import math

import jax
import jax.numpy as jnp
from jax import lax
from jax.experimental import pallas as pl
from jax.experimental.pallas import tpu as pltpu
from jax.sharding import PartitionSpec as P

HEAD = 128
SIDE = 4
SCALE = HEAD ** (-0.5)
LOG2E = math.log2(math.e)
NEG_BIG = -1e30
SUB = 256


def along_z(r):
    return [(4 * z + x, 4 * ((z + r) % SIDE) + x) for z in range(SIDE) for x in range(SIDE)]


def along_x(r):
    return [(4 * z + x, 4 * z + (x + r) % SIDE) for z in range(SIDE) for x in range(SIDE)]


def fetched(array, axis_perm):
    return [array] + [lax.ppermute(array, "sp", axis_perm(-r)) for r in range(1, SIDE)]


def dot_nt(a, b):
    return lax.dot_general(a, b, (((1,), (1,)), ((), ())), preferred_element_type=jnp.float32)


def dot_nn(a, b):
    return lax.dot_general(a, b, (((1,), (0,)), ((), ())), preferred_element_type=jnp.float32)


def start_loads(z_refs, x_refs, qd, kv, sems):
    copies = []
    for r in range(SIDE):
        for ref, dst, half in (
            (z_refs[r], qd.at[0, r], 0),
            (x_refs[r], kv.at[0, r], 0),
            (x_refs[r], qd.at[1, r], 1),
            (z_refs[r], kv.at[1, r], 1),
        ):
            cols = pl.ds(half * 2 * HEAD, 2 * HEAD)
            copies.append(pltpu.make_async_copy(ref.at[:, cols], dst, sems.at[len(copies)]))
    for c in copies:
        c.start()
    return copies


def fill_bias(pos_ref, bias_ref, bcol, h):
    def one(r, _):
        rows = bias_ref[h, pos_ref[h, 1, r]]
        for j in range(4):
            tile = jnp.broadcast_to(rows[j : j + 1, :], (HEAD, HEAD))
            bcol[r, j * HEAD : (j + 1) * HEAD, :] = tile.T
        return 0

    lax.fori_loop(0, SIDE, one, 0)


def visible_mask(shape, first_query):
    key_at = lax.broadcasted_iota(jnp.int32, shape, 0)
    query_at = lax.broadcasted_iota(jnp.int32, shape, 1) + first_query
    return key_at <= query_at


def wide(tile, width):
    return jnp.concatenate([tile] * (width // tile.shape[1]), axis=1)


def stats_kernel(pos_ref, bias_ref, *rest):
    z_refs, x_refs = rest[:4], rest[4:8]
    outs = rest[8:10]
    qd, kv, bcol, stats, sems = rest[10:]
    span = qd.shape[2]
    copies = start_loads(z_refs, x_refs, qd, kv, sems)
    stats[...] = jnp.zeros_like(stats)
    stats[:, :, 0:1, :] = jnp.full((2, SIDE, 1, span), NEG_BIG, jnp.float32)
    for c in copies:
        c.wait()

    def block(h, qi, ki, diagonal):
        for s in range(span // SUB):
            cols = slice(s * SUB, (s + 1) * SUB)
            q = qd[h, qi, cols, :HEAD]
            do = qd[h, qi, cols, HEAD:]
            k = kv[h, ki, :, :HEAD]
            v = kv[h, ki, :, HEAD:]
            x = dot_nt(k, q) * (SCALE * LOG2E) - wide(bcol[ki], SUB)
            if diagonal:
                x = jnp.where(visible_mask(x.shape, s * SUB), x, NEG_BIG)
            dp = dot_nt(v, do)
            old = stats[h, qi, 0:1, cols]
            new = jnp.maximum(old, jnp.max(x, axis=0, keepdims=True))
            p = jnp.exp2(x - new)
            shrink = jnp.exp2(old - new)
            stats[h, qi, 0:1, cols] = new
            stats[h, qi, 1:2, cols] = stats[h, qi, 1:2, cols] * shrink + jnp.sum(
                p, axis=0, keepdims=True
            )
            stats[h, qi, 2:3, cols] = stats[h, qi, 2:3, cols] * shrink + jnp.sum(
                p * dp, axis=0, keepdims=True
            )

    def one_head(h, _):
        fill_bias(pos_ref, bias_ref, bcol, h)

        def one_pair(n, _):
            qi, ki = n // SIDE, n % SIDE
            q_span, k_span = pos_ref[h, 0, qi], pos_ref[h, 1, ki]

            @pl.when(k_span < q_span)
            def _():
                block(h, qi, ki, False)

            @pl.when(k_span == q_span)
            def _():
                block(h, qi, ki, True)

            return 0

        lax.fori_loop(0, SIDE * SIDE, one_pair, 0)
        return 0

    lax.fori_loop(0, 2, one_head, 0)
    outs[0][...] = stats[0]
    outs[1][...] = stats[1]


def grads_kernel(pos_ref, bias_ref, *rest):
    z_refs, x_refs = rest[:4], rest[4:8]
    stat_refs = (rest[8:12], rest[12:16])
    own_z, own_x = rest[16:18]
    send_z, send_x = rest[18:21], rest[21:24]
    qd, kv, bcol, rows, kt, dqt, dkv, sems = rest[24:]
    span = qd.shape[2]
    copies = start_loads(z_refs, x_refs, qd, kv, sems)
    dqt[...] = jnp.zeros_like(dqt)
    dkv[...] = jnp.zeros_like(dkv)
    for h in range(2):
        for r in range(SIDE):
            parts = [stat_refs[h][s][(r - s) % SIDE] for s in range(SIDE)]
            top = functools.reduce(jnp.maximum, [p[0:1, :] for p in parts])
            factors = [jnp.exp2(p[0:1, :] - top) for p in parts]
            total = sum(p[1:2, :] * f for p, f in zip(parts, factors))
            mixed = sum(p[2:3, :] * f for p, f in zip(parts, factors))
            rows[h, r, 0:1, :] = top + jnp.log2(total)
            rows[h, r, 1:2, :] = mixed / total
    for c in copies:
        c.wait()

    def block(h, qi, ki, diagonal):
        for s in range(span // SUB):
            cols = slice(s * SUB, (s + 1) * SUB)
            q = qd[h, qi, cols, :HEAD]
            do = qd[h, qi, cols, HEAD:]
            k = kv[h, ki, :, :HEAD]
            v = kv[h, ki, :, HEAD:]
            x = dot_nt(k, q) * (SCALE * LOG2E) - wide(bcol[ki], SUB) - rows[h, qi, 0:1, cols]
            if diagonal:
                x = jnp.where(visible_mask(x.shape, s * SUB), x, NEG_BIG)
            p = jnp.exp2(x)
            ds = (p * (dot_nt(v, do) - rows[h, qi, 1:2, cols])).astype(jnp.bfloat16)
            dkv[h, ki, :, HEAD:] += dot_nn(p.astype(jnp.bfloat16), do)
            dkv[h, ki, :, :HEAD] += dot_nn(ds, q)
            dqt[h, qi, :, cols] += dot_nn(kt[ki], ds)

    def one_head(h, _):
        fill_bias(pos_ref, bias_ref, bcol, h)

        def turn(r, _):
            kt[r] = kv[h, r, :, :HEAD].astype(jnp.float32).T.astype(jnp.bfloat16)
            return 0

        lax.fori_loop(0, SIDE, turn, 0)

        def one_pair(n, _):
            ki, qi = n // SIDE, n % SIDE
            q_span, k_span = pos_ref[h, 0, qi], pos_ref[h, 1, ki]

            @pl.when(k_span < q_span)
            def _():
                block(h, qi, ki, False)

            @pl.when(k_span == q_span)
            def _():
                block(h, qi, ki, True)

            return 0

        lax.fori_loop(0, SIDE * SIDE, one_pair, 0)
        return 0

    lax.fori_loop(0, 2, one_head, 0)
    for r in range(SIDE):
        for own, send, hq, hk in ((own_z, send_z, 0, 1), (own_x, send_x, 1, 0)):
            out = own if r == 0 else send[r - 1]
            out[:, :HEAD] = (dqt[hq, r].T * SCALE).astype(out.dtype)
            out[:, HEAD : 2 * HEAD] = (dkv[hk, r, :, :HEAD] * SCALE).astype(out.dtype)
            out[:, 2 * HEAD :] = dkv[hk, r, :, HEAD:].astype(out.dtype)


def weight_kernel(at_ref, dq_ref, x0, x1, x2, x3, other, out_ref, inputs, sems):
    copies = []
    for r, ref in enumerate((x0, x1, x2, x3)):
        copies.append(pltpu.make_async_copy(ref, inputs.at[at_ref[0, r]], sems.at[r]))
        copies.append(pltpu.make_async_copy(other.at[r], inputs.at[at_ref[1, r]], sems.at[4 + r]))
    for c in copies:
        c.start()
    turned = dq_ref[...].T.astype(jnp.bfloat16)
    for c in copies:
        c.wait()

    def one(n, _):
        both = dot_nn(turned, inputs[n]).astype(jnp.bfloat16)
        half = both.shape[1] // 2
        out_ref[2 * n] = both[:, :half]
        out_ref[2 * n + 1] = both[:, half:]
        return 0

    lax.fori_loop(0, 8, one, 0)


ANY = pl.BlockSpec(memory_space=pl.ANY)
VM = pl.BlockSpec(memory_space=pltpu.VMEM)
SM = pl.BlockSpec(memory_space=pltpu.SMEM)


def stats_call(pos, bias, z_parts, x_parts):
    span = z_parts[0].shape[0]
    pairs = 17 * span * span
    return pl.pallas_call(
        stats_kernel,
        out_shape=[jax.ShapeDtypeStruct((SIDE, 8, span), jnp.float32)] * 2,
        in_specs=[SM, VM] + [ANY] * 8,
        out_specs=[VM] * 2,
        scratch_shapes=[
            pltpu.VMEM((2, SIDE, span, 2 * HEAD), jnp.bfloat16),
            pltpu.VMEM((2, SIDE, span, 2 * HEAD), jnp.bfloat16),
            pltpu.VMEM((SIDE, span, HEAD), jnp.float32),
            pltpu.VMEM((2, SIDE, 8, span), jnp.float32),
            pltpu.SemaphoreType.DMA((16,)),
        ],
        compiler_params=pltpu.CompilerParams(vmem_limit_bytes=40 << 20),
        cost_estimate=pl.CostEstimate(
            flops=4 * HEAD * pairs, bytes_accessed=4 << 20, transcendentals=pairs
        ),
        name="stats",
    )(pos, bias, *z_parts, *x_parts)


def grads_call(pos, bias, z_parts, x_parts, z_stats, x_stats):
    span = z_parts[0].shape[0]
    pairs = 17 * span * span
    own = jax.ShapeDtypeStruct((span, 3 * HEAD), jnp.float32)
    send = jax.ShapeDtypeStruct((span, 3 * HEAD), jnp.bfloat16)
    return pl.pallas_call(
        grads_kernel,
        out_shape=[own] * 2 + [send] * 6,
        in_specs=[SM, VM] + [ANY] * 8 + [VM] * 8,
        out_specs=[VM] * 8,
        scratch_shapes=[
            pltpu.VMEM((2, SIDE, span, 2 * HEAD), jnp.bfloat16),
            pltpu.VMEM((2, SIDE, span, 2 * HEAD), jnp.bfloat16),
            pltpu.VMEM((SIDE, span, HEAD), jnp.float32),
            pltpu.VMEM((2, SIDE, 8, span), jnp.float32),
            pltpu.VMEM((SIDE, HEAD, span), jnp.bfloat16),
            pltpu.VMEM((2, SIDE, HEAD, span), jnp.float32),
            pltpu.VMEM((2, SIDE, span, 2 * HEAD), jnp.float32),
            pltpu.SemaphoreType.DMA((16,)),
        ],
        compiler_params=pltpu.CompilerParams(vmem_limit_bytes=48 << 20),
        cost_estimate=pl.CostEstimate(
            flops=10 * HEAD * pairs, bytes_accessed=8 << 20, transcendentals=pairs
        ),
        name="grads",
    )(pos, bias, *z_parts, *x_parts, *z_stats, *x_stats)


def weight_call(at, query_grad, own_parts, other):
    rows, width = own_parts[0].shape
    cols = query_grad.shape[1]
    return pl.pallas_call(
        weight_kernel,
        out_shape=jax.ShapeDtypeStruct((16, cols, width // 2), jnp.bfloat16),
        in_specs=[SM, VM] + [ANY] * 5,
        out_specs=VM,
        scratch_shapes=[
            pltpu.VMEM((8, rows, width), jnp.bfloat16),
            pltpu.SemaphoreType.DMA((8,)),
        ],
        compiler_params=pltpu.CompilerParams(vmem_limit_bytes=32 << 20),
        cost_estimate=pl.CostEstimate(
            flops=16 * rows * width * cols, bytes_accessed=6 << 20, transcendentals=0
        ),
        name="weight",
    )(at, query_grad, *own_parts, other)


def head_of(array, h):
    return array[:, h * HEAD : (h + 1) * HEAD]


def local(queries, keys, values, forget_logits, layer_input, out_grad):
    span = queries.shape[0]
    here = lax.axis_index("sp")
    z, x = here // SIDE, here % SIDE
    part = lax.axis_index("tp")
    y, core = part // 2, part % 2
    steps = jnp.arange(SIDE, dtype=jnp.int32)
    z_spans = 4 * ((z + steps) % SIDE) + x
    x_spans = 4 * z + (x + steps) % SIDE
    pos = jnp.stack([jnp.stack([z_spans, x_spans]), jnp.stack([x_spans, z_spans])]).astype(
        jnp.int32
    )

    for_z = jnp.concatenate(
        [head_of(queries, 0), head_of(out_grad, 0), head_of(keys, 1), head_of(values, 1)], axis=1
    )
    for_x = jnp.concatenate(
        [head_of(keys, 0), head_of(values, 0), head_of(queries, 1), head_of(out_grad, 1)], axis=1
    )
    z_parts = fetched(for_z, along_z)
    x_parts = fetched(for_x, along_x)

    gates = jnp.cumsum(jax.nn.log_sigmoid(forget_logits).T, axis=1).reshape(1, 2, span // HEAD, HEAD)
    gates = lax.all_to_all(
        jnp.broadcast_to(gates, (16,) + gates.shape[1:]), "sp", 0, 0, tiled=True
    )
    totals = gates[:, :, -1, -1]
    before = jnp.cumsum(totals, axis=0) - totals
    bias = ((gates + before[:, :, None, None]) * LOG2E).transpose(1, 0, 2, 3)

    own_inputs = [layer_input] + [
        lax.ppermute(layer_input, "tp", [(p, (p - 2 * r) % 8) for p in range(8)])
        for r in range(1, SIDE)
    ]
    other_inputs = lax.ppermute(jnp.stack(own_inputs), "tp", [(p, p ^ 1) for p in range(8)])
    at = 2 * ((y + steps) % SIDE)
    at = jnp.stack([at + core, at + 1 - core]).astype(jnp.int32)

    stats_z, stats_x = stats_call(pos, bias, z_parts, x_parts)
    z_stats = fetched(stats_z, along_z)
    x_stats = fetched(stats_x, along_x)
    own_z, own_x, *sends = grads_call(pos, bias, z_parts, x_parts, z_stats, x_stats)

    def summed(own, sent, axis_perm):
        for r in range(1, SIDE):
            own = own + lax.ppermute(sent[r - 1], "sp", axis_perm(r)).astype(jnp.float32)
        return own

    sum_z = summed(own_z, sends[:3], along_z)
    sum_x = summed(own_x, sends[3:], along_x)
    query_grad = jnp.concatenate([head_of(sum_z, 0), head_of(sum_x, 0)], axis=1)
    key_grad = jnp.concatenate([head_of(sum_x, 1), head_of(sum_z, 1)], axis=1)
    value_grad = jnp.concatenate([head_of(sum_x, 2), head_of(sum_z, 2)], axis=1)

    terms = weight_call(at, query_grad, own_inputs, other_inputs)
    arrived = lax.all_to_all(terms, "sp", 0, 0, tiled=True)
    weight_grad = arrived.astype(jnp.float32).sum(axis=0).T
    return (query_grad, key_grad, value_grad, weight_grad)


def solution(mesh):
    placed = P("sp", "tp")
    return jax.shard_map(
        local,
        mesh=mesh,
        in_specs=(placed,) * 6,
        out_specs=(placed,) * 4,
        check_vma=False,
    )
```

```python
import functools
import math

import jax
import jax.numpy as jnp
from jax import lax
from jax.experimental import pallas as pl
from jax.experimental.pallas import tpu as pltpu
from jax.sharding import PartitionSpec as P


HEAD = 128
SIDE = 4
SCALE = HEAD ** (-0.5)
LOG2E = math.log2(math.e)
NEG_BIG = -1e30
SUB = 256


def along_z(r):
    return [(4 * z + x, 4 * ((z + r) % SIDE) + x) for z in range(SIDE) for x in range(SIDE)]


def along_x(r):
    return [(4 * z + x, 4 * z + (x + r) % SIDE) for z in range(SIDE) for x in range(SIDE)]


def fetched(array, axis_perm):
    return [array] + [lax.ppermute(array, "sp", axis_perm(-r)) for r in range(1, SIDE)]


def dot_nt(a, b):
    return lax.dot_general(a, b, (((1,), (1,)), ((), ())), preferred_element_type=jnp.float32)


def dot_nn(a, b):
    return lax.dot_general(a, b, (((1,), (0,)), ((), ())), preferred_element_type=jnp.float32)


def start_loads(z_refs, x_refs, slots, qd, kv, sems):
    copies = []
    for r, z_ref, x_ref in zip(slots, z_refs, x_refs):
        for ref, dst, half in (
            (z_ref, qd.at[0, r], 0),
            (x_ref, kv.at[0, r], 0),
            (x_ref, qd.at[1, r], 1),
            (z_ref, kv.at[1, r], 1),
        ):
            cols = pl.ds(half * 2 * HEAD, 2 * HEAD)
            copies.append(pltpu.make_async_copy(ref.at[:, cols], dst, sems.at[len(copies)]))
    for c in copies:
        c.start()
    return copies


def gates_kernel(logits_ref, out_ref):
    sums = jax.nn.log_sigmoid(logits_ref[...])
    rows, width = sums.shape
    lane = lax.broadcasted_iota(jnp.int32, sums.shape, 1)
    step = 1
    while step < width:
        sums = sums + jnp.where(lane >= step, pltpu.roll(sums, step, axis=1), 0.0)
        step *= 2
    shape = (rows, rows)
    mine, other = (lax.broadcasted_iota(jnp.int32, shape, d) for d in (0, 1))
    earlier = jnp.where((other < mine) & (other % 2 == mine % 2), 1.0, 0.0)
    totals = jnp.broadcast_to(sums[:, width - 1 :], (rows, HEAD))
    before = jnp.dot(
        earlier, totals, preferred_element_type=jnp.float32, precision=lax.Precision.HIGHEST
    )
    out_ref[...] = (sums + wide(before, width)) * LOG2E


def fill_bias(pos_ref, bias_ref, bcol, h):
    def one(r, _):
        row = bias_ref[pl.ds(2 * pos_ref[h, 1, r] + h, 1), :]
        for j in range(4):
            tile = jnp.broadcast_to(row[:, j * HEAD : (j + 1) * HEAD], (HEAD, HEAD))
            bcol[r, j * HEAD : (j + 1) * HEAD, :] = tile.T
        return 0

    lax.fori_loop(0, SIDE, one, 0)


def visible_mask(shape, first_query):
    key_at = lax.broadcasted_iota(jnp.int32, shape, 0)
    query_at = lax.broadcasted_iota(jnp.int32, shape, 1) + first_query
    return key_at <= query_at


def wide(tile, width):
    return jnp.concatenate([tile] * (width // tile.shape[1]), axis=1)


NEAR = (0, 1, 3)


def near_slot(n):
    return n + n // 2


def near_pairs(n):
    return near_slot(n // 3), near_slot(n % 3)


def far_pairs(n):
    near = near_slot(jnp.maximum(n - SIDE, 0))
    return jnp.where(n < SIDE, 2, near), jnp.where(n < SIDE, n, 2)


def stats_kernel(slots, pair_count, pair_of, pos_ref, bias_ref, *rest):
    n_slots = len(slots)
    z_refs, x_refs = rest[:n_slots], rest[n_slots : 2 * n_slots]
    rest = rest[2 * n_slots :]
    known, rest = rest[:-7], rest[-7:]
    outs = rest[:2]
    qd, kv, bcol, stats, sems = rest[2:]
    span = qd.shape[2]
    copies = start_loads(z_refs, x_refs, slots, qd, kv, sems)
    if known:
        stats[0] = known[0][...]
        stats[1] = known[1][...]
    else:
        stats[...] = jnp.zeros_like(stats)
        stats[:, :, 0:1, :] = jnp.full((2, SIDE, 1, span), NEG_BIG, jnp.float32)
    for c in copies:
        c.wait()

    def block(h, qi, ki, diagonal):
        for s in range(span // SUB):
            cols = slice(s * SUB, (s + 1) * SUB)
            q = qd[h, qi, cols, :HEAD]
            do = qd[h, qi, cols, HEAD:]
            k = kv[h, ki, :, :HEAD]
            v = kv[h, ki, :, HEAD:]
            x = dot_nt(k, q) * (SCALE * LOG2E) - wide(bcol[ki], SUB)
            if diagonal:
                x = jnp.where(visible_mask(x.shape, s * SUB), x, NEG_BIG)
            dp = dot_nt(v, do)
            old = stats[h, qi, 0:1, cols]
            new = jnp.maximum(old, jnp.max(x, axis=0, keepdims=True))
            p = jnp.exp2(x - new)
            shrink = jnp.exp2(old - new)
            stats[h, qi, 0:1, cols] = new
            stats[h, qi, 1:2, cols] = stats[h, qi, 1:2, cols] * shrink + jnp.sum(
                p, axis=0, keepdims=True
            )
            stats[h, qi, 2:3, cols] = stats[h, qi, 2:3, cols] * shrink + jnp.sum(
                p * dp, axis=0, keepdims=True
            )

    def one_head(h, _):
        fill_bias(pos_ref, bias_ref, bcol, h)

        def one_pair(n, _):
            qi, ki = pair_of(n)
            q_span, k_span = pos_ref[h, 0, qi], pos_ref[h, 1, ki]

            @pl.when(k_span < q_span)
            def _():
                block(h, qi, ki, False)

            @pl.when(k_span == q_span)
            def _():
                block(h, qi, ki, True)

            return 0

        lax.fori_loop(0, pair_count, one_pair, 0)
        return 0

    lax.fori_loop(0, 2, one_head, 0)
    outs[0][...] = stats[0]
    outs[1][...] = stats[1]


def grads_kernel(pos_ref, bias_ref, *rest):
    z_refs, x_refs = rest[:4], rest[4:8]
    stat_refs = (rest[8:12], rest[12:16])
    outs = rest[16:32]
    qd, kv, bcol, rows, kt, dqt, dkv, sems = rest[32:]
    span = qd.shape[2]
    copies = start_loads(z_refs, x_refs, range(SIDE), qd, kv, sems)
    dqt[...] = jnp.zeros_like(dqt)
    dkv[...] = jnp.zeros_like(dkv)
    for h in range(2):
        for r in range(SIDE):
            parts = [stat_refs[h][s][(r - s) % SIDE] for s in range(SIDE)]
            top = functools.reduce(jnp.maximum, [p[0:1, :] for p in parts])
            factors = [jnp.exp2(p[0:1, :] - top) for p in parts]
            total = sum(p[1:2, :] * f for p, f in zip(parts, factors))
            mixed = sum(p[2:3, :] * f for p, f in zip(parts, factors))
            rows[h, r, 0:1, :] = top + jnp.log2(total)
            rows[h, r, 1:2, :] = mixed / total
    for c in copies:
        c.wait()

    def block(h, qi, ki, diagonal):
        for s in range(span // SUB):
            cols = slice(s * SUB, (s + 1) * SUB)
            q = qd[h, qi, cols, :HEAD]
            do = qd[h, qi, cols, HEAD:]
            k = kv[h, ki, :, :HEAD]
            v = kv[h, ki, :, HEAD:]
            x = dot_nt(k, q) * (SCALE * LOG2E) - wide(bcol[ki], SUB) - rows[h, qi, 0:1, cols]
            if diagonal:
                x = jnp.where(visible_mask(x.shape, s * SUB), x, NEG_BIG)
            p = jnp.exp2(x)
            ds = (p * (dot_nt(v, do) - rows[h, qi, 1:2, cols])).astype(jnp.bfloat16)
            dkv[h, ki, :, HEAD:] += dot_nn(p.astype(jnp.bfloat16), do)
            dkv[h, ki, :, :HEAD] += dot_nn(ds, q)
            dqt[h, qi, :, cols] += dot_nn(kt[ki], ds)

    def one_head(h, _):
        fill_bias(pos_ref, bias_ref, bcol, h)

        def turn(r, _):
            kt[r] = kv[h, r, :, :HEAD].astype(jnp.float32).T.astype(jnp.bfloat16)
            return 0

        lax.fori_loop(0, SIDE, turn, 0)

        def one_pair(n, _):
            ki, qi = n // SIDE, n % SIDE
            q_span, k_span = pos_ref[h, 0, qi], pos_ref[h, 1, ki]

            @pl.when(k_span < q_span)
            def _():
                block(h, qi, ki, False)

            @pl.when(k_span == q_span)
            def _():
                block(h, qi, ki, True)

            return 0

        lax.fori_loop(0, SIDE * SIDE, one_pair, 0)
        return 0

    lax.fori_loop(0, 2, one_head, 0)
    for h in range(2):
        for r in range(SIDE):
            dq_out, dkv_out = outs[SIDE * h + r], outs[8 + SIDE * h + r]
            dq_out[...] = (dqt[h, r] * SCALE).astype(dq_out.dtype)
            dkv_out[:, :HEAD] = (dkv[h, r, :, :HEAD] * SCALE).astype(dkv_out.dtype)
            dkv_out[:, HEAD:] = dkv[h, r, :, HEAD:].astype(dkv_out.dtype)


def weight_kernel(at_ref, *rest):
    dq_refs, in_refs, outs = rest[:4], rest[4:12], rest[12:16]
    dqs, inputs, sems = rest[16:]
    copies = []
    for r in range(SIDE):
        for other in range(2):
            copies.append(
                pltpu.make_async_copy(
                    in_refs[SIDE * other + r],
                    inputs.at[at_ref[3, other], at_ref[0, r]],
                    sems.at[2 * r + other],
                )
            )
        copies.append(pltpu.make_async_copy(dq_refs[r], dqs.at[at_ref[1, r]], sems.at[8 + r]))
    for c in copies:
        c.start()
    for c in copies:
        c.wait()
    width = outs[0].shape[1]
    for r in (1, 2, 3, 0):
        block = at_ref[2, r]
        cols = pl.ds(pl.multiple_of((block % 2) * width, width), width)
        total = sum(dot_nn(dqs[a], inputs[block // 2, a, :, cols]) for a in range(SIDE))
        outs[r][...] = total.astype(outs[r].dtype)


ANY = pl.BlockSpec(memory_space=pl.ANY)
VM = pl.BlockSpec(memory_space=pltpu.VMEM)
SM = pl.BlockSpec(memory_space=pltpu.SMEM)


def stats_call(pos, bias, z_parts, x_parts, known=None):
    span = z_parts[0].shape[0]
    if known is None:
        slots, pair_count, pair_of, known = NEAR, 9, near_pairs, ()
        z_parts, x_parts = ([parts[r] for r in NEAR] for parts in (z_parts, x_parts))
    else:
        slots, pair_count, pair_of = range(SIDE), 7, far_pairs
    pairs = pair_count * span * span
    return pl.pallas_call(
        functools.partial(stats_kernel, slots, pair_count, pair_of),
        out_shape=[jax.ShapeDtypeStruct((SIDE, 8, span), jnp.float32)] * 2,
        in_specs=[SM, VM] + [ANY] * (2 * len(slots)) + [VM] * len(known),
        out_specs=[VM] * 2,
        scratch_shapes=[
            pltpu.VMEM((2, SIDE, span, 2 * HEAD), jnp.bfloat16),
            pltpu.VMEM((2, SIDE, span, 2 * HEAD), jnp.bfloat16),
            pltpu.VMEM((SIDE, span, HEAD), jnp.float32),
            pltpu.VMEM((2, SIDE, 8, span), jnp.float32),
            pltpu.SemaphoreType.DMA((16,)),
        ],
        compiler_params=pltpu.CompilerParams(vmem_limit_bytes=20 << 20),
        cost_estimate=pl.CostEstimate(
            flops=4 * HEAD * pairs, bytes_accessed=4 << 20, transcendentals=pairs
        ),
        name="stats",
    )(pos, bias, *z_parts, *x_parts, *known)


def grads_call(pos, bias, z_parts, x_parts, z_stats, x_stats):
    span = z_parts[0].shape[0]
    pairs = 17 * span * span

    def shapes(*shape):
        own = jax.ShapeDtypeStruct(shape, jnp.float32)
        send = jax.ShapeDtypeStruct(shape, jnp.bfloat16)
        return ([own] + [send] * 3) * 2

    outs = pl.pallas_call(
        grads_kernel,
        out_shape=shapes(HEAD, span) + shapes(span, 2 * HEAD),
        in_specs=[SM, VM] + [ANY] * 8 + [VM] * 8,
        out_specs=[VM] * 16,
        scratch_shapes=[
            pltpu.VMEM((2, SIDE, span, 2 * HEAD), jnp.bfloat16),
            pltpu.VMEM((2, SIDE, span, 2 * HEAD), jnp.bfloat16),
            pltpu.VMEM((SIDE, span, HEAD), jnp.float32),
            pltpu.VMEM((2, SIDE, 8, span), jnp.float32),
            pltpu.VMEM((SIDE, HEAD, span), jnp.bfloat16),
            pltpu.VMEM((2, SIDE, HEAD, span), jnp.float32),
            pltpu.VMEM((2, SIDE, span, 2 * HEAD), jnp.float32),
            pltpu.SemaphoreType.DMA((16,)),
        ],
        compiler_params=pltpu.CompilerParams(vmem_limit_bytes=32 << 20),
        cost_estimate=pl.CostEstimate(
            flops=10 * HEAD * pairs, bytes_accessed=8 << 20, transcendentals=pairs
        ),
        name="grads",
    )(pos, bias, *z_parts, *x_parts, *z_stats, *x_stats)
    return outs[:4], outs[4:8], outs[8:12], outs[12:]


def weight_call(at, query_grads, inputs):
    cols, rows = query_grads[0].shape
    width = inputs[0].shape[1]
    own = jax.ShapeDtypeStruct((cols, width // 2), jnp.float32)
    send = jax.ShapeDtypeStruct((cols, width // 2), jnp.bfloat16)
    return pl.pallas_call(
        weight_kernel,
        out_shape=[own] + [send] * 3,
        in_specs=[SM] + [ANY] * 12,
        out_specs=[VM] * 4,
        scratch_shapes=[
            pltpu.VMEM((SIDE, cols, rows), jnp.bfloat16),
            pltpu.VMEM((2, SIDE, rows, width), jnp.bfloat16),
            pltpu.SemaphoreType.DMA((12,)),
        ],
        compiler_params=pltpu.CompilerParams(vmem_limit_bytes=32 << 20),
        cost_estimate=pl.CostEstimate(
            flops=16 * rows * width * cols, bytes_accessed=6 << 20, transcendentals=0
        ),
        name="weight",
    )(at, *query_grads, *inputs)


def head_of(array, h):
    return array[:, h * HEAD : (h + 1) * HEAD]


def local(queries, keys, values, forget_logits, layer_input, out_grad):
    here = lax.axis_index("sp")
    z, x = here // SIDE, here % SIDE
    part = lax.axis_index("tp")
    y, core = part // 2, part % 2
    steps = jnp.arange(SIDE, dtype=jnp.int32)
    z_spans = 4 * ((z + steps) % SIDE) + x
    x_spans = 4 * z + (x + steps) % SIDE
    pos = jnp.stack([jnp.stack([z_spans, x_spans]), jnp.stack([x_spans, z_spans])]).astype(
        jnp.int32
    )
    cores = jnp.stack([core, 1 - core, core, 1 - core])
    at = jnp.stack([(y + steps) % SIDE, (z + steps) % SIDE, (x + steps) % SIDE, cores]).astype(
        jnp.int32
    )

    gates = lax.all_to_all(jnp.tile(forget_logits.T, (16, 1)), "sp", 0, 0, tiled=True)

    for_z = jnp.concatenate(
        [head_of(queries, 0), head_of(out_grad, 0), head_of(keys, 1), head_of(values, 1)], axis=1
    )
    for_x = jnp.concatenate(
        [head_of(keys, 0), head_of(values, 0), head_of(queries, 1), head_of(out_grad, 1)], axis=1
    )
    z_parts = fetched(for_z, along_z)
    x_parts = fetched(for_x, along_x)

    bias = pl.pallas_call(
        gates_kernel,
        out_shape=jax.ShapeDtypeStruct(gates.shape, jnp.float32),
        in_specs=[VM],
        out_specs=VM,
        cost_estimate=pl.CostEstimate(flops=10**6, bytes_accessed=1 << 17, transcendentals=0),
        name="gate_sums",
    )(gates)

    swap = [
        (((a * SIDE + b) * SIDE + c) * 2 + d, ((c * SIDE + b) * SIDE + a) * 2 + d)
        for a in range(SIDE)
        for b in range(SIDE)
        for c in range(SIDE)
        for d in range(2)
    ]
    moved = lax.ppermute(layer_input, ("sp", "tp"), swap)
    inputs = [moved]
    for r in range(1, SIDE):
        inputs.append(lax.ppermute(moved, "tp", [(p, (p - 2 * r) % 8) for p in range(8)]))
    for part in list(inputs):
        inputs.append(lax.ppermute(part, "tp", [(p, p ^ 1) for p in range(8)]))

    known = stats_call(pos, bias, z_parts, x_parts)
    stats_z, stats_x = stats_call(pos, bias, z_parts, x_parts, known)
    z_stats = fetched(stats_z, along_z)
    x_stats = fetched(stats_x, along_x)
    dq_0, dq_1, dkv_0, dkv_1 = grads_call(pos, bias, z_parts, x_parts, z_stats, x_stats)

    def summed(parts, axis_perm):
        total = parts[0]
        for r in range(1, SIDE):
            total = total + lax.ppermute(parts[r], "sp", axis_perm(r)).astype(jnp.float32)
        return total

    query_t = jnp.concatenate([summed(dq_0, along_z), summed(dq_1, along_x)], axis=0)
    low, dkv_0, dkv_1 = lax.optimization_barrier((query_t.astype(jnp.bfloat16), dkv_0, dkv_1))
    low_parts = fetched(low, along_z)
    terms = weight_call(at, low_parts, inputs)
    weight_grad = summed(terms, along_x).T
    sum_0, sum_1 = summed(dkv_0, along_x), summed(dkv_1, along_z)
    query_grad = query_t.T
    key_grad = jnp.concatenate([head_of(sum_0, 0), head_of(sum_1, 0)], axis=1)
    value_grad = jnp.concatenate([head_of(sum_0, 1), head_of(sum_1, 1)], axis=1)
    return (query_grad, key_grad, value_grad, weight_grad)


def solution(mesh):
    placed = P("sp", "tp")

    return jax.shard_map(
        local,
        mesh=mesh,
        in_specs=(placed,) * 6,
        out_specs=(placed,) * 4,
        check_vma=False,
    )
```

```python
import functools
import math

import jax
import jax.numpy as jnp
from jax import lax
from jax.experimental import pallas as pl
from jax.experimental.pallas import tpu as pltpu
from jax.sharding import PartitionSpec as P


HEAD = 128
SIDE = 4
SCALE = HEAD ** (-0.5)
LOG2E = math.log2(math.e)
NEG_BIG = -1e30
SUB = 256


def along_z(r):
    return [(4 * z + x, 4 * ((z + r) % SIDE) + x) for z in range(SIDE) for x in range(SIDE)]


def along_x(r):
    return [(4 * z + x, 4 * z + (x + r) % SIDE) for z in range(SIDE) for x in range(SIDE)]


def fetched(array, axis_perm):
    parts = [array]
    for r in range(1, SIDE):
        parts.append(lax.ppermute(array, "sp", axis_perm(-r)))
    return parts


def dot_nt(a, b):
    return lax.dot_general(a, b, (((1,), (1,)), ((), ())), preferred_element_type=jnp.float32)


def dot_nn(a, b):
    return lax.dot_general(a, b, (((1,), (0,)), ((), ())), preferred_element_type=jnp.float32)


def start_loads(z_refs, x_refs, slots, qd, kv, sems):
    copies = []
    for r, z_ref, x_ref in zip(slots, z_refs, x_refs):
        for ref, dst, half in (
            (z_ref, qd.at[0, r], 0),
            (x_ref, kv.at[0, r], 0),
            (x_ref, qd.at[1, r], 1),
            (z_ref, kv.at[1, r], 1),
        ):
            cols = pl.ds(half * 2 * HEAD, 2 * HEAD)
            copies.append(pltpu.make_async_copy(ref.at[:, cols], dst, sems.at[len(copies)]))
    for c in copies:
        c.start()
    return copies


def gates_kernel(logits_ref, out_ref):
    sums = jax.nn.log_sigmoid(logits_ref[...])
    rows, width = sums.shape
    lane = lax.broadcasted_iota(jnp.int32, sums.shape, 1)
    step = 1
    while step < width:
        sums = sums + jnp.where(lane >= step, pltpu.roll(sums, step, axis=1), 0.0)
        step *= 2
    shape = (rows, rows)
    mine, other = (lax.broadcasted_iota(jnp.int32, shape, d) for d in (0, 1))
    earlier = jnp.where((other < mine) & (other % 2 == mine % 2), 1.0, 0.0)
    totals = jnp.broadcast_to(sums[:, width - 1 :], (rows, HEAD))
    before = jnp.dot(
        earlier, totals, preferred_element_type=jnp.float32, precision=lax.Precision.HIGHEST
    )
    out_ref[...] = (sums + wide(before, width)) * LOG2E


def fill_bias(pos_ref, bias_ref, bcol, h):
    def one(r, _):
        row = bias_ref[pl.ds(2 * pos_ref[h, 1, r] + h, 1), :]
        for j in range(4):
            tile = jnp.broadcast_to(row[:, j * HEAD : (j + 1) * HEAD], (HEAD, HEAD))
            bcol[r, j * HEAD : (j + 1) * HEAD, :] = tile.T
        return 0

    lax.fori_loop(0, SIDE, one, 0)


def visible_mask(shape, first_query):
    key_at = lax.broadcasted_iota(jnp.int32, shape, 0)
    query_at = lax.broadcasted_iota(jnp.int32, shape, 1) + first_query
    return key_at <= query_at


def wide(tile, width):
    return jnp.concatenate([tile] * (width // tile.shape[1]), axis=1)


NEAR = (0, 1, 3)


def near_slot(n):
    return n + n // 2


def near_pairs(n):
    return near_slot(n // 3), near_slot(n % 3)


def far_pairs(n):
    near = near_slot(jnp.maximum(n - SIDE, 0))
    return jnp.where(n < SIDE, 2, near), jnp.where(n < SIDE, n, 2)


def stats_kernel(slots, pair_count, pair_of, pos_ref, bias_ref, *rest):
    n_slots = len(slots)
    z_refs, x_refs = rest[:n_slots], rest[n_slots : 2 * n_slots]
    rest = rest[2 * n_slots :]
    known, rest = rest[:-7], rest[-7:]
    outs = rest[:2]
    qd, kv, bcol, stats, sems = rest[2:]
    span = qd.shape[2]
    copies = start_loads(z_refs, x_refs, slots, qd, kv, sems)
    if known:
        stats[0] = known[0][...]
        stats[1] = known[1][...]
    else:
        stats[...] = jnp.zeros_like(stats)
        stats[:, :, 0:1, :] = jnp.full((2, SIDE, 1, span), NEG_BIG, jnp.float32)
    for c in copies:
        c.wait()

    def block(h, qi, ki, diagonal):
        for s in range(span // SUB):
            cols = slice(s * SUB, (s + 1) * SUB)
            q = qd[h, qi, cols, :HEAD]
            do = qd[h, qi, cols, HEAD:]
            k = kv[h, ki, :, :HEAD]
            v = kv[h, ki, :, HEAD:]
            x = dot_nt(k, q) * (SCALE * LOG2E) - wide(bcol[ki], SUB)
            if diagonal:
                x = jnp.where(visible_mask(x.shape, s * SUB), x, NEG_BIG)
            dp = dot_nt(v, do)
            old = stats[h, qi, 0:1, cols]
            new = jnp.maximum(old, jnp.max(x, axis=0, keepdims=True))
            p = jnp.exp2(x - new)
            shrink = jnp.exp2(old - new)
            stats[h, qi, 0:1, cols] = new
            stats[h, qi, 1:2, cols] = stats[h, qi, 1:2, cols] * shrink + jnp.sum(
                p, axis=0, keepdims=True
            )
            stats[h, qi, 2:3, cols] = stats[h, qi, 2:3, cols] * shrink + jnp.sum(
                p * dp, axis=0, keepdims=True
            )

    def one_head(h, _):
        fill_bias(pos_ref, bias_ref, bcol, h)

        def one_pair(n, _):
            qi, ki = pair_of(n)
            q_span, k_span = pos_ref[h, 0, qi], pos_ref[h, 1, ki]

            @pl.when(k_span < q_span)
            def _():
                block(h, qi, ki, False)

            @pl.when(k_span == q_span)
            def _():
                block(h, qi, ki, True)

            return 0

        lax.fori_loop(0, pair_count, one_pair, 0)
        return 0

    lax.fori_loop(0, 2, one_head, 0)
    outs[0][...] = stats[0]
    outs[1][...] = stats[1]


def grads_kernel(pos_ref, bias_ref, *rest):
    z_refs, x_refs = rest[:4], rest[4:8]
    stat_refs = (rest[8:12], rest[12:16])
    outs = rest[16:32]
    qd, kv, bcol, rows, kt, dqt, dkv, sems = rest[32:]
    span = qd.shape[2]
    copies = start_loads(z_refs, x_refs, range(SIDE), qd, kv, sems)
    dqt[...] = jnp.zeros_like(dqt)
    dkv[...] = jnp.zeros_like(dkv)
    for h in range(2):
        for r in range(SIDE):
            parts = [stat_refs[h][s][(r - s) % SIDE] for s in range(SIDE)]
            top = functools.reduce(jnp.maximum, [p[0:1, :] for p in parts])
            factors = [jnp.exp2(p[0:1, :] - top) for p in parts]
            total = sum(p[1:2, :] * f for p, f in zip(parts, factors))
            mixed = sum(p[2:3, :] * f for p, f in zip(parts, factors))
            rows[h, r, 0:1, :] = top + jnp.log2(total)
            rows[h, r, 1:2, :] = mixed / total
    for c in copies:
        c.wait()

    def block(h, qi, ki, diagonal):
        for s in range(span // SUB):
            cols = slice(s * SUB, (s + 1) * SUB)
            q = qd[h, qi, cols, :HEAD]
            do = qd[h, qi, cols, HEAD:]
            k = kv[h, ki, :, :HEAD]
            v = kv[h, ki, :, HEAD:]
            x = dot_nt(k, q) * (SCALE * LOG2E) - wide(bcol[ki], SUB) - rows[h, qi, 0:1, cols]
            if diagonal:
                x = jnp.where(visible_mask(x.shape, s * SUB), x, NEG_BIG)
            p = jnp.exp2(x)
            ds = (p * (dot_nt(v, do) - rows[h, qi, 1:2, cols])).astype(jnp.bfloat16)
            dkv[h, ki, :, HEAD:] += dot_nn(p.astype(jnp.bfloat16), do)
            dkv[h, ki, :, :HEAD] += dot_nn(ds, q)
            dqt[h, qi, :, cols] += dot_nn(kt[ki], ds)

    def one_head(h, _):
        fill_bias(pos_ref, bias_ref, bcol, h)

        def turn(r, _):
            kt[r] = kv[h, r, :, :HEAD].astype(jnp.float32).T.astype(jnp.bfloat16)
            return 0

        lax.fori_loop(0, SIDE, turn, 0)

        def one_pair(n, _):
            ki, qi = n // SIDE, n % SIDE
            q_span, k_span = pos_ref[h, 0, qi], pos_ref[h, 1, ki]

            @pl.when(k_span < q_span)
            def _():
                block(h, qi, ki, False)

            @pl.when(k_span == q_span)
            def _():
                block(h, qi, ki, True)

            return 0

        lax.fori_loop(0, SIDE * SIDE, one_pair, 0)
        return 0

    lax.fori_loop(0, 2, one_head, 0)
    for h in range(2):
        for r in range(SIDE):
            dq_out, dkv_out = outs[SIDE * h + r], outs[8 + SIDE * h + r]
            dq_out[...] = (dqt[h, r] * SCALE).astype(dq_out.dtype)
            dkv_out[:, :HEAD] = (dkv[h, r, :, :HEAD] * SCALE).astype(dkv_out.dtype)
            dkv_out[:, HEAD:] = dkv[h, r, :, HEAD:].astype(dkv_out.dtype)


def weight_kernel(at_ref, *rest):
    dq_refs, in_refs, outs = rest[:4], rest[4:12], rest[12:16]
    dqs, inputs, sems = rest[16:]
    copies = []
    for r in range(SIDE):
        for other in range(2):
            copies.append(
                pltpu.make_async_copy(
                    in_refs[SIDE * other + r],
                    inputs.at[at_ref[3, other], at_ref[0, r]],
                    sems.at[2 * r + other],
                )
            )
        copies.append(pltpu.make_async_copy(dq_refs[r], dqs.at[at_ref[1, r]], sems.at[8 + r]))
    for c in copies:
        c.start()
    for c in copies:
        c.wait()
    width = outs[0].shape[1]
    for r in (1, 2, 3, 0):
        block = at_ref[2, r]
        cols = pl.ds(pl.multiple_of((block % 2) * width, width), width)
        total = sum(dot_nn(dqs[a], inputs[block // 2, a, :, cols]) for a in range(SIDE))
        outs[r][...] = total.astype(outs[r].dtype)


ANY = pl.BlockSpec(memory_space=pl.ANY)
VM = pl.BlockSpec(memory_space=pltpu.VMEM)
SM = pl.BlockSpec(memory_space=pltpu.SMEM)


def stats_call(pos, bias, z_parts, x_parts, known=None):
    span = z_parts[0].shape[0]
    if known is None:
        slots, pair_count, pair_of, known = NEAR, 9, near_pairs, ()
        z_parts, x_parts = ([parts[r] for r in NEAR] for parts in (z_parts, x_parts))
    else:
        slots, pair_count, pair_of = range(SIDE), 7, far_pairs
    pairs = pair_count * span * span
    return pl.pallas_call(
        functools.partial(stats_kernel, slots, pair_count, pair_of),
        out_shape=[jax.ShapeDtypeStruct((SIDE, 8, span), jnp.float32)] * 2,
        in_specs=[SM, VM] + [ANY] * (2 * len(slots)) + [VM] * len(known),
        out_specs=[VM] * 2,
        scratch_shapes=[
            pltpu.VMEM((2, SIDE, span, 2 * HEAD), jnp.bfloat16),
            pltpu.VMEM((2, SIDE, span, 2 * HEAD), jnp.bfloat16),
            pltpu.VMEM((SIDE, span, HEAD), jnp.float32),
            pltpu.VMEM((2, SIDE, 8, span), jnp.float32),
            pltpu.SemaphoreType.DMA((16,)),
        ],
        compiler_params=pltpu.CompilerParams(vmem_limit_bytes=62 << 20),
        cost_estimate=pl.CostEstimate(
            flops=4 * HEAD * pairs, bytes_accessed=4 << 20, transcendentals=pairs
        ),
        name="stats",
    )(pos, bias, *z_parts, *x_parts, *known)


def grads_call(pos, bias, z_parts, x_parts, z_stats, x_stats):
    span = z_parts[0].shape[0]
    pairs = 17 * span * span

    def shapes(*shape):
        own = jax.ShapeDtypeStruct(shape, jnp.float32)
        send = jax.ShapeDtypeStruct(shape, jnp.bfloat16)
        return ([own] + [send] * 3) * 2

    outs = pl.pallas_call(
        grads_kernel,
        out_shape=shapes(HEAD, span) + shapes(span, 2 * HEAD),
        in_specs=[SM, VM] + [ANY] * 8 + [VM] * 8,
        out_specs=[VM] * 16,
        scratch_shapes=[
            pltpu.VMEM((2, SIDE, span, 2 * HEAD), jnp.bfloat16),
            pltpu.VMEM((2, SIDE, span, 2 * HEAD), jnp.bfloat16),
            pltpu.VMEM((SIDE, span, HEAD), jnp.float32),
            pltpu.VMEM((2, SIDE, 8, span), jnp.float32),
            pltpu.VMEM((SIDE, HEAD, span), jnp.bfloat16),
            pltpu.VMEM((2, SIDE, HEAD, span), jnp.float32),
            pltpu.VMEM((2, SIDE, span, 2 * HEAD), jnp.float32),
            pltpu.SemaphoreType.DMA((16,)),
        ],
        compiler_params=pltpu.CompilerParams(vmem_limit_bytes=62 << 20),
        cost_estimate=pl.CostEstimate(
            flops=10 * HEAD * pairs, bytes_accessed=8 << 20, transcendentals=pairs
        ),
        name="grads",
    )(pos, bias, *z_parts, *x_parts, *z_stats, *x_stats)
    return outs[:4], outs[4:8], outs[8:12], outs[12:]


def weight_call(at, query_grads, inputs):
    cols, rows = query_grads[0].shape
    width = inputs[0].shape[1]
    own = jax.ShapeDtypeStruct((cols, width // 2), jnp.float32)
    send = jax.ShapeDtypeStruct((cols, width // 2), jnp.bfloat16)
    return pl.pallas_call(
        weight_kernel,
        out_shape=[own] + [send] * 3,
        in_specs=[SM] + [ANY] * 12,
        out_specs=[VM] * 4,
        scratch_shapes=[
            pltpu.VMEM((SIDE, cols, rows), jnp.bfloat16),
            pltpu.VMEM((2, SIDE, rows, width), jnp.bfloat16),
            pltpu.SemaphoreType.DMA((12,)),
        ],
        compiler_params=pltpu.CompilerParams(vmem_limit_bytes=62 << 20),
        cost_estimate=pl.CostEstimate(
            flops=16 * rows * width * cols, bytes_accessed=6 << 20, transcendentals=0
        ),
        name="weight",
    )(at, *query_grads, *inputs)


def head_of(array, h):
    return array[:, h * HEAD : (h + 1) * HEAD]


def local(queries, keys, values, forget_logits, layer_input, out_grad):
    here = lax.axis_index("sp")
    z, x = here // SIDE, here % SIDE
    part = lax.axis_index("tp")
    y, core = part // 2, part % 2
    steps = jnp.arange(SIDE, dtype=jnp.int32)
    z_spans = 4 * ((z + steps) % SIDE) + x
    x_spans = 4 * z + (x + steps) % SIDE
    pos = jnp.stack([jnp.stack([z_spans, x_spans]), jnp.stack([x_spans, z_spans])]).astype(
        jnp.int32
    )
    cores = jnp.stack([core, 1 - core, core, 1 - core])
    at = jnp.stack([(y - z + steps) % SIDE, (z + steps) % SIDE, (x + steps) % SIDE, cores]).astype(
        jnp.int32
    )

    gates = lax.all_to_all(jnp.tile(forget_logits.T, (16, 1)), "sp", 0, 0, tiled=True)

    for_z = jnp.concatenate(
        [head_of(queries, 0), head_of(out_grad, 0), head_of(keys, 1), head_of(values, 1)], axis=1
    )
    for_x = jnp.concatenate(
        [head_of(keys, 0), head_of(values, 0), head_of(queries, 1), head_of(out_grad, 1)], axis=1
    )
    z_parts = fetched(for_z, along_z)
    x_parts = fetched(for_x, along_x)

    bias = pl.pallas_call(
        gates_kernel,
        out_shape=jax.ShapeDtypeStruct(gates.shape, jnp.float32),
        in_specs=[VM],
        out_specs=VM,
        cost_estimate=pl.CostEstimate(flops=10**6, bytes_accessed=1 << 17, transcendentals=0),
        name="gate_sums",
    )(gates)

    def over_zy(target):
        pairs = []
        for n in range(SIDE**3 * 2):
            zxyc = (n // 32, n // 8 % SIDE, n // 2 % SIDE, n % 2)
            new_z, new_y = target(zxyc[0], zxyc[2])
            pairs.append((n, new_z % SIDE * 32 + zxyc[1] * 8 + new_y % SIDE * 2 + zxyc[3]))
        return pairs

    everywhere = ("sp", "tp")
    moved = lax.ppermute(layer_input, everywhere, over_zy(lambda a, b: (a, a + b)))
    moved = lax.ppermute(moved, everywhere, over_zy(lambda a, b: (b - a, b)))
    inputs = [moved]
    for r in range(1, SIDE):
        inputs.append(lax.ppermute(moved, "tp", [(p, (p - 2 * r) % 8) for p in range(8)]))
    for part in list(inputs):
        inputs.append(lax.ppermute(part, "tp", [(p, p ^ 1) for p in range(8)]))

    known = stats_call(pos, bias, z_parts, x_parts)
    stats_z, stats_x = stats_call(pos, bias, z_parts, x_parts, known)
    z_stats = fetched(stats_z, along_z)
    x_stats = fetched(stats_x, along_x)
    dq_0, dq_1, dkv_0, dkv_1 = grads_call(pos, bias, z_parts, x_parts, z_stats, x_stats)

    def summed(parts, axis_perm):
        total = parts[0]
        for r in range(1, SIDE):
            total = total + lax.ppermute(parts[r], "sp", axis_perm(r)).astype(jnp.float32)
        return total

    query_t = jnp.concatenate([summed(dq_0, along_z), summed(dq_1, along_x)], axis=0)
    low, dkv_0, dkv_1 = lax.optimization_barrier((query_t.astype(jnp.bfloat16), dkv_0, dkv_1))
    low_parts = fetched(low, along_z)
    terms = weight_call(at, low_parts, inputs)
    weight_grad = summed(terms, along_x).T
    sum_0, sum_1 = summed(dkv_0, along_x), summed(dkv_1, along_z)
    query_grad = query_t.T
    key_grad = jnp.concatenate([head_of(sum_0, 0), head_of(sum_1, 0)], axis=1)
    value_grad = jnp.concatenate([head_of(sum_0, 1), head_of(sum_1, 1)], axis=1)
    return (query_grad, key_grad, value_grad, weight_grad)


def solution(mesh):
    placed = P("sp", "tp")

    return jax.shard_map(
        local,
        mesh=mesh,
        in_specs=(placed,) * 6,
        out_specs=(placed,) * 4,
        check_vma=False,
    )
```

```python
import functools
import math

import jax
import jax.numpy as jnp
from jax import lax
from jax.experimental import pallas as pl
from jax.experimental.pallas import tpu as pltpu
from jax.sharding import PartitionSpec as P


HEAD = 128
SIDE = 4
SCALE = HEAD ** (-0.5)
LOG2E = math.log2(math.e)
NEG_BIG = -1e30
SUB = 256


def along_z(r):
    return [(4 * z + x, 4 * ((z + r) % SIDE) + x) for z in range(SIDE) for x in range(SIDE)]


def along_x(r):
    return [(4 * z + x, 4 * z + (x + r) % SIDE) for z in range(SIDE) for x in range(SIDE)]


def fetched(array, axis_perm):
    parts = [array]
    for r in range(1, SIDE):
        parts.append(lax.ppermute(array, "sp", axis_perm(-r)))
    return parts


def dot_nt(a, b):
    return lax.dot_general(a, b, (((1,), (1,)), ((), ())), preferred_element_type=jnp.float32)


def dot_nn(a, b):
    return lax.dot_general(a, b, (((1,), (0,)), ((), ())), preferred_element_type=jnp.float32)


def copy_list(sems):
    made = []

    def begin(src, dst):
        copy = pltpu.make_async_copy(src, dst, sems.at[len(made)])
        made.append(copy)
        copy.start()
        return copy

    return begin


def wait_all(copies):
    for c in copies:
        c.wait()


def start_loads(begin, h, z_refs, x_refs, slots, qd, kv):
    cols = pl.ds(h * 2 * HEAD, 2 * HEAD)
    q_refs, k_refs = (z_refs, x_refs) if h == 0 else (x_refs, z_refs)
    copies = []
    for r, q_ref, k_ref in zip(slots, q_refs, k_refs):
        copies.append(begin(q_ref.at[:, cols], qd.at[h, r]))
        copies.append(begin(k_ref.at[:, cols], kv.at[h, r]))
    return copies


def span_at(h, keys, r):
    here = lax.axis_index("sp")
    z, x = here // SIDE, here % SIDE
    if (h == 0) != keys:
        return SIDE * ((z + r) % SIDE) + x
    return SIDE * z + (x + r) % SIDE


def gates_kernel(logits_ref, out_ref):
    sums = jax.nn.log_sigmoid(logits_ref[...])
    rows, width = sums.shape
    lane = lax.broadcasted_iota(jnp.int32, sums.shape, 1)
    step = 1
    while step < width:
        sums = sums + jnp.where(lane >= step, pltpu.roll(sums, step, axis=1), 0.0)
        step *= 2
    shape = (rows, rows)
    mine, other = (lax.broadcasted_iota(jnp.int32, shape, d) for d in (0, 1))
    earlier = jnp.where((other < mine) & (other % 2 == mine % 2), 1.0, 0.0)
    totals = jnp.broadcast_to(sums[:, width - 1 :], (rows, HEAD))
    before = jnp.dot(
        earlier, totals, preferred_element_type=jnp.float32, precision=lax.Precision.HIGHEST
    )
    out_ref[...] = (sums + wide(before, width)) * LOG2E


def fill_bias(bias, bcol, h):
    def one(r, _):
        row = bias[pl.ds(2 * span_at(h, True, r) + h, 1), :]
        for j in range(4):
            tile = jnp.broadcast_to(row[:, j * HEAD : (j + 1) * HEAD], (HEAD, HEAD))
            bcol[r, j * HEAD : (j + 1) * HEAD, :] = tile.T
        return 0

    lax.fori_loop(0, SIDE, one, 0)


def for_visible(h, qi, ki, block):
    q_span, k_span = span_at(h, False, qi), span_at(h, True, ki)

    @pl.when(k_span < q_span)
    def _():
        block(h, qi, ki, False)

    @pl.when(k_span == q_span)
    def _():
        block(h, qi, ki, True)


def visible_mask(shape, first_query):
    key_at = lax.broadcasted_iota(jnp.int32, shape, 0)
    query_at = lax.broadcasted_iota(jnp.int32, shape, 1) + first_query
    return key_at <= query_at


def wide(tile, width):
    return jnp.concatenate([tile] * (width // tile.shape[1]), axis=1)


NEAR = (0, 1, 3)


def near_slot(n):
    return n + n // 2


def near_pairs(n):
    return near_slot(n // 3), near_slot(n % 3)


def far_pairs(n):
    near = near_slot(jnp.maximum(n - SIDE, 0))
    return jnp.where(n < SIDE, 2, near), jnp.where(n < SIDE, n, 2)


def stats_kernel(slots, pair_count, pair_of, bias_ref, *rest):
    n_slots = len(slots)
    z_refs, x_refs = rest[:n_slots], rest[n_slots : 2 * n_slots]
    rest = rest[2 * n_slots :]
    known, rest = rest[:-8], rest[-8:]
    outs = rest[:2]
    bias, qd, kv, bcol, stats, sems = rest[2:]
    span = qd.shape[2]
    begin = copy_list(sems)
    bias_copy = begin(bias_ref, bias)
    loads = []
    for h in range(2):
        loads.append(start_loads(begin, h, z_refs, x_refs, slots, qd, kv))
        if known:
            loads[h].append(begin(known[h], stats.at[h]))
        else:
            stats[h] = jnp.zeros((SIDE, 8, span), jnp.float32)
            stats[h, :, 0:1, :] = jnp.full((SIDE, 1, span), NEG_BIG, jnp.float32)

    def block(h, qi, ki, diagonal):
        for s in range(span // SUB):
            cols = slice(s * SUB, (s + 1) * SUB)
            q = qd[h, qi, cols, :HEAD]
            do = qd[h, qi, cols, HEAD:]
            k = kv[h, ki, :, :HEAD]
            v = kv[h, ki, :, HEAD:]
            x = dot_nt(k, q) * (SCALE * LOG2E) - wide(bcol[ki], SUB)
            if diagonal:
                x = jnp.where(visible_mask(x.shape, s * SUB), x, NEG_BIG)
            dp = dot_nt(v, do)
            old = stats[h, qi, 0:1, cols]
            new = jnp.maximum(old, jnp.max(x, axis=0, keepdims=True))
            p = jnp.exp2(x - new)
            shrink = jnp.exp2(old - new)
            stats[h, qi, 0:1, cols] = new
            stats[h, qi, 1:2, cols] = stats[h, qi, 1:2, cols] * shrink + jnp.sum(
                p, axis=0, keepdims=True
            )
            stats[h, qi, 2:3, cols] = stats[h, qi, 2:3, cols] * shrink + jnp.sum(
                p * dp, axis=0, keepdims=True
            )

    bias_copy.wait()
    stores = []
    for h in range(2):
        fill_bias(bias, bcol, h)
        wait_all(loads[h])

        def one_pair(n, _, h=h):
            qi, ki = pair_of(n)
            for_visible(h, qi, ki, block)
            return 0

        lax.fori_loop(0, pair_count, one_pair, 0)
        stores.append(begin(stats.at[h], outs[h]))
    wait_all(stores)


def grads_kernel(bias_ref, *rest):
    z_refs, x_refs = rest[:4], rest[4:8]
    stat_refs = (rest[8:12], rest[12:16])
    outs = rest[16:32]
    bias, qd, kv, bcol, parts, rows, kt, dqt, dkv, dq_send, dkv_send, sems = rest[32:]
    span = qd.shape[2]
    begin = copy_list(sems)
    bias_copy = begin(bias_ref, bias)
    loads = []
    for h in range(2):
        stat_copies = [begin(stat_refs[h][s], parts.at[h, s]) for s in range(SIDE)]
        loads.append(stat_copies + start_loads(begin, h, z_refs, x_refs, range(SIDE), qd, kv))

    def combine(h):
        for r in range(SIDE):
            found = [parts[h, s, (r - s) % SIDE] for s in range(SIDE)]
            top = functools.reduce(jnp.maximum, [p[0:1, :] for p in found])
            factors = [jnp.exp2(p[0:1, :] - top) for p in found]
            total = sum(p[1:2, :] * f for p, f in zip(found, factors))
            mixed = sum(p[2:3, :] * f for p, f in zip(found, factors))
            rows[h, r, 0:1, :] = top + jnp.log2(total)
            rows[h, r, 1:2, :] = mixed / total

    def block(h, qi, ki, diagonal):
        for s in range(span // SUB):
            cols = slice(s * SUB, (s + 1) * SUB)
            q = qd[h, qi, cols, :HEAD]
            do = qd[h, qi, cols, HEAD:]
            k = kv[h, ki, :, :HEAD]
            v = kv[h, ki, :, HEAD:]
            x = dot_nt(k, q) * (SCALE * LOG2E) - wide(bcol[ki], SUB) - rows[h, qi, 0:1, cols]
            if diagonal:
                x = jnp.where(visible_mask(x.shape, s * SUB), x, NEG_BIG)
            p = jnp.exp2(x)
            ds = (p * (dot_nt(v, do) - rows[h, qi, 1:2, cols])).astype(jnp.bfloat16)
            dkv[h, ki, :, HEAD:] += dot_nn(p.astype(jnp.bfloat16), do)
            dkv[h, ki, :, :HEAD] += dot_nn(ds, q)
            dqt[h, qi, :, cols] += dot_nn(kt[ki], ds)

    bias_copy.wait()
    stores = []
    for h in range(2):
        dqt[h] = jnp.zeros((SIDE, HEAD, span), jnp.float32)
        dkv[h] = jnp.zeros((SIDE, span, 2 * HEAD), jnp.float32)
        fill_bias(bias, bcol, h)
        wait_all(loads[h])
        combine(h)
        key_outs = outs[8 + SIDE * h : 8 + SIDE * (h + 1)]
        key_sources = [dkv.at[h, 0]] + [dkv_send.at[h, r] for r in range(1, SIDE)]
        key_stores = [
            pltpu.make_async_copy(source, out, sems.at[40 + SIDE * h + r])
            for r, (source, out) in enumerate(zip(key_sources, key_outs))
        ]

        def turn(r, _, h=h):
            kt[r] = kv[h, r, :, :HEAD].astype(jnp.float32).T.astype(jnp.bfloat16)
            return 0

        lax.fori_loop(0, SIDE, turn, 0)

        def one_key_span(ki, _, h=h, key_stores=key_stores):
            def one_query_span(qi, _):
                for_visible(h, qi, ki, block)
                return 0

            lax.fori_loop(0, SIDE, one_query_span, 0)
            scaled = dkv[h, ki, :, :HEAD] * SCALE
            dkv[h, ki, :, :HEAD] = scaled
            dkv_send[h, ki, :, :HEAD] = scaled.astype(jnp.bfloat16)
            dkv_send[h, ki, :, HEAD:] = dkv[h, ki, :, HEAD:].astype(jnp.bfloat16)
            for r in range(SIDE):
                pl.when(ki == r)(key_stores[r].start)
            return 0

        lax.fori_loop(0, SIDE, one_key_span, 0)
        stores += key_stores
        dqt[h, 0] = dqt[h, 0] * SCALE
        stores.append(begin(dqt.at[h, 0], outs[SIDE * h]))
        for r in range(1, SIDE):
            dq_send[h, r] = (dqt[h, r] * SCALE).astype(jnp.bfloat16)
            stores.append(begin(dq_send.at[h, r], outs[SIDE * h + r]))
    wait_all(stores)


def weight_kernel(*rest):
    dq_refs, in_refs, outs = rest[:4], rest[4:12], rest[12:16]
    dqs, inputs, sems = rest[16:]
    here, part = lax.axis_index("sp"), lax.axis_index("tp")
    z, x, y, core = here // SIDE, here % SIDE, part // 2, part % 2
    begin = copy_list(sems)
    copies = []
    for r in range(SIDE):
        of_span = (y - z + r + SIDE) % SIDE
        for other in range(2):
            held_by = core if other == 0 else 1 - core
            copies.append(begin(in_refs[SIDE * other + r], inputs.at[held_by, of_span]))
        copies.append(begin(dq_refs[r], dqs.at[(z + r) % SIDE]))
    wait_all(copies)
    width = outs[0].shape[1]
    for r in (1, 2, 3, 0):
        block = (x + r) % SIDE
        cols = pl.ds(pl.multiple_of((block % 2) * width, width), width)
        total = sum(dot_nn(dqs[a], inputs[block // 2, a, :, cols]) for a in range(SIDE))
        outs[r][...] = total.astype(outs[r].dtype)


ANY = pl.BlockSpec(memory_space=pl.ANY)
VM = pl.BlockSpec(memory_space=pltpu.VMEM)


def stats_call(bias, z_parts, x_parts, known=None):
    span = z_parts[0].shape[0]
    if known is None:
        slots, pair_count, pair_of, known = NEAR, 9, near_pairs, ()
        z_parts, x_parts = ([parts[r] for r in NEAR] for parts in (z_parts, x_parts))
    else:
        slots, pair_count, pair_of = range(SIDE), 7, far_pairs
    pairs = pair_count * span * span
    return pl.pallas_call(
        functools.partial(stats_kernel, slots, pair_count, pair_of),
        out_shape=[jax.ShapeDtypeStruct((SIDE, 8, span), jnp.float32)] * 2,
        in_specs=[ANY] * (1 + 2 * len(slots) + len(known)),
        out_specs=[ANY] * 2,
        scratch_shapes=[
            pltpu.VMEM(bias.shape, jnp.float32),
            pltpu.VMEM((2, SIDE, span, 2 * HEAD), jnp.bfloat16),
            pltpu.VMEM((2, SIDE, span, 2 * HEAD), jnp.bfloat16),
            pltpu.VMEM((SIDE, span, HEAD), jnp.float32),
            pltpu.VMEM((2, SIDE, 8, span), jnp.float32),
            pltpu.SemaphoreType.DMA((24,)),
        ],
        compiler_params=pltpu.CompilerParams(vmem_limit_bytes=62 << 20),
        cost_estimate=pl.CostEstimate(
            flops=4 * HEAD * pairs, bytes_accessed=4 << 20, transcendentals=pairs
        ),
        name="stats",
    )(bias, *z_parts, *x_parts, *known)


def grads_call(bias, z_parts, x_parts, z_stats, x_stats):
    span = z_parts[0].shape[0]
    pairs = 17 * span * span

    def shapes(*shape):
        own = jax.ShapeDtypeStruct(shape, jnp.float32)
        send = jax.ShapeDtypeStruct(shape, jnp.bfloat16)
        return ([own] + [send] * 3) * 2

    outs = pl.pallas_call(
        grads_kernel,
        out_shape=shapes(HEAD, span) + shapes(span, 2 * HEAD),
        in_specs=[ANY] * 17,
        out_specs=[ANY] * 16,
        scratch_shapes=[
            pltpu.VMEM(bias.shape, jnp.float32),
            pltpu.VMEM((2, SIDE, span, 2 * HEAD), jnp.bfloat16),
            pltpu.VMEM((2, SIDE, span, 2 * HEAD), jnp.bfloat16),
            pltpu.VMEM((SIDE, span, HEAD), jnp.float32),
            pltpu.VMEM((2, SIDE, SIDE, 8, span), jnp.float32),
            pltpu.VMEM((2, SIDE, 8, span), jnp.float32),
            pltpu.VMEM((SIDE, HEAD, span), jnp.bfloat16),
            pltpu.VMEM((2, SIDE, HEAD, span), jnp.float32),
            pltpu.VMEM((2, SIDE, span, 2 * HEAD), jnp.float32),
            pltpu.VMEM((2, SIDE, HEAD, span), jnp.bfloat16),
            pltpu.VMEM((2, SIDE, span, 2 * HEAD), jnp.bfloat16),
            pltpu.SemaphoreType.DMA((48,)),
        ],
        compiler_params=pltpu.CompilerParams(vmem_limit_bytes=62 << 20),
        cost_estimate=pl.CostEstimate(
            flops=10 * HEAD * pairs, bytes_accessed=8 << 20, transcendentals=pairs
        ),
        name="grads",
    )(bias, *z_parts, *x_parts, *z_stats, *x_stats)
    return outs[:4], outs[4:8], outs[8:12], outs[12:]


def weight_call(query_grads, inputs):
    cols, rows = query_grads[0].shape
    width = inputs[0].shape[1]
    own = jax.ShapeDtypeStruct((cols, width // 2), jnp.float32)
    send = jax.ShapeDtypeStruct((cols, width // 2), jnp.bfloat16)
    return pl.pallas_call(
        weight_kernel,
        out_shape=[own] + [send] * 3,
        in_specs=[ANY] * 12,
        out_specs=[VM] * 4,
        scratch_shapes=[
            pltpu.VMEM((SIDE, cols, rows), jnp.bfloat16),
            pltpu.VMEM((2, SIDE, rows, width), jnp.bfloat16),
            pltpu.SemaphoreType.DMA((12,)),
        ],
        compiler_params=pltpu.CompilerParams(vmem_limit_bytes=16 << 20),
        cost_estimate=pl.CostEstimate(
            flops=16 * rows * width * cols, bytes_accessed=6 << 20, transcendentals=0
        ),
        name="weight",
    )(*query_grads, *inputs)


def head_of(array, h):
    return array[:, h * HEAD : (h + 1) * HEAD]


def local(queries, keys, values, forget_logits, layer_input, out_grad):
    gates = lax.all_to_all(jnp.tile(forget_logits.T, (16, 1)), "sp", 0, 0, tiled=True)

    for_z = jnp.concatenate(
        [head_of(queries, 0), head_of(out_grad, 0), head_of(keys, 1), head_of(values, 1)], axis=1
    )
    for_x = jnp.concatenate(
        [head_of(keys, 0), head_of(values, 0), head_of(queries, 1), head_of(out_grad, 1)], axis=1
    )
    z_parts = fetched(for_z, along_z)
    x_parts = fetched(for_x, along_x)

    bias = pl.pallas_call(
        gates_kernel,
        out_shape=jax.ShapeDtypeStruct(gates.shape, jnp.float32),
        in_specs=[VM],
        out_specs=VM,
        cost_estimate=pl.CostEstimate(flops=10**6, bytes_accessed=1 << 17, transcendentals=0),
        name="gate_sums",
    )(gates)

    def over_zy(target):
        pairs = []
        for n in range(SIDE**3 * 2):
            zxyc = (n // 32, n // 8 % SIDE, n // 2 % SIDE, n % 2)
            new_z, new_y = target(zxyc[0], zxyc[2])
            pairs.append((n, new_z % SIDE * 32 + zxyc[1] * 8 + new_y % SIDE * 2 + zxyc[3]))
        return pairs

    everywhere = ("sp", "tp")
    moved = lax.ppermute(layer_input, everywhere, over_zy(lambda a, b: (a, a + b)))
    moved = lax.ppermute(moved, everywhere, over_zy(lambda a, b: (b - a, b)))
    inputs = [moved]
    for r in range(1, SIDE):
        inputs.append(lax.ppermute(moved, "tp", [(p, (p - 2 * r) % 8) for p in range(8)]))
    for part in list(inputs):
        inputs.append(lax.ppermute(part, "tp", [(p, p ^ 1) for p in range(8)]))

    known = stats_call(bias, z_parts, x_parts)
    stats_z, stats_x = stats_call(bias, z_parts, x_parts, known)
    z_stats = fetched(stats_z, along_z)
    x_stats = fetched(stats_x, along_x)
    dq_0, dq_1, dkv_0, dkv_1 = grads_call(bias, z_parts, x_parts, z_stats, x_stats)

    def summed(parts, axis_perm):
        total = parts[0]
        for r in range(1, SIDE):
            total = total + lax.ppermute(parts[r], "sp", axis_perm(r)).astype(jnp.float32)
        return total

    query_t = jnp.concatenate([summed(dq_0, along_z), summed(dq_1, along_x)], axis=0)
    low, dkv_0, dkv_1 = lax.optimization_barrier((query_t.astype(jnp.bfloat16), dkv_0, dkv_1))
    low_parts = fetched(low, along_z)
    terms = weight_call(low_parts, inputs)
    weight_grad = summed(terms, along_x).T
    sum_0, sum_1 = summed(dkv_0, along_x), summed(dkv_1, along_z)
    query_grad = query_t.T
    key_grad = jnp.concatenate([head_of(sum_0, 0), head_of(sum_1, 0)], axis=1)
    value_grad = jnp.concatenate([head_of(sum_0, 1), head_of(sum_1, 1)], axis=1)
    return (query_grad, key_grad, value_grad, weight_grad)


def solution(mesh):
    placed = P("sp", "tp")

    return jax.shard_map(
        local,
        mesh=mesh,
        in_specs=(placed,) * 6,
        out_specs=(placed,) * 4,
        check_vma=False,
    )
```

```python
import functools
import math

import jax
import jax.numpy as jnp
from jax import lax
from jax.experimental import pallas as pl
from jax.experimental.pallas import tpu as pltpu
from jax.sharding import PartitionSpec as P


HEAD = 128
SIDE = 4
SCALE = HEAD ** (-0.5)
LOG2E = math.log2(math.e)
NEG_BIG = -1e30
SUB = 256


def along_z(r):
    return [(4 * z + x, 4 * ((z + r) % SIDE) + x) for z in range(SIDE) for x in range(SIDE)]


def along_x(r):
    return [(4 * z + x, 4 * z + (x + r) % SIDE) for z in range(SIDE) for x in range(SIDE)]


def fetched(array, axis_perm):
    parts = [array]
    for r in range(1, SIDE):
        parts.append(lax.ppermute(array, "sp", axis_perm(-r)))
    return parts


def dot_nt(a, b):
    return lax.dot_general(a, b, (((1,), (1,)), ((), ())), preferred_element_type=jnp.float32)


def dot_nn(a, b):
    return lax.dot_general(a, b, (((1,), (0,)), ((), ())), preferred_element_type=jnp.float32)


def copy_list(sems):
    made = []

    def begin(src, dst):
        copy = pltpu.make_async_copy(src, dst, sems.at[len(made)])
        made.append(copy)
        copy.start()
        return copy

    return begin


def wait_all(copies):
    for c in copies:
        c.wait()


def start_loads(begin, h, z_refs, x_refs, slots, qd, kv):
    cols = pl.ds(h * 2 * HEAD, 2 * HEAD)
    q_refs, k_refs = (z_refs, x_refs) if h == 0 else (x_refs, z_refs)
    copies = []
    for r, q_ref, k_ref in zip(slots, q_refs, k_refs):
        copies.append(begin(q_ref.at[:, cols], qd.at[h, r]))
        copies.append(begin(k_ref.at[:, cols], kv.at[h, r]))
    return copies


def span_at(h, keys, r):
    here = lax.axis_index("sp")
    z, x = here // SIDE, here % SIDE
    if (h == 0) != keys:
        return SIDE * ((z + r) % SIDE) + x
    return SIDE * z + (x + r) % SIDE


def gates_kernel(logits_ref, out_ref):
    sums = jax.nn.log_sigmoid(logits_ref[...])
    rows, width = sums.shape
    lane = lax.broadcasted_iota(jnp.int32, sums.shape, 1)
    step = 1
    while step < width:
        sums = sums + jnp.where(lane >= step, pltpu.roll(sums, step, axis=1), 0.0)
        step *= 2
    shape = (rows, rows)
    mine, other = (lax.broadcasted_iota(jnp.int32, shape, d) for d in (0, 1))
    earlier = jnp.where((other < mine) & (other % 2 == mine % 2), 1.0, 0.0)
    totals = jnp.broadcast_to(sums[:, width - 1 :], (rows, HEAD))
    before = jnp.dot(
        earlier, totals, preferred_element_type=jnp.float32, precision=lax.Precision.HIGHEST
    )
    out_ref[...] = (sums + wide(before, width)) * LOG2E


def fill_bias(bias, bcol, h):
    def one(r, _):
        row = bias[pl.ds(2 * span_at(h, True, r) + h, 1), :]
        for j in range(4):
            tile = jnp.broadcast_to(row[:, j * HEAD : (j + 1) * HEAD], (HEAD, HEAD))
            bcol[h, r, j * HEAD : (j + 1) * HEAD, :] = tile.T
        return 0

    lax.fori_loop(0, SIDE, one, 0)


def for_visible(h, qi, ki, block):
    q_span, k_span = span_at(h, False, qi), span_at(h, True, ki)

    @pl.when(k_span < q_span)
    def _():
        block(h, qi, ki, False)

    @pl.when(k_span == q_span)
    def _():
        block(h, qi, ki, True)


def visible_mask(shape, first_query):
    key_at = lax.broadcasted_iota(jnp.int32, shape, 0)
    query_at = lax.broadcasted_iota(jnp.int32, shape, 1) + first_query
    return key_at <= query_at


def wide(tile, width):
    return jnp.concatenate([tile] * (width // tile.shape[1]), axis=1)


NEAR = (0, 1, 3)


def near_slot(n):
    return n + n // 2


def near_pairs(n):
    return near_slot(n // 3), near_slot(n % 3)


def far_pairs(n):
    near = near_slot(jnp.maximum(n - SIDE, 0))
    return jnp.where(n < SIDE, 2, near), jnp.where(n < SIDE, n, 2)


def stats_kernel(slots, pair_count, pair_of, bias_ref, *rest):
    n_slots = len(slots)
    z_refs, x_refs = rest[:n_slots], rest[n_slots : 2 * n_slots]
    rest = rest[2 * n_slots :]
    known, rest = rest[:-8], rest[-8:]
    outs = rest[:2]
    bias, qd, kv, bcol, stats, sems = rest[2:]
    span = qd.shape[2]
    begin = copy_list(sems)
    bias_copy = begin(bias_ref, bias)
    loads = []
    for h in range(2):
        loads.append(start_loads(begin, h, z_refs, x_refs, slots, qd, kv))
        if known:
            loads[h].append(begin(known[h], stats.at[h]))
        else:
            stats[h] = jnp.zeros((SIDE, 8, span), jnp.float32)
            stats[h, :, 0:1, :] = jnp.full((SIDE, 1, span), NEG_BIG, jnp.float32)

    def block(h, qi, ki, diagonal):
        for s in range(span // SUB):
            cols = slice(s * SUB, (s + 1) * SUB)
            q = qd[h, qi, cols, :HEAD]
            do = qd[h, qi, cols, HEAD:]
            seen = (s + 1) * SUB if diagonal else span
            k = kv[h, ki, :seen, :HEAD]
            v = kv[h, ki, :seen, HEAD:]
            x = dot_nt(k, q) * (SCALE * LOG2E) - wide(bcol[h, ki, :seen], SUB)
            if diagonal:
                x = jnp.where(visible_mask(x.shape, s * SUB), x, NEG_BIG)
            dp = dot_nt(v, do)
            old = stats[h, qi, 0:1, cols]
            new = jnp.maximum(old, jnp.max(x, axis=0, keepdims=True))
            p = jnp.exp2(x - new)
            shrink = jnp.exp2(old - new)
            stats[h, qi, 0:1, cols] = new
            stats[h, qi, 1:2, cols] = stats[h, qi, 1:2, cols] * shrink + jnp.sum(
                p, axis=0, keepdims=True
            )
            stats[h, qi, 2:3, cols] = stats[h, qi, 2:3, cols] * shrink + jnp.sum(
                p * dp, axis=0, keepdims=True
            )

    bias_copy.wait()
    stores = []
    for h in range(2):
        fill_bias(bias, bcol, h)
    for h in range(2):
        wait_all(loads[h])

        def one_pair(n, _, h=h):
            qi, ki = pair_of(n)
            for_visible(h, qi, ki, block)
            return 0

        lax.fori_loop(0, pair_count, one_pair, 0)
        stores.append(begin(stats.at[h], outs[h]))
    wait_all(stores)


def grads_kernel(bias_ref, *rest):
    z_refs, x_refs = rest[:4], rest[4:8]
    stat_refs = (rest[8:12], rest[12:16])
    outs = rest[16:32]
    bias, qd, kv, bcol, parts, rows, kt, dqt, dkv, dq_send, dkv_send, sems = rest[32:]
    span = qd.shape[2]
    begin = copy_list(sems)
    bias_copy = begin(bias_ref, bias)
    loads = []
    for h in range(2):
        stat_copies = [begin(stat_refs[h][s], parts.at[h, s]) for s in range(SIDE)]
        loads.append(stat_copies + start_loads(begin, h, z_refs, x_refs, range(SIDE), qd, kv))

    def combine(h):
        for r in range(SIDE):
            found = [parts[h, s, (r - s) % SIDE] for s in range(SIDE)]
            top = functools.reduce(jnp.maximum, [p[0:1, :] for p in found])
            factors = [jnp.exp2(p[0:1, :] - top) for p in found]
            total = sum(p[1:2, :] * f for p, f in zip(found, factors))
            mixed = sum(p[2:3, :] * f for p, f in zip(found, factors))
            rows[h, r, 0:1, :] = top + jnp.log2(total)
            rows[h, r, 1:2, :] = mixed / total

    def block(h, qi, ki, diagonal):
        for s in range(span // SUB):
            cols = slice(s * SUB, (s + 1) * SUB)
            q = qd[h, qi, cols, :HEAD]
            do = qd[h, qi, cols, HEAD:]
            seen = (s + 1) * SUB if diagonal else span
            k = kv[h, ki, :seen, :HEAD]
            v = kv[h, ki, :seen, HEAD:]
            x = dot_nt(k, q) * (SCALE * LOG2E) - wide(bcol[h, ki, :seen], SUB)
            x = x - rows[h, qi, 0:1, cols]
            if diagonal:
                x = jnp.where(visible_mask(x.shape, s * SUB), x, NEG_BIG)
            p = jnp.exp2(x)
            ds = (p * (dot_nt(v, do) - rows[h, qi, 1:2, cols])).astype(jnp.bfloat16)
            dkv[h, ki, :seen, HEAD:] += dot_nn(p.astype(jnp.bfloat16), do)
            dkv[h, ki, :seen, :HEAD] += dot_nn(ds, q)
            dqt[h, qi, :, cols] += dot_nn(kt[ki, :, :seen], ds)

    dqt[...] = jnp.zeros_like(dqt)
    dkv[...] = jnp.zeros_like(dkv)
    bias_copy.wait()
    stores = []
    for h in range(2):
        fill_bias(bias, bcol, h)
    for h in range(2):
        wait_all(loads[h])
        combine(h)
        key_outs = outs[8 + SIDE * h : 8 + SIDE * (h + 1)]
        key_sources = [dkv.at[h, 0]] + [dkv_send.at[h, r] for r in range(1, SIDE)]
        key_stores = [
            pltpu.make_async_copy(source, out, sems.at[40 + SIDE * h + r])
            for r, (source, out) in enumerate(zip(key_sources, key_outs))
        ]

        def turn(r, _, h=h):
            kt[r] = kv[h, r, :, :HEAD].astype(jnp.float32).T.astype(jnp.bfloat16)
            return 0

        lax.fori_loop(0, SIDE, turn, 0)

        def one_key_span(ki, _, h=h, key_stores=key_stores):
            def one_query_span(qi, _):
                for_visible(h, qi, ki, block)
                return 0

            lax.fori_loop(0, SIDE, one_query_span, 0)
            scaled = dkv[h, ki, :, :HEAD] * SCALE
            dkv[h, ki, :, :HEAD] = scaled
            dkv_send[h, ki, :, :HEAD] = scaled.astype(jnp.bfloat16)
            dkv_send[h, ki, :, HEAD:] = dkv[h, ki, :, HEAD:].astype(jnp.bfloat16)
            for r in range(SIDE):
                pl.when(ki == r)(key_stores[r].start)
            return 0

        lax.fori_loop(0, SIDE, one_key_span, 0)
        stores += key_stores
        dqt[h, 0] = dqt[h, 0] * SCALE
        stores.append(begin(dqt.at[h, 0], outs[SIDE * h]))
        for r in range(1, SIDE):
            dq_send[h, r] = (dqt[h, r] * SCALE).astype(jnp.bfloat16)
            stores.append(begin(dq_send.at[h, r], outs[SIDE * h + r]))
    wait_all(stores)


def weight_kernel(*rest):
    dq_refs, in_refs, outs = rest[:4], rest[4:12], rest[12:16]
    dqs, inputs, sems = rest[16:]
    here, part = lax.axis_index("sp"), lax.axis_index("tp")
    z, x, y, core = here // SIDE, here % SIDE, part // 2, part % 2
    begin = copy_list(sems)
    copies = []
    for r in range(SIDE):
        of_span = (y - z + r + SIDE) % SIDE
        for other in range(2):
            held_by = core if other == 0 else 1 - core
            copies.append(begin(in_refs[SIDE * other + r], inputs.at[held_by, of_span]))
        copies.append(begin(dq_refs[r], dqs.at[(z + r) % SIDE]))
    wait_all(copies)
    width = outs[0].shape[1]
    for r in (1, 2, 3, 0):
        block = (x + r) % SIDE
        cols = pl.ds(pl.multiple_of((block % 2) * width, width), width)
        total = sum(dot_nn(dqs[a], inputs[block // 2, a, :, cols]) for a in range(SIDE))
        outs[r][...] = total.astype(outs[r].dtype)


def query_kernel(*refs):
    parts, (low_ref, grad_ref) = refs[:8], refs[8:]
    for h in range(2):
        total = sum(ref[...].astype(jnp.float32) for ref in parts[SIDE * h : SIDE * (h + 1)])
        cut = slice(h * HEAD, (h + 1) * HEAD)
        low_ref[cut, :] = total.astype(jnp.bfloat16)
        grad_ref[:, cut] = total.T


def keys_kernel(*refs):
    parts, outs = refs[:8], refs[8:]
    for h in range(2):
        for n, out in enumerate(outs):
            cut = slice(n * HEAD, (n + 1) * HEAD)
            out[:, h * HEAD : (h + 1) * HEAD] = sum(
                ref[:, cut].astype(jnp.float32) for ref in parts[SIDE * h : SIDE * (h + 1)]
            )


ANY = pl.BlockSpec(memory_space=pl.ANY)
VM = pl.BlockSpec(memory_space=pltpu.VMEM)


def stats_call(bias, z_parts, x_parts, known=None):
    span = z_parts[0].shape[0]
    if known is None:
        slots, pair_count, pair_of, known = NEAR, 9, near_pairs, ()
        z_parts, x_parts = ([parts[r] for r in NEAR] for parts in (z_parts, x_parts))
    else:
        slots, pair_count, pair_of = range(SIDE), 7, far_pairs
    pairs = pair_count * span * span
    return pl.pallas_call(
        functools.partial(stats_kernel, slots, pair_count, pair_of),
        out_shape=[jax.ShapeDtypeStruct((SIDE, 8, span), jnp.float32)] * 2,
        in_specs=[ANY] * (1 + 2 * len(slots) + len(known)),
        out_specs=[ANY] * 2,
        scratch_shapes=[
            pltpu.VMEM(bias.shape, jnp.float32),
            pltpu.VMEM((2, SIDE, span, 2 * HEAD), jnp.bfloat16),
            pltpu.VMEM((2, SIDE, span, 2 * HEAD), jnp.bfloat16),
            pltpu.VMEM((2, SIDE, span, HEAD), jnp.float32),
            pltpu.VMEM((2, SIDE, 8, span), jnp.float32),
            pltpu.SemaphoreType.DMA((24,)),
        ],
        compiler_params=pltpu.CompilerParams(vmem_limit_bytes=62 << 20),
        cost_estimate=pl.CostEstimate(
            flops=4 * HEAD * pairs, bytes_accessed=4 << 20, transcendentals=pairs
        ),
        name="stats",
    )(bias, *z_parts, *x_parts, *known)


def grads_call(bias, z_parts, x_parts, z_stats, x_stats):
    span = z_parts[0].shape[0]
    pairs = 17 * span * span

    def shapes(*shape):
        own = jax.ShapeDtypeStruct(shape, jnp.float32)
        send = jax.ShapeDtypeStruct(shape, jnp.bfloat16)
        return ([own] + [send] * 3) * 2

    outs = pl.pallas_call(
        grads_kernel,
        out_shape=shapes(HEAD, span) + shapes(span, 2 * HEAD),
        in_specs=[ANY] * 17,
        out_specs=[ANY] * 16,
        scratch_shapes=[
            pltpu.VMEM(bias.shape, jnp.float32),
            pltpu.VMEM((2, SIDE, span, 2 * HEAD), jnp.bfloat16),
            pltpu.VMEM((2, SIDE, span, 2 * HEAD), jnp.bfloat16),
            pltpu.VMEM((2, SIDE, span, HEAD), jnp.float32),
            pltpu.VMEM((2, SIDE, SIDE, 8, span), jnp.float32),
            pltpu.VMEM((2, SIDE, 8, span), jnp.float32),
            pltpu.VMEM((SIDE, HEAD, span), jnp.bfloat16),
            pltpu.VMEM((2, SIDE, HEAD, span), jnp.float32),
            pltpu.VMEM((2, SIDE, span, 2 * HEAD), jnp.float32),
            pltpu.VMEM((2, SIDE, HEAD, span), jnp.bfloat16),
            pltpu.VMEM((2, SIDE, span, 2 * HEAD), jnp.bfloat16),
            pltpu.SemaphoreType.DMA((48,)),
        ],
        compiler_params=pltpu.CompilerParams(vmem_limit_bytes=62 << 20),
        cost_estimate=pl.CostEstimate(
            flops=10 * HEAD * pairs, bytes_accessed=8 << 20, transcendentals=pairs
        ),
        name="grads",
    )(bias, *z_parts, *x_parts, *z_stats, *x_stats)
    return outs[:4], outs[4:8], outs[8:12], outs[12:]


def weight_call(query_grads, inputs):
    cols, rows = query_grads[0].shape
    width = inputs[0].shape[1]
    own = jax.ShapeDtypeStruct((cols, width // 2), jnp.float32)
    send = jax.ShapeDtypeStruct((cols, width // 2), jnp.bfloat16)
    return pl.pallas_call(
        weight_kernel,
        out_shape=[own] + [send] * 3,
        in_specs=[ANY] * 12,
        out_specs=[VM] * 4,
        scratch_shapes=[
            pltpu.VMEM((SIDE, cols, rows), jnp.bfloat16),
            pltpu.VMEM((2, SIDE, rows, width), jnp.bfloat16),
            pltpu.SemaphoreType.DMA((12,)),
        ],
        compiler_params=pltpu.CompilerParams(vmem_limit_bytes=16 << 20),
        cost_estimate=pl.CostEstimate(
            flops=16 * rows * width * cols, bytes_accessed=6 << 20, transcendentals=0
        ),
        name="weight",
    )(*query_grads, *inputs)


def query_call(parts_0, parts_1):
    rows, span = parts_0[0].shape
    return pl.pallas_call(
        query_kernel,
        out_shape=[
            jax.ShapeDtypeStruct((2 * rows, span), jnp.bfloat16),
            jax.ShapeDtypeStruct((span, 2 * rows), jnp.float32),
        ],
        in_specs=[VM] * 8,
        out_specs=[VM] * 2,
        compiler_params=pltpu.CompilerParams(vmem_limit_bytes=16 << 20),
        cost_estimate=pl.CostEstimate(flops=10**6, bytes_accessed=2 << 20, transcendentals=0),
        name="query_sums",
    )(*parts_0, *parts_1)


def keys_call(parts_0, parts_1):
    span, cols = parts_0[0].shape
    block = pl.BlockSpec((span // SIDE, cols), lambda n: (n, 0))
    return pl.pallas_call(
        keys_kernel,
        grid=(SIDE,),
        out_shape=[jax.ShapeDtypeStruct((span, cols), jnp.float32)] * 2,
        in_specs=[block] * 8,
        out_specs=[block] * 2,
        compiler_params=pltpu.CompilerParams(vmem_limit_bytes=16 << 20),
        cost_estimate=pl.CostEstimate(flops=10**6, bytes_accessed=4 << 20, transcendentals=0),
        name="key_sums",
    )(*parts_0, *parts_1)


def head_of(array, h):
    return array[:, h * HEAD : (h + 1) * HEAD]


def local(queries, keys, values, forget_logits, layer_input, out_grad):
    gates = lax.all_to_all(jnp.tile(forget_logits.T, (16, 1)), "sp", 0, 0, tiled=True)

    for_z = jnp.concatenate(
        [head_of(queries, 0), head_of(out_grad, 0), head_of(keys, 1), head_of(values, 1)], axis=1
    )
    for_x = jnp.concatenate(
        [head_of(keys, 0), head_of(values, 0), head_of(queries, 1), head_of(out_grad, 1)], axis=1
    )
    z_parts = fetched(for_z, along_z)
    x_parts = fetched(for_x, along_x)

    bias = pl.pallas_call(
        gates_kernel,
        out_shape=jax.ShapeDtypeStruct(gates.shape, jnp.float32),
        in_specs=[VM],
        out_specs=VM,
        cost_estimate=pl.CostEstimate(flops=10**6, bytes_accessed=1 << 17, transcendentals=0),
        name="gate_sums",
    )(gates)

    def over_zy(target):
        pairs = []
        for n in range(SIDE**3 * 2):
            zxyc = (n // 32, n // 8 % SIDE, n // 2 % SIDE, n % 2)
            new_z, new_y = target(zxyc[0], zxyc[2])
            pairs.append((n, new_z % SIDE * 32 + zxyc[1] * 8 + new_y % SIDE * 2 + zxyc[3]))
        return pairs

    everywhere = ("sp", "tp")
    moved = lax.ppermute(layer_input, everywhere, over_zy(lambda a, b: (a, a + b)))
    moved = lax.ppermute(moved, everywhere, over_zy(lambda a, b: (b - a, b)))
    inputs = [moved]
    for r in range(1, SIDE):
        inputs.append(lax.ppermute(moved, "tp", [(p, (p - 2 * r) % 8) for p in range(8)]))
    for part in list(inputs):
        inputs.append(lax.ppermute(part, "tp", [(p, p ^ 1) for p in range(8)]))

    known = stats_call(bias, z_parts, x_parts)
    stats_z, stats_x = stats_call(bias, z_parts, x_parts, known)
    z_stats = fetched(stats_z, along_z)
    x_stats = fetched(stats_x, along_x)
    dq_0, dq_1, dkv_0, dkv_1 = grads_call(bias, z_parts, x_parts, z_stats, x_stats)

    def arrived(parts, axis_perm):
        return [parts[0]] + [
            lax.ppermute(parts[r], "sp", axis_perm(r)) for r in range(1, SIDE)
        ]

    dq_0, dq_1 = arrived(dq_0, along_z), arrived(dq_1, along_x)
    low, query_grad = query_call(dq_0, dq_1)
    low, dkv_0, dkv_1 = lax.optimization_barrier((low, dkv_0, dkv_1))
    low_parts = fetched(low, along_z)
    terms = weight_call(low_parts, inputs)
    terms = arrived(terms, along_x)
    weight_grad = sum(part.astype(jnp.float32) for part in terms).T
    dkv_0, dkv_1 = arrived(dkv_0, along_x), arrived(dkv_1, along_z)
    key_grad, value_grad = keys_call(dkv_0, dkv_1)
    return (query_grad, key_grad, value_grad, weight_grad)


def solution(mesh):
    placed = P("sp", "tp")

    return jax.shard_map(
        local,
        mesh=mesh,
        in_specs=(placed,) * 6,
        out_specs=(placed,) * 4,
        check_vma=False,
    )
```

```python
import functools
import math

import jax
import jax.numpy as jnp
from jax import lax
from jax.experimental import pallas as pl
from jax.experimental.pallas import tpu as pltpu
from jax.sharding import PartitionSpec as P


HEAD = 128
SIDE = 4
SCALE = HEAD ** (-0.5)
LOG2E = math.log2(math.e)
NEG_BIG = -1e30
SUB = 256


def along_z(r):
    return [(4 * z + x, 4 * ((z + r) % SIDE) + x) for z in range(SIDE) for x in range(SIDE)]


def along_x(r):
    return [(4 * z + x, 4 * z + (x + r) % SIDE) for z in range(SIDE) for x in range(SIDE)]


def fetched(array, axis_perm):
    parts = [array]
    for r in range(1, SIDE):
        parts.append(lax.ppermute(array, "sp", axis_perm(-r)))
    return parts


def dot_nt(a, b):
    return lax.dot_general(a, b, (((1,), (1,)), ((), ())), preferred_element_type=jnp.float32)


def dot_nn(a, b):
    return lax.dot_general(a, b, (((1,), (0,)), ((), ())), preferred_element_type=jnp.float32)


def copy_list(sems):
    made = []

    def begin(src, dst):
        copy = pltpu.make_async_copy(src, dst, sems.at[len(made)])
        made.append(copy)
        copy.start()
        return copy

    return begin


def wait_all(copies):
    for c in copies:
        c.wait()


def start_loads(begin, h, z_refs, x_refs, slots, qd, kv):
    cols = pl.ds(h * 2 * HEAD, 2 * HEAD)
    q_refs, k_refs = (z_refs, x_refs) if h == 0 else (x_refs, z_refs)
    copies = []
    for r, q_ref, k_ref in zip(slots, q_refs, k_refs):
        copies.append(begin(q_ref.at[:, cols], qd.at[h, r]))
        copies.append(begin(k_ref.at[:, cols], kv.at[h, r]))
    return copies


def span_at(h, keys, r):
    here = lax.axis_index("sp")
    z, x = here // SIDE, here % SIDE
    if (h == 0) != keys:
        return SIDE * ((z + r) % SIDE) + x
    return SIDE * z + (x + r) % SIDE


def gate_sums(gates, bias):
    spans, heads, width = gates.shape
    for n in range(spans):
        bias[heads * n : heads * (n + 1), :] = gates[n]
    sums = jax.nn.log_sigmoid(bias[...])
    rows = spans * heads
    lane = lax.broadcasted_iota(jnp.int32, sums.shape, 1)
    step = 1
    while step < width:
        sums = sums + jnp.where(lane >= step, pltpu.roll(sums, step, axis=1), 0.0)
        step *= 2
    shape = (rows, rows)
    mine, other = (lax.broadcasted_iota(jnp.int32, shape, d) for d in (0, 1))
    earlier = jnp.where((other < mine) & (other % heads == mine % heads), 1.0, 0.0)
    totals = jnp.broadcast_to(sums[:, width - 1 :], (rows, HEAD))
    before = jnp.dot(
        earlier, totals, preferred_element_type=jnp.float32, precision=lax.Precision.HIGHEST
    )
    bias[...] = (sums + wide(before, width)) * LOG2E


def fill_bias(bias, bcol, h):
    def one(r, _):
        row = bias[pl.ds(2 * span_at(h, True, r) + h, 1), :]
        for j in range(4):
            tile = jnp.broadcast_to(row[:, j * HEAD : (j + 1) * HEAD], (HEAD, HEAD))
            bcol[h, r, j * HEAD : (j + 1) * HEAD, :] = tile.T
        return 0

    lax.fori_loop(0, SIDE, one, 0)


def for_visible(h, qi, ki, block):
    q_span, k_span = span_at(h, False, qi), span_at(h, True, ki)

    @pl.when(k_span < q_span)
    def _():
        block(h, qi, ki, False)

    @pl.when(k_span == q_span)
    def _():
        block(h, qi, ki, True)


def visible_mask(shape, first_query):
    key_at = lax.broadcasted_iota(jnp.int32, shape, 0)
    query_at = lax.broadcasted_iota(jnp.int32, shape, 1) + first_query
    return key_at <= query_at


def wide(tile, width):
    return jnp.concatenate([tile] * (width // tile.shape[1]), axis=1)


NEAR = (0, 1, 3)


def near_slot(n):
    return n + n // 2


def near_pairs(n):
    return near_slot(n // 3), near_slot(n % 3)


def far_pairs(n):
    near = near_slot(jnp.maximum(n - SIDE, 0))
    return jnp.where(n < SIDE, 2, near), jnp.where(n < SIDE, n, 2)


def stats_kernel(slots, pair_count, pair_of, near, bias_ref, *rest):
    n_slots = len(slots)
    z_refs, x_refs = rest[:n_slots], rest[n_slots : 2 * n_slots]
    rest = rest[2 * n_slots :]
    n_scratch = 7 if near else 6
    n_outs = 3 if near else 2
    scratch, rest = rest[-n_scratch:], rest[:-n_scratch]
    outs, known = rest[-n_outs:], rest[:-n_outs]
    bias, qd, kv, bcol, stats, sems = scratch[:6]
    span = qd.shape[2]
    begin = copy_list(sems)
    bias_copy = begin(bias_ref, scratch[6] if near else bias)
    loads = []
    for h in range(2):
        loads.append(start_loads(begin, h, z_refs, x_refs, slots, qd, kv))
        if near:
            stats[h] = jnp.zeros((SIDE, 8, span), jnp.float32)
            stats[h, :, 0:1, :] = jnp.full((SIDE, 1, span), NEG_BIG, jnp.float32)
        else:
            loads[h].append(begin(known[h], stats.at[h]))

    def block(h, qi, ki, diagonal):
        for s in range(span // SUB):
            cols = slice(s * SUB, (s + 1) * SUB)
            q = qd[h, qi, cols, :HEAD]
            do = qd[h, qi, cols, HEAD:]
            seen = (s + 1) * SUB if diagonal else span
            k = kv[h, ki, :seen, :HEAD]
            v = kv[h, ki, :seen, HEAD:]
            x = dot_nt(k, q) * (SCALE * LOG2E) - wide(bcol[h, ki, :seen], SUB)
            if diagonal:
                x = jnp.where(visible_mask(x.shape, s * SUB), x, NEG_BIG)
            dp = dot_nt(v, do)
            old = stats[h, qi, 0:1, cols]
            new = jnp.maximum(old, jnp.max(x, axis=0, keepdims=True))
            p = jnp.exp2(x - new)
            shrink = jnp.exp2(old - new)
            stats[h, qi, 0:1, cols] = new
            stats[h, qi, 1:2, cols] = stats[h, qi, 1:2, cols] * shrink + jnp.sum(
                p, axis=0, keepdims=True
            )
            stats[h, qi, 2:3, cols] = stats[h, qi, 2:3, cols] * shrink + jnp.sum(
                p * dp, axis=0, keepdims=True
            )

    bias_copy.wait()
    stores = []
    if near:
        gate_sums(scratch[6], bias)
        stores.append(begin(bias, outs[2]))
    for h in range(2):
        fill_bias(bias, bcol, h)
    for h in range(2):
        wait_all(loads[h])

        def one_pair(n, _, h=h):
            qi, ki = pair_of(n)
            for_visible(h, qi, ki, block)
            return 0

        lax.fori_loop(0, pair_count, one_pair, 0)
        stores.append(begin(stats.at[h], outs[h]))
    wait_all(stores)


def grads_kernel(bias_ref, *rest):
    z_refs, x_refs = rest[:4], rest[4:8]
    stat_refs = (rest[8:12], rest[12:16])
    outs = rest[16:32]
    bias, qd, kv, bcol, parts, rows, kt, dqt, dkv, dq_send, dkv_send, sems = rest[32:]
    span = qd.shape[2]
    begin = copy_list(sems)
    bias_copy = begin(bias_ref, bias)
    loads = []
    for h in range(2):
        stat_copies = [begin(stat_refs[h][s], parts.at[h, s]) for s in range(SIDE)]
        loads.append(stat_copies + start_loads(begin, h, z_refs, x_refs, range(SIDE), qd, kv))

    def combine(h):
        for r in range(SIDE):
            found = [parts[h, s, (r - s) % SIDE] for s in range(SIDE)]
            top = functools.reduce(jnp.maximum, [p[0:1, :] for p in found])
            factors = [jnp.exp2(p[0:1, :] - top) for p in found]
            total = sum(p[1:2, :] * f for p, f in zip(found, factors))
            mixed = sum(p[2:3, :] * f for p, f in zip(found, factors))
            rows[h, r, 0:1, :] = top + jnp.log2(total)
            rows[h, r, 1:2, :] = mixed / total

    def block(h, qi, ki, diagonal):
        for s in range(span // SUB):
            cols = slice(s * SUB, (s + 1) * SUB)
            q = qd[h, qi, cols, :HEAD]
            do = qd[h, qi, cols, HEAD:]
            seen = (s + 1) * SUB if diagonal else span
            k = kv[h, ki, :seen, :HEAD]
            v = kv[h, ki, :seen, HEAD:]
            x = dot_nt(k, q) * (SCALE * LOG2E) - wide(bcol[h, ki, :seen], SUB)
            x = x - rows[h, qi, 0:1, cols]
            if diagonal:
                x = jnp.where(visible_mask(x.shape, s * SUB), x, NEG_BIG)
            p = jnp.exp2(x)
            ds = (p * (dot_nt(v, do) - rows[h, qi, 1:2, cols])).astype(jnp.bfloat16)
            dkv[h, ki, :seen, HEAD:] += dot_nn(p.astype(jnp.bfloat16), do)
            dkv[h, ki, :seen, :HEAD] += dot_nn(ds, q)
            dqt[h, qi, :, cols] += dot_nn(kt[ki, :, :seen], ds)

    dqt[...] = jnp.zeros_like(dqt)
    dkv[...] = jnp.zeros_like(dkv)
    bias_copy.wait()
    stores = []
    for h in range(2):
        fill_bias(bias, bcol, h)
    for h in range(2):
        wait_all(loads[h])
        combine(h)
        key_outs = outs[8 + SIDE * h : 8 + SIDE * (h + 1)]
        key_sources = [dkv.at[h, 0]] + [dkv_send.at[h, r] for r in range(1, SIDE)]
        key_stores = [
            pltpu.make_async_copy(source, out, sems.at[40 + SIDE * h + r])
            for r, (source, out) in enumerate(zip(key_sources, key_outs))
        ]

        def turn(r, _, h=h):
            kt[r] = kv[h, r, :, :HEAD].astype(jnp.float32).T.astype(jnp.bfloat16)
            return 0

        lax.fori_loop(0, SIDE, turn, 0)

        def one_key_span(ki, _, h=h, key_stores=key_stores):
            def one_query_span(qi, _):
                for_visible(h, qi, ki, block)
                return 0

            lax.fori_loop(0, SIDE, one_query_span, 0)
            scaled = dkv[h, ki, :, :HEAD] * SCALE
            dkv[h, ki, :, :HEAD] = scaled
            dkv_send[h, ki, :, :HEAD] = scaled.astype(jnp.bfloat16)
            dkv_send[h, ki, :, HEAD:] = dkv[h, ki, :, HEAD:].astype(jnp.bfloat16)
            for r in range(SIDE):
                pl.when(ki == r)(key_stores[r].start)
            return 0

        lax.fori_loop(0, SIDE, one_key_span, 0)
        stores += key_stores
        dqt[h, 0] = dqt[h, 0] * SCALE
        stores.append(begin(dqt.at[h, 0], outs[SIDE * h]))
        for r in range(1, SIDE):
            dq_send[h, r] = (dqt[h, r] * SCALE).astype(jnp.bfloat16)
            stores.append(begin(dq_send.at[h, r], outs[SIDE * h + r]))
    wait_all(stores)


def weight_kernel(*rest):
    dq_refs, in_refs, outs = rest[:4], rest[4:12], rest[12:16]
    dqs, inputs, sems = rest[16:]
    here, part = lax.axis_index("sp"), lax.axis_index("tp")
    z, x, y, core = here // SIDE, here % SIDE, part // 2, part % 2
    begin = copy_list(sems)
    copies = []
    for r in range(SIDE):
        of_span = (y - z + r + SIDE) % SIDE
        for other in range(2):
            held_by = core if other == 0 else 1 - core
            copies.append(begin(in_refs[SIDE * other + r], inputs.at[held_by, of_span]))
        copies.append(begin(dq_refs[r], dqs.at[(z + r) % SIDE]))
    wait_all(copies)
    width = outs[0].shape[1]
    for r in (1, 2, 3, 0):
        block = (x + r) % SIDE
        cols = pl.ds(pl.multiple_of((block % 2) * width, width), width)
        total = sum(dot_nn(dqs[a], inputs[block // 2, a, :, cols]) for a in range(SIDE))
        outs[r][...] = total.astype(outs[r].dtype)


def query_kernel(*refs):
    parts, (low_ref, grad_ref, own, sent, sems) = refs[:8], refs[8:]
    begin = copy_list(sems)
    loads = []
    for h in range(2):
        loads.append([begin(parts[SIDE * h], own.at[h])])
        loads[h] += [begin(parts[SIDE * h + r], sent.at[h, r]) for r in range(1, SIDE)]
    for h in range(2):
        wait_all(loads[h])
        total = own[h] + sum(sent[h, r].astype(jnp.float32) for r in range(1, SIDE))
        cut = slice(h * HEAD, (h + 1) * HEAD)
        low_ref[cut, :] = total.astype(jnp.bfloat16)
        grad_ref[:, cut] = total.T


def keys_kernel(*refs):
    parts, outs = refs[:8], refs[8:]
    for h in range(2):
        for n, out in enumerate(outs):
            cut = slice(n * HEAD, (n + 1) * HEAD)
            out[:, h * HEAD : (h + 1) * HEAD] = sum(
                ref[:, cut].astype(jnp.float32) for ref in parts[SIDE * h : SIDE * (h + 1)]
            )


ANY = pl.BlockSpec(memory_space=pl.ANY)
VM = pl.BlockSpec(memory_space=pltpu.VMEM)


def stats_call(bias, z_parts, x_parts, known=()):
    span = z_parts[0].shape[0]
    near = not known
    rows = 2 * SIDE * SIDE
    out_shape = [jax.ShapeDtypeStruct((SIDE, 8, span), jnp.float32)] * 2
    scratch = [
        pltpu.VMEM((rows, span), jnp.float32),
        pltpu.VMEM((2, SIDE, span, 2 * HEAD), jnp.bfloat16),
        pltpu.VMEM((2, SIDE, span, 2 * HEAD), jnp.bfloat16),
        pltpu.VMEM((2, SIDE, span, HEAD), jnp.float32),
        pltpu.VMEM((2, SIDE, 8, span), jnp.float32),
        pltpu.SemaphoreType.DMA((24,)),
    ]
    if near:
        slots, pair_count, pair_of = NEAR, 9, near_pairs
        z_parts, x_parts = ([parts[r] for r in NEAR] for parts in (z_parts, x_parts))
        out_shape.append(jax.ShapeDtypeStruct((rows, span), jnp.float32))
        scratch.append(pltpu.VMEM(bias.shape, jnp.float32))
    else:
        slots, pair_count, pair_of = range(SIDE), 7, far_pairs
    pairs = pair_count * span * span
    return pl.pallas_call(
        functools.partial(stats_kernel, slots, pair_count, pair_of, near),
        out_shape=out_shape,
        in_specs=[ANY] * (1 + 2 * len(slots) + len(known)),
        out_specs=[ANY] * len(out_shape),
        scratch_shapes=scratch,
        compiler_params=pltpu.CompilerParams(vmem_limit_bytes=62 << 20),
        cost_estimate=pl.CostEstimate(
            flops=4 * HEAD * pairs, bytes_accessed=4 << 20, transcendentals=pairs
        ),
        name="stats",
    )(bias, *z_parts, *x_parts, *known)


def grads_call(bias, z_parts, x_parts, z_stats, x_stats):
    span = z_parts[0].shape[0]
    pairs = 17 * span * span

    def shapes(*shape):
        own = jax.ShapeDtypeStruct(shape, jnp.float32)
        send = jax.ShapeDtypeStruct(shape, jnp.bfloat16)
        return ([own] + [send] * 3) * 2

    outs = pl.pallas_call(
        grads_kernel,
        out_shape=shapes(HEAD, span) + shapes(span, 2 * HEAD),
        in_specs=[ANY] * 17,
        out_specs=[ANY] * 16,
        scratch_shapes=[
            pltpu.VMEM(bias.shape, jnp.float32),
            pltpu.VMEM((2, SIDE, span, 2 * HEAD), jnp.bfloat16),
            pltpu.VMEM((2, SIDE, span, 2 * HEAD), jnp.bfloat16),
            pltpu.VMEM((2, SIDE, span, HEAD), jnp.float32),
            pltpu.VMEM((2, SIDE, SIDE, 8, span), jnp.float32),
            pltpu.VMEM((2, SIDE, 8, span), jnp.float32),
            pltpu.VMEM((SIDE, HEAD, span), jnp.bfloat16),
            pltpu.VMEM((2, SIDE, HEAD, span), jnp.float32),
            pltpu.VMEM((2, SIDE, span, 2 * HEAD), jnp.float32),
            pltpu.VMEM((2, SIDE, HEAD, span), jnp.bfloat16),
            pltpu.VMEM((2, SIDE, span, 2 * HEAD), jnp.bfloat16),
            pltpu.SemaphoreType.DMA((48,)),
        ],
        compiler_params=pltpu.CompilerParams(vmem_limit_bytes=62 << 20),
        cost_estimate=pl.CostEstimate(
            flops=10 * HEAD * pairs, bytes_accessed=8 << 20, transcendentals=pairs
        ),
        name="grads",
    )(bias, *z_parts, *x_parts, *z_stats, *x_stats)
    return outs[:4], outs[4:8], outs[8:12], outs[12:]


def weight_call(query_grads, inputs):
    cols, rows = query_grads[0].shape
    width = inputs[0].shape[1]
    own = jax.ShapeDtypeStruct((cols, width // 2), jnp.float32)
    send = jax.ShapeDtypeStruct((cols, width // 2), jnp.bfloat16)
    return pl.pallas_call(
        weight_kernel,
        out_shape=[own] + [send] * 3,
        in_specs=[ANY] * 12,
        out_specs=[VM] * 4,
        scratch_shapes=[
            pltpu.VMEM((SIDE, cols, rows), jnp.bfloat16),
            pltpu.VMEM((2, SIDE, rows, width), jnp.bfloat16),
            pltpu.SemaphoreType.DMA((12,)),
        ],
        compiler_params=pltpu.CompilerParams(vmem_limit_bytes=16 << 20),
        cost_estimate=pl.CostEstimate(
            flops=16 * rows * width * cols, bytes_accessed=6 << 20, transcendentals=0
        ),
        name="weight",
    )(*query_grads, *inputs)


def query_call(parts_0, parts_1):
    rows, span = parts_0[0].shape
    return pl.pallas_call(
        query_kernel,
        out_shape=[
            jax.ShapeDtypeStruct((2 * rows, span), jnp.bfloat16),
            jax.ShapeDtypeStruct((span, 2 * rows), jnp.float32),
        ],
        in_specs=[ANY] * 8,
        out_specs=[VM] * 2,
        scratch_shapes=[
            pltpu.VMEM((2, rows, span), jnp.float32),
            pltpu.VMEM((2, SIDE, rows, span), jnp.bfloat16),
            pltpu.SemaphoreType.DMA((8,)),
        ],
        compiler_params=pltpu.CompilerParams(vmem_limit_bytes=16 << 20),
        cost_estimate=pl.CostEstimate(flops=10**6, bytes_accessed=2 << 20, transcendentals=0),
        name="query_sums",
    )(*parts_0, *parts_1)


def keys_call(parts_0, parts_1):
    span, cols = parts_0[0].shape
    block = pl.BlockSpec((span // SIDE, cols), lambda n: (n, 0))
    return pl.pallas_call(
        keys_kernel,
        grid=(SIDE,),
        out_shape=[jax.ShapeDtypeStruct((span, cols), jnp.float32)] * 2,
        in_specs=[block] * 8,
        out_specs=[block] * 2,
        compiler_params=pltpu.CompilerParams(vmem_limit_bytes=16 << 20),
        cost_estimate=pl.CostEstimate(flops=10**6, bytes_accessed=4 << 20, transcendentals=0),
        name="key_sums",
    )(*parts_0, *parts_1)


def head_of(array, h):
    return array[:, h * HEAD : (h + 1) * HEAD]


def local(queries, keys, values, forget_logits, layer_input, out_grad):
    gates = jnp.broadcast_to(forget_logits.T, (SIDE * SIDE,) + forget_logits.shape[::-1])
    gates = lax.all_to_all(gates, "sp", 0, 0, tiled=True)

    for_z = jnp.concatenate(
        [head_of(queries, 0), head_of(out_grad, 0), head_of(keys, 1), head_of(values, 1)], axis=1
    )
    for_x = jnp.concatenate(
        [head_of(keys, 0), head_of(values, 0), head_of(queries, 1), head_of(out_grad, 1)], axis=1
    )
    z_parts = fetched(for_z, along_z)
    x_parts = fetched(for_x, along_x)

    def over_zy(target):
        pairs = []
        for n in range(SIDE**3 * 2):
            zxyc = (n // 32, n // 8 % SIDE, n // 2 % SIDE, n % 2)
            new_z, new_y = target(zxyc[0], zxyc[2])
            pairs.append((n, new_z % SIDE * 32 + zxyc[1] * 8 + new_y % SIDE * 2 + zxyc[3]))
        return pairs

    moved = lax.ppermute(layer_input, ("sp", "tp"), over_zy(lambda a, b: (b, a + b)))
    inputs = [moved]
    for r in range(1, SIDE):
        inputs.append(lax.ppermute(moved, "tp", [(p, (p - 2 * r) % 8) for p in range(8)]))
    for part in list(inputs):
        inputs.append(lax.ppermute(part, "tp", [(p, p ^ 1) for p in range(8)]))

    *known, bias = stats_call(gates, z_parts, x_parts)
    stats_z, stats_x = stats_call(bias, z_parts, x_parts, known)
    z_stats = fetched(stats_z, along_z)
    x_stats = fetched(stats_x, along_x)
    dq_0, dq_1, dkv_0, dkv_1 = grads_call(bias, z_parts, x_parts, z_stats, x_stats)

    def arrived(parts, axis_perm):
        return [parts[0]] + [
            lax.ppermute(parts[r], "sp", axis_perm(r)) for r in range(1, SIDE)
        ]

    dq_0, dq_1 = arrived(dq_0, along_z), arrived(dq_1, along_x)
    low, query_grad = query_call(dq_0, dq_1)
    low, dkv_0, dkv_1 = lax.optimization_barrier((low, dkv_0, dkv_1))
    low_parts = fetched(low, along_z)
    terms = weight_call(low_parts, inputs)
    terms = arrived(terms, along_x)
    weight_grad = sum(part.astype(jnp.float32) for part in terms).T
    dkv_0, dkv_1 = arrived(dkv_0, along_x), arrived(dkv_1, along_z)
    key_grad, value_grad = keys_call(dkv_0, dkv_1)
    return (query_grad, key_grad, value_grad, weight_grad)


def solution(mesh):
    placed = P("sp", "tp")

    return jax.shard_map(
        local,
        mesh=mesh,
        in_specs=(placed,) * 6,
        out_specs=(placed,) * 4,
        check_vma=False,
    )
```

```python
import functools
import math

import jax
import jax.numpy as jnp
from jax import lax
from jax.experimental import pallas as pl
from jax.experimental.pallas import tpu as pltpu
from jax.sharding import PartitionSpec as P


HEAD = 128
SIDE = 4
SCALE = HEAD ** (-0.5)
LOG2E = math.log2(math.e)
NEG_BIG = -1e30
SUB = 256


def along_z(r):
    return [(4 * z + x, 4 * ((z + r) % SIDE) + x) for z in range(SIDE) for x in range(SIDE)]


def along_x(r):
    return [(4 * z + x, 4 * z + (x + r) % SIDE) for z in range(SIDE) for x in range(SIDE)]


def fetched(array, axis_perm):
    parts = [array]
    for r in range(1, SIDE):
        parts.append(lax.ppermute(array, "sp", axis_perm(-r)))
    return parts


def dot_nt(a, b):
    return lax.dot_general(a, b, (((1,), (1,)), ((), ())), preferred_element_type=jnp.float32)


def dot_nn(a, b):
    return lax.dot_general(a, b, (((1,), (0,)), ((), ())), preferred_element_type=jnp.float32)


def copy_list(sems):
    made = []

    def begin(src, dst):
        copy = pltpu.make_async_copy(src, dst, sems.at[len(made)])
        made.append(copy)
        copy.start()
        return copy

    return begin


def wait_all(copies):
    for c in copies:
        c.wait()


def start_loads(begin, h, z_refs, x_refs, slots, qd, kv):
    cols = pl.ds(h * 2 * HEAD, 2 * HEAD)
    q_refs, k_refs = (z_refs, x_refs) if h == 0 else (x_refs, z_refs)
    copies = []
    for r, q_ref, k_ref in zip(slots, q_refs, k_refs):
        copies.append(begin(q_ref.at[:, cols], qd.at[h, r]))
        copies.append(begin(k_ref.at[:, cols], kv.at[h, r]))
    return copies


def span_at(h, keys, r):
    here = lax.axis_index("sp")
    z, x = here // SIDE, here % SIDE
    if (h == 0) != keys:
        return SIDE * ((z + r) % SIDE) + x
    return SIDE * z + (x + r) % SIDE


def gate_sums(gates, bias):
    spans, heads, width = gates.shape
    for n in range(spans):
        bias[heads * n : heads * (n + 1), :] = gates[n]
    sums = jax.nn.log_sigmoid(bias[...])
    rows = spans * heads
    lane = lax.broadcasted_iota(jnp.int32, sums.shape, 1)
    step = 1
    while step < width:
        sums = sums + jnp.where(lane >= step, pltpu.roll(sums, step, axis=1), 0.0)
        step *= 2
    shape = (rows, rows)
    mine, other = (lax.broadcasted_iota(jnp.int32, shape, d) for d in (0, 1))
    earlier = jnp.where((other < mine) & (other % heads == mine % heads), 1.0, 0.0)
    totals = jnp.broadcast_to(sums[:, width - 1 :], (rows, HEAD))
    before = jnp.dot(
        earlier, totals, preferred_element_type=jnp.float32, precision=lax.Precision.HIGHEST
    )
    bias[...] = (sums + wide(before, width)) * LOG2E


def fill_bias(bias, bcol, h):
    def one(r, _):
        row = bias[pl.ds(2 * span_at(h, True, r) + h, 1), :]
        for j in range(4):
            tile = jnp.broadcast_to(row[:, j * HEAD : (j + 1) * HEAD], (HEAD, HEAD))
            bcol[h, r, j * HEAD : (j + 1) * HEAD, :] = tile.T
        return 0

    lax.fori_loop(0, SIDE, one, 0)


def for_visible(h, qi, ki, block):
    q_span, k_span = span_at(h, False, qi), span_at(h, True, ki)

    @pl.when(k_span < q_span)
    def _():
        block(h, qi, ki, False)

    @pl.when(k_span == q_span)
    def _():
        block(h, qi, ki, True)


def visible_mask(shape, first_query):
    key_at = lax.broadcasted_iota(jnp.int32, shape, 0)
    query_at = lax.broadcasted_iota(jnp.int32, shape, 1) + first_query
    return key_at <= query_at


def wide(tile, width):
    return jnp.concatenate([tile] * (width // tile.shape[1]), axis=1)


NEAR = (0, 1, 3)


def near_slot(n):
    return n + n // 2


def near_pairs(n):
    return near_slot(n // 3), near_slot(n % 3)


def far_pairs(n):
    near = near_slot(jnp.maximum(n - SIDE, 0))
    return jnp.where(n < SIDE, 2, near), jnp.where(n < SIDE, n, 2)


def stats_kernel(slots, pair_count, pair_of, near, bias_ref, *rest):
    n_slots = len(slots)
    z_refs, x_refs = rest[:n_slots], rest[n_slots : 2 * n_slots]
    rest = rest[2 * n_slots :]
    n_scratch = 7 if near else 6
    n_outs = 3 if near else 2
    scratch, rest = rest[-n_scratch:], rest[:-n_scratch]
    outs, known = rest[-n_outs:], rest[:-n_outs]
    bias, qd, kv, bcol, stats, sems = scratch[:6]
    span = qd.shape[2]
    begin = copy_list(sems)
    bias_copy = begin(bias_ref, scratch[6] if near else bias)
    loads = []
    for h in range(2):
        loads.append(start_loads(begin, h, z_refs, x_refs, slots, qd, kv))
        if near:
            stats[h] = jnp.zeros((SIDE, 8, span), jnp.float32)
            stats[h, :, 0:1, :] = jnp.full((SIDE, 1, span), NEG_BIG, jnp.float32)
        else:
            loads[h].append(begin(known[h], stats.at[h]))

    def block(h, qi, ki, diagonal):
        for s in range(span // SUB):
            cols = slice(s * SUB, (s + 1) * SUB)
            q = qd[h, qi, cols, :HEAD]
            do = qd[h, qi, cols, HEAD:]
            seen = (s + 1) * SUB if diagonal else span
            k = kv[h, ki, :seen, :HEAD]
            v = kv[h, ki, :seen, HEAD:]
            x = dot_nt(k, q) * (SCALE * LOG2E) - wide(bcol[h, ki, :seen], SUB)
            if diagonal:
                x = jnp.where(visible_mask(x.shape, s * SUB), x, NEG_BIG)
            dp = dot_nt(v, do)
            old = stats[h, qi, 0:1, cols]
            new = jnp.maximum(old, jnp.max(x, axis=0, keepdims=True))
            p = jnp.exp2(x - new)
            shrink = jnp.exp2(old - new)
            stats[h, qi, 0:1, cols] = new
            stats[h, qi, 1:2, cols] = stats[h, qi, 1:2, cols] * shrink + jnp.sum(
                p, axis=0, keepdims=True
            )
            stats[h, qi, 2:3, cols] = stats[h, qi, 2:3, cols] * shrink + jnp.sum(
                p * dp, axis=0, keepdims=True
            )

    bias_copy.wait()
    stores = []
    if near:
        gate_sums(scratch[6], bias)
        stores.append(begin(bias, outs[2]))
    for h in range(2):
        fill_bias(bias, bcol, h)
    for h in range(2):
        wait_all(loads[h])

        def one_pair(n, _, h=h):
            qi, ki = pair_of(n)
            for_visible(h, qi, ki, block)
            return 0

        lax.fori_loop(0, pair_count, one_pair, 0)
        stores.append(begin(stats.at[h], outs[h]))
    wait_all(stores)


def grads_kernel(bias_ref, *rest):
    z_refs, x_refs = rest[:4], rest[4:8]
    stat_refs = (rest[8:12], rest[12:16])
    outs = rest[16:32]
    bias, qd, kv, bcol, parts, rows, kt, dqt, dkv, dq_send, dkv_send, sems = rest[32:]
    span = qd.shape[2]
    begin = copy_list(sems)
    bias_copy = begin(bias_ref, bias)
    loads = []
    for h in range(2):
        stat_copies = [begin(stat_refs[h][s], parts.at[h, s]) for s in range(SIDE)]
        loads.append(stat_copies + start_loads(begin, h, z_refs, x_refs, range(SIDE), qd, kv))

    def combine(h):
        for r in range(SIDE):
            found = [parts[h, s, (r - s) % SIDE] for s in range(SIDE)]
            top = functools.reduce(jnp.maximum, [p[0:1, :] for p in found])
            factors = [jnp.exp2(p[0:1, :] - top) for p in found]
            total = sum(p[1:2, :] * f for p, f in zip(found, factors))
            mixed = sum(p[2:3, :] * f for p, f in zip(found, factors))
            rows[h, r, 0:1, :] = top + jnp.log2(total)
            rows[h, r, 1:2, :] = mixed / total

    def block(h, qi, ki, diagonal):
        for s in range(span // SUB):
            cols = slice(s * SUB, (s + 1) * SUB)
            q = qd[h, qi, cols, :HEAD]
            do = qd[h, qi, cols, HEAD:]
            seen = (s + 1) * SUB if diagonal else span
            k = kv[h, ki, :seen, :HEAD]
            v = kv[h, ki, :seen, HEAD:]
            x = dot_nt(k, q) * (SCALE * LOG2E) - wide(bcol[h, ki, :seen], SUB)
            x = x - rows[h, qi, 0:1, cols]
            if diagonal:
                x = jnp.where(visible_mask(x.shape, s * SUB), x, NEG_BIG)
            p = jnp.exp2(x)
            ds = (p * (dot_nt(v, do) - rows[h, qi, 1:2, cols])).astype(jnp.bfloat16)
            dkv[h, ki, :seen, HEAD:] += dot_nn(p.astype(jnp.bfloat16), do)
            dkv[h, ki, :seen, :HEAD] += dot_nn(ds, q)
            dqt[h, qi, :, cols] += dot_nn(kt[ki, :, :seen], ds)

    dqt[...] = jnp.zeros_like(dqt)
    dkv[...] = jnp.zeros_like(dkv)
    bias_copy.wait()
    stores = []
    for h in range(2):
        fill_bias(bias, bcol, h)
    for h in range(2):
        wait_all(loads[h])
        combine(h)
        key_outs = outs[8 + SIDE * h : 8 + SIDE * (h + 1)]
        key_sources = [dkv.at[h, 0]] + [dkv_send.at[h, r] for r in range(1, SIDE)]
        key_stores = [
            pltpu.make_async_copy(source, out, sems.at[40 + SIDE * h + r])
            for r, (source, out) in enumerate(zip(key_sources, key_outs))
        ]

        def turn(r, _, h=h):
            kt[r] = kv[h, r, :, :HEAD].astype(jnp.float32).T.astype(jnp.bfloat16)
            return 0

        lax.fori_loop(0, SIDE, turn, 0)

        def one_key_span(ki, _, h=h, key_stores=key_stores):
            def one_query_span(qi, _):
                for_visible(h, qi, ki, block)
                return 0

            lax.fori_loop(0, SIDE, one_query_span, 0)
            scaled = dkv[h, ki, :, :HEAD] * SCALE
            dkv[h, ki, :, :HEAD] = scaled
            dkv_send[h, ki, :, :HEAD] = scaled.astype(jnp.bfloat16)
            dkv_send[h, ki, :, HEAD:] = dkv[h, ki, :, HEAD:].astype(jnp.bfloat16)
            for r in range(SIDE):
                pl.when(ki == r)(key_stores[r].start)
            return 0

        lax.fori_loop(0, SIDE, one_key_span, 0)
        stores += key_stores
        dqt[h, 0] = dqt[h, 0] * SCALE
        stores.append(begin(dqt.at[h, 0], outs[SIDE * h]))
        for r in range(1, SIDE):
            dq_send[h, r] = (dqt[h, r] * SCALE).astype(jnp.bfloat16)
            stores.append(begin(dq_send.at[h, r], outs[SIDE * h + r]))
    wait_all(stores)


def weight_kernel(*rest):
    dq_refs, in_refs, outs = rest[:4], rest[4:12], rest[12:16]
    dqs, inputs, sems = rest[16:]
    here, part = lax.axis_index("sp"), lax.axis_index("tp")
    z, x, y, core = here // SIDE, here % SIDE, part // 2, part % 2
    begin = copy_list(sems)
    copies = []
    for r in range(SIDE):
        of_span = (y - z + r + SIDE) % SIDE
        for other in range(2):
            held_by = core if other == 0 else 1 - core
            copies.append(begin(in_refs[SIDE * other + r], inputs.at[held_by, of_span]))
        copies.append(begin(dq_refs[r], dqs.at[(z + r) % SIDE]))
    wait_all(copies)
    width = outs[0].shape[1]
    for r in (1, 2, 3, 0):
        block = (x + r) % SIDE
        cols = pl.ds(pl.multiple_of((block % 2) * width, width), width)
        total = sum(dot_nn(dqs[a], inputs[block // 2, a, :, cols]) for a in range(SIDE))
        outs[r][...] = total.astype(outs[r].dtype)


def query_kernel(*refs):
    parts, (low_ref, grad_ref, own, sent, sems) = refs[:8], refs[8:]
    begin = copy_list(sems)
    loads = []
    for h in range(2):
        loads.append([begin(parts[SIDE * h], own.at[h])])
        loads[h] += [begin(parts[SIDE * h + r], sent.at[h, r]) for r in range(1, SIDE)]
    for h in range(2):
        wait_all(loads[h])
        total = own[h] + sum(sent[h, r].astype(jnp.float32) for r in range(1, SIDE))
        cut = slice(h * HEAD, (h + 1) * HEAD)
        low_ref[cut, :] = total.astype(jnp.bfloat16)
        grad_ref[:, cut] = total.T


def keys_kernel(*refs):
    parts, outs = refs[:8], refs[8:]
    for h in range(2):
        for n, out in enumerate(outs):
            cut = slice(n * HEAD, (n + 1) * HEAD)
            out[:, h * HEAD : (h + 1) * HEAD] = sum(
                ref[:, cut].astype(jnp.float32) for ref in parts[SIDE * h : SIDE * (h + 1)]
            )


ANY = pl.BlockSpec(memory_space=pl.ANY)
VM = pl.BlockSpec(memory_space=pltpu.VMEM)


def stats_call(bias, z_parts, x_parts, known=()):
    span = z_parts[0].shape[0]
    near = not known
    rows = 2 * SIDE * SIDE
    out_shape = [jax.ShapeDtypeStruct((SIDE, 8, span), jnp.float32)] * 2
    scratch = [
        pltpu.VMEM((rows, span), jnp.float32),
        pltpu.VMEM((2, SIDE, span, 2 * HEAD), jnp.bfloat16),
        pltpu.VMEM((2, SIDE, span, 2 * HEAD), jnp.bfloat16),
        pltpu.VMEM((2, SIDE, span, HEAD), jnp.float32),
        pltpu.VMEM((2, SIDE, 8, span), jnp.float32),
        pltpu.SemaphoreType.DMA((24,)),
    ]
    if near:
        slots, pair_count, pair_of = NEAR, 9, near_pairs
        z_parts, x_parts = ([parts[r] for r in NEAR] for parts in (z_parts, x_parts))
        out_shape.append(jax.ShapeDtypeStruct((rows, span), jnp.float32))
        scratch.append(pltpu.VMEM(bias.shape, jnp.float32))
    else:
        slots, pair_count, pair_of = range(SIDE), 7, far_pairs
    pairs = pair_count * span * span
    return pl.pallas_call(
        functools.partial(stats_kernel, slots, pair_count, pair_of, near),
        out_shape=out_shape,
        in_specs=[ANY] * (1 + 2 * len(slots) + len(known)),
        out_specs=[ANY] * len(out_shape),
        scratch_shapes=scratch,
        compiler_params=pltpu.CompilerParams(vmem_limit_bytes=62 << 20),
        cost_estimate=pl.CostEstimate(
            flops=4 * HEAD * pairs, bytes_accessed=4 << 20, transcendentals=pairs
        ),
        name="stats",
    )(bias, *z_parts, *x_parts, *known)


def grads_call(bias, z_parts, x_parts, z_stats, x_stats):
    span = z_parts[0].shape[0]
    pairs = 17 * span * span

    def shapes(*shape):
        own = jax.ShapeDtypeStruct(shape, jnp.float32)
        send = jax.ShapeDtypeStruct(shape, jnp.bfloat16)
        return ([own] + [send] * 3) * 2

    outs = pl.pallas_call(
        grads_kernel,
        out_shape=shapes(HEAD, span) + shapes(span, 2 * HEAD),
        in_specs=[ANY] * 17,
        out_specs=[ANY] * 16,
        scratch_shapes=[
            pltpu.VMEM(bias.shape, jnp.float32),
            pltpu.VMEM((2, SIDE, span, 2 * HEAD), jnp.bfloat16),
            pltpu.VMEM((2, SIDE, span, 2 * HEAD), jnp.bfloat16),
            pltpu.VMEM((2, SIDE, span, HEAD), jnp.float32),
            pltpu.VMEM((2, SIDE, SIDE, 8, span), jnp.float32),
            pltpu.VMEM((2, SIDE, 8, span), jnp.float32),
            pltpu.VMEM((SIDE, HEAD, span), jnp.bfloat16),
            pltpu.VMEM((2, SIDE, HEAD, span), jnp.float32),
            pltpu.VMEM((2, SIDE, span, 2 * HEAD), jnp.float32),
            pltpu.VMEM((2, SIDE, HEAD, span), jnp.bfloat16),
            pltpu.VMEM((2, SIDE, span, 2 * HEAD), jnp.bfloat16),
            pltpu.SemaphoreType.DMA((48,)),
        ],
        compiler_params=pltpu.CompilerParams(vmem_limit_bytes=62 << 20),
        cost_estimate=pl.CostEstimate(
            flops=10 * HEAD * pairs, bytes_accessed=8 << 20, transcendentals=pairs
        ),
        name="grads",
    )(bias, *z_parts, *x_parts, *z_stats, *x_stats)
    return outs[:4], outs[4:8], outs[8:12], outs[12:]


def weight_call(query_grads, inputs):
    cols, rows = query_grads[0].shape
    width = inputs[0].shape[1]
    own = jax.ShapeDtypeStruct((cols, width // 2), jnp.float32)
    send = jax.ShapeDtypeStruct((cols, width // 2), jnp.bfloat16)
    return pl.pallas_call(
        weight_kernel,
        out_shape=[own] + [send] * 3,
        in_specs=[ANY] * 12,
        out_specs=[VM] * 4,
        scratch_shapes=[
            pltpu.VMEM((SIDE, cols, rows), jnp.bfloat16),
            pltpu.VMEM((2, SIDE, rows, width), jnp.bfloat16),
            pltpu.SemaphoreType.DMA((12,)),
        ],
        compiler_params=pltpu.CompilerParams(vmem_limit_bytes=16 << 20),
        cost_estimate=pl.CostEstimate(
            flops=16 * rows * width * cols, bytes_accessed=6 << 20, transcendentals=0
        ),
        name="weight",
    )(*query_grads, *inputs)


def query_call(parts_0, parts_1):
    rows, span = parts_0[0].shape
    return pl.pallas_call(
        query_kernel,
        out_shape=[
            jax.ShapeDtypeStruct((2 * rows, span), jnp.bfloat16),
            jax.ShapeDtypeStruct((span, 2 * rows), jnp.float32),
        ],
        in_specs=[ANY] * 8,
        out_specs=[VM] * 2,
        scratch_shapes=[
            pltpu.VMEM((2, rows, span), jnp.float32),
            pltpu.VMEM((2, SIDE, rows, span), jnp.bfloat16),
            pltpu.SemaphoreType.DMA((8,)),
        ],
        compiler_params=pltpu.CompilerParams(vmem_limit_bytes=62 << 20),
        cost_estimate=pl.CostEstimate(flops=10**6, bytes_accessed=2 << 20, transcendentals=0),
        name="query_sums",
    )(*parts_0, *parts_1)


def keys_call(parts_0, parts_1):
    span, cols = parts_0[0].shape
    block = pl.BlockSpec((span // SIDE, cols), lambda n: (n, 0))
    return pl.pallas_call(
        keys_kernel,
        grid=(SIDE,),
        out_shape=[jax.ShapeDtypeStruct((span, cols), jnp.float32)] * 2,
        in_specs=[block] * 8,
        out_specs=[block] * 2,
        compiler_params=pltpu.CompilerParams(vmem_limit_bytes=16 << 20),
        cost_estimate=pl.CostEstimate(flops=10**6, bytes_accessed=4 << 20, transcendentals=0),
        name="key_sums",
    )(*parts_0, *parts_1)


def head_of(array, h):
    return array[:, h * HEAD : (h + 1) * HEAD]


def local(queries, keys, values, forget_logits, layer_input, out_grad):
    gates = jnp.broadcast_to(forget_logits.T, (SIDE * SIDE,) + forget_logits.shape[::-1])
    gates = lax.all_to_all(gates, "sp", 0, 0, tiled=True)

    for_z = jnp.concatenate(
        [head_of(queries, 0), head_of(out_grad, 0), head_of(keys, 1), head_of(values, 1)], axis=1
    )
    for_x = jnp.concatenate(
        [head_of(keys, 0), head_of(values, 0), head_of(queries, 1), head_of(out_grad, 1)], axis=1
    )
    z_parts = fetched(for_z, along_z)
    x_parts = fetched(for_x, along_x)

    def over_zy(target):
        pairs = []
        for n in range(SIDE**3 * 2):
            zxyc = (n // 32, n // 8 % SIDE, n // 2 % SIDE, n % 2)
            new_z, new_y = target(zxyc[0], zxyc[2])
            pairs.append((n, new_z % SIDE * 32 + zxyc[1] * 8 + new_y % SIDE * 2 + zxyc[3]))
        return pairs

    everywhere = ("sp", "tp")
    moved = lax.ppermute(layer_input, everywhere, over_zy(lambda a, b: (a, a + b)))
    moved = lax.ppermute(moved, everywhere, over_zy(lambda a, b: (b - a, b)))
    inputs = [moved]
    for r in range(1, SIDE):
        inputs.append(lax.ppermute(moved, "tp", [(p, (p - 2 * r) % 8) for p in range(8)]))
    for part in list(inputs):
        inputs.append(lax.ppermute(part, "tp", [(p, p ^ 1) for p in range(8)]))

    *known, bias = stats_call(gates, z_parts, x_parts)
    stats_z, stats_x = stats_call(bias, z_parts, x_parts, known)
    z_stats = fetched(stats_z, along_z)
    x_stats = fetched(stats_x, along_x)
    dq_0, dq_1, dkv_0, dkv_1 = grads_call(bias, z_parts, x_parts, z_stats, x_stats)

    def arrived(parts, axis_perm):
        return [parts[0]] + [
            lax.ppermute(parts[r], "sp", axis_perm(r)) for r in range(1, SIDE)
        ]

    dq_0, dq_1 = arrived(dq_0, along_z), arrived(dq_1, along_x)
    low, query_grad = query_call(dq_0, dq_1)
    low, dkv_0, dkv_1 = lax.optimization_barrier((low, dkv_0, dkv_1))
    low_parts = fetched(low, along_z)
    terms = weight_call(low_parts, inputs)
    terms = arrived(terms, along_x)
    weight_grad = sum(part.astype(jnp.float32) for part in terms).T
    dkv_0, dkv_1 = arrived(dkv_0, along_x), arrived(dkv_1, along_z)
    key_grad, value_grad = keys_call(dkv_0, dkv_1)
    return (query_grad, key_grad, value_grad, weight_grad)


def solution(mesh):
    placed = P("sp", "tp")

    return jax.shard_map(
        local,
        mesh=mesh,
        in_specs=(placed,) * 6,
        out_specs=(placed,) * 4,
        check_vma=False,
    )
```

```python
import functools
import math

import jax
import jax.numpy as jnp
from jax import lax
from jax.experimental import pallas as pl
from jax.experimental.pallas import tpu as pltpu
from jax.sharding import PartitionSpec as P


HEAD = 128
SIDE = 4
SCALE = HEAD ** (-0.5)
LOG2E = math.log2(math.e)
NEG_BIG = -1e30
SUB = 256


def along_z(r):
    return [(4 * z + x, 4 * ((z + r) % SIDE) + x) for z in range(SIDE) for x in range(SIDE)]


def along_x(r):
    return [(4 * z + x, 4 * z + (x + r) % SIDE) for z in range(SIDE) for x in range(SIDE)]


def fetched(array, axis_perm, axis="sp"):
    after, before = (lax.ppermute(array, axis, axis_perm(-r)) for r in (1, SIDE - 1))
    across = lax.ppermute(after, axis, axis_perm(-1))
    return [array, after, across, before]


def dot_nt(a, b):
    return lax.dot_general(a, b, (((1,), (1,)), ((), ())), preferred_element_type=jnp.float32)


def dot_nn(a, b):
    return lax.dot_general(a, b, (((1,), (0,)), ((), ())), preferred_element_type=jnp.float32)


def copy_list(sems):
    made = []

    def begin(src, dst):
        copy = pltpu.make_async_copy(src, dst, sems.at[len(made)])
        made.append(copy)
        copy.start()
        return copy

    return begin


def wait_all(copies):
    for c in copies:
        c.wait()


def start_loads(begin, h, z_refs, x_refs, slots, qd, kv):
    cols = pl.ds(h * 2 * HEAD, 2 * HEAD)
    q_refs, k_refs = (z_refs, x_refs) if h == 0 else (x_refs, z_refs)
    copies = []
    for r, q_ref, k_ref in zip(slots, q_refs, k_refs):
        copies.append(begin(q_ref.at[:, cols], qd.at[h, r]))
        copies.append(begin(k_ref.at[:, cols], kv.at[h, r]))
    return copies


def span_at(h, keys, r):
    here = lax.axis_index("sp")
    z, x = here // SIDE, here % SIDE
    if (h == 0) != keys:
        return SIDE * ((z + r) % SIDE) + x
    return SIDE * z + (x + r) % SIDE


def gate_sums(gates, bias):
    spans, heads, width = gates.shape
    for n in range(spans):
        bias[heads * n : heads * (n + 1), :] = gates[n]
    sums = jax.nn.log_sigmoid(bias[...])
    rows = spans * heads
    lane = lax.broadcasted_iota(jnp.int32, sums.shape, 1)
    step = 1
    while step < width:
        sums = sums + jnp.where(lane >= step, pltpu.roll(sums, step, axis=1), 0.0)
        step *= 2
    shape = (rows, rows)
    mine, other = (lax.broadcasted_iota(jnp.int32, shape, d) for d in (0, 1))
    earlier = jnp.where((other < mine) & (other % heads == mine % heads), 1.0, 0.0)
    totals = jnp.broadcast_to(sums[:, width - 1 :], (rows, HEAD))
    before = jnp.dot(
        earlier, totals, preferred_element_type=jnp.float32, precision=lax.Precision.HIGHEST
    )
    bias[...] = (sums + wide(before, width)) * LOG2E


def fill_bias(bias, bcol, h):
    def one(r, _):
        row = bias[pl.ds(2 * span_at(h, True, r) + h, 1), :]
        for j in range(4):
            tile = jnp.broadcast_to(row[:, j * HEAD : (j + 1) * HEAD], (HEAD, HEAD))
            bcol[h, r, j * HEAD : (j + 1) * HEAD, :] = tile.T
        return 0

    lax.fori_loop(0, SIDE, one, 0)


def for_visible(h, qi, ki, block):
    q_span, k_span = span_at(h, False, qi), span_at(h, True, ki)

    @pl.when(k_span < q_span)
    def _():
        block(h, qi, ki, False)

    @pl.when(k_span == q_span)
    def _():
        block(h, qi, ki, True)


def visible_mask(shape, first_query):
    key_at = lax.broadcasted_iota(jnp.int32, shape, 0)
    query_at = lax.broadcasted_iota(jnp.int32, shape, 1) + first_query
    return key_at <= query_at


def wide(tile, width):
    return jnp.concatenate([tile] * (width // tile.shape[1]), axis=1)


NEAR = (0, 1, 3)


def near_slot(n):
    return n + n // 2


def near_pairs(n):
    return near_slot(n // 3), near_slot(n % 3)


def far_pairs(n):
    near = near_slot(jnp.maximum(n - SIDE, 0))
    return jnp.where(n < SIDE, 2, near), jnp.where(n < SIDE, n, 2)


def stats_kernel(slots, pair_count, pair_of, near, bias_ref, *rest):
    n_slots = len(slots)
    z_refs, x_refs = rest[:n_slots], rest[n_slots : 2 * n_slots]
    rest = rest[2 * n_slots :]
    n_scratch = 7 if near else 6
    n_outs = 3 if near else 2
    scratch, rest = rest[-n_scratch:], rest[:-n_scratch]
    outs, known = rest[-n_outs:], rest[:-n_outs]
    bias, qd, kv, bcol, stats, sems = scratch[:6]
    span = qd.shape[2]
    begin = copy_list(sems)
    bias_copy = begin(bias_ref, scratch[6] if near else bias)
    loads = []
    for h in range(2):
        loads.append(start_loads(begin, h, z_refs, x_refs, slots, qd, kv))
        if near:
            stats[h] = jnp.zeros((SIDE, 8, span), jnp.float32)
            stats[h, :, 0:1, :] = jnp.full((SIDE, 1, span), NEG_BIG, jnp.float32)
        else:
            loads[h].append(begin(known[h], stats.at[h]))

    def block(h, qi, ki, diagonal):
        for s in range(span // SUB):
            cols = slice(s * SUB, (s + 1) * SUB)
            q = qd[h, qi, cols, :HEAD]
            do = qd[h, qi, cols, HEAD:]
            seen = (s + 1) * SUB if diagonal else span
            k = kv[h, ki, :seen, :HEAD]
            v = kv[h, ki, :seen, HEAD:]
            x = dot_nt(k, q) * (SCALE * LOG2E) - wide(bcol[h, ki, :seen], SUB)
            if diagonal:
                x = jnp.where(visible_mask(x.shape, s * SUB), x, NEG_BIG)
            dp = dot_nt(v, do)
            old = stats[h, qi, 0:1, cols]
            new = jnp.maximum(old, jnp.max(x, axis=0, keepdims=True))
            p = jnp.exp2(x - new)
            shrink = jnp.exp2(old - new)
            stats[h, qi, 0:1, cols] = new
            stats[h, qi, 1:2, cols] = stats[h, qi, 1:2, cols] * shrink + jnp.sum(
                p, axis=0, keepdims=True
            )
            stats[h, qi, 2:3, cols] = stats[h, qi, 2:3, cols] * shrink + jnp.sum(
                p * dp, axis=0, keepdims=True
            )

    bias_copy.wait()
    stores = []
    if near:
        gate_sums(scratch[6], bias)
        stores.append(begin(bias, outs[2]))
    for h in range(2):
        fill_bias(bias, bcol, h)
    for h in range(2):
        wait_all(loads[h])

        def one_pair(n, _, h=h):
            qi, ki = pair_of(n)
            for_visible(h, qi, ki, block)
            return 0

        lax.fori_loop(0, pair_count, one_pair, 0)
        stores.append(begin(stats.at[h], outs[h]))
    wait_all(stores)


def grads_kernel(bias_ref, *rest):
    z_refs, x_refs = rest[:4], rest[4:8]
    stat_refs = (rest[8:12], rest[12:16])
    outs = rest[16:32]
    bias, qd, kv, bcol, parts, rows, kt, dqt, dkv, dq_send, dkv_send, sems = rest[32:]
    span = qd.shape[2]
    begin = copy_list(sems)
    bias_copy = begin(bias_ref, bias)
    loads = []
    for h in range(2):
        stat_copies = [begin(stat_refs[h][s], parts.at[h, s]) for s in range(SIDE)]
        loads.append(stat_copies + start_loads(begin, h, z_refs, x_refs, range(SIDE), qd, kv))

    def combine(h):
        for r in range(SIDE):
            found = [parts[h, s, (r - s) % SIDE] for s in range(SIDE)]
            top = functools.reduce(jnp.maximum, [p[0:1, :] for p in found])
            factors = [jnp.exp2(p[0:1, :] - top) for p in found]
            total = sum(p[1:2, :] * f for p, f in zip(found, factors))
            mixed = sum(p[2:3, :] * f for p, f in zip(found, factors))
            rows[h, r, 0:1, :] = top + jnp.log2(total)
            rows[h, r, 1:2, :] = mixed / total

    def block(h, qi, ki, diagonal):
        for s in range(span // SUB):
            cols = slice(s * SUB, (s + 1) * SUB)
            q = qd[h, qi, cols, :HEAD]
            do = qd[h, qi, cols, HEAD:]
            seen = (s + 1) * SUB if diagonal else span
            k = kv[h, ki, :seen, :HEAD]
            v = kv[h, ki, :seen, HEAD:]
            x = dot_nt(k, q) * (SCALE * LOG2E) - wide(bcol[h, ki, :seen], SUB)
            x = x - rows[h, qi, 0:1, cols]
            if diagonal:
                x = jnp.where(visible_mask(x.shape, s * SUB), x, NEG_BIG)
            p = jnp.exp2(x)
            ds = (p * (dot_nt(v, do) - rows[h, qi, 1:2, cols])).astype(jnp.bfloat16)
            dkv[h, ki, :seen, HEAD:] += dot_nn(p.astype(jnp.bfloat16), do)
            dkv[h, ki, :seen, :HEAD] += dot_nn(ds, q)
            dqt[h, qi, :, cols] += dot_nn(kt[ki, :, :seen], ds)

    dqt[...] = jnp.zeros_like(dqt)
    dkv[...] = jnp.zeros_like(dkv)
    bias_copy.wait()
    stores = []
    for h in range(2):
        fill_bias(bias, bcol, h)
    for h in range(2):
        wait_all(loads[h])
        combine(h)
        key_outs = outs[8 + SIDE * h : 8 + SIDE * (h + 1)]
        key_sources = [dkv.at[h, 0]] + [dkv_send.at[h, r] for r in range(1, SIDE)]
        key_stores = [
            pltpu.make_async_copy(source, out, sems.at[40 + SIDE * h + r])
            for r, (source, out) in enumerate(zip(key_sources, key_outs))
        ]

        def turn(r, _, h=h):
            kt[r] = kv[h, r, :, :HEAD].astype(jnp.float32).T.astype(jnp.bfloat16)
            return 0

        lax.fori_loop(0, SIDE, turn, 0)

        def one_key_span(ki, _, h=h, key_stores=key_stores):
            def one_query_span(qi, _):
                for_visible(h, qi, ki, block)
                return 0

            lax.fori_loop(0, SIDE, one_query_span, 0)
            scaled = dkv[h, ki, :, :HEAD] * SCALE
            dkv[h, ki, :, :HEAD] = scaled
            dkv_send[h, ki, :, :HEAD] = scaled.astype(jnp.bfloat16)
            dkv_send[h, ki, :, HEAD:] = dkv[h, ki, :, HEAD:].astype(jnp.bfloat16)
            for r in range(SIDE):
                pl.when(ki == r)(key_stores[r].start)
            return 0

        lax.fori_loop(0, SIDE, one_key_span, 0)
        stores += key_stores
        dqt[h, 0] = dqt[h, 0] * SCALE
        stores.append(begin(dqt.at[h, 0], outs[SIDE * h]))
        for r in range(1, SIDE):
            dq_send[h, r] = (dqt[h, r] * SCALE).astype(jnp.bfloat16)
            stores.append(begin(dq_send.at[h, r], outs[SIDE * h + r]))
    wait_all(stores)


def weight_kernel(*rest):
    dq_refs, in_refs, outs = rest[:4], rest[4:12], rest[12:16]
    dqs, inputs, sems = rest[16:]
    here, part = lax.axis_index("sp"), lax.axis_index("tp")
    z, x, y, core = here // SIDE, here % SIDE, part // 2, part % 2
    begin = copy_list(sems)
    copies = []
    for r in range(SIDE):
        of_span = (y - z + r + SIDE) % SIDE
        for other in range(2):
            held_by = core if other == 0 else 1 - core
            copies.append(begin(in_refs[SIDE * other + r], inputs.at[held_by, of_span]))
        copies.append(begin(dq_refs[r], dqs.at[(z + r) % SIDE]))
    wait_all(copies)
    width = outs[0].shape[1]
    for r in (1, 2, 3, 0):
        block = (x + r) % SIDE
        cols = pl.ds(pl.multiple_of((block % 2) * width, width), width)
        total = sum(dot_nn(dqs[a], inputs[block // 2, a, :, cols]) for a in range(SIDE))
        outs[r][...] = total.astype(outs[r].dtype)


def query_kernel(*refs):
    parts, (low_ref, grad_ref) = refs[:8], refs[8:]
    for h in range(2):
        total = sum(ref[...].astype(jnp.float32) for ref in parts[SIDE * h : SIDE * (h + 1)])
        cut = slice(h * HEAD, (h + 1) * HEAD)
        low_ref[cut, :] = total.astype(jnp.bfloat16)
        grad_ref[:, cut] = total.T


def keys_kernel(*refs):
    parts, outs = refs[:8], refs[8:]
    for h in range(2):
        for n, out in enumerate(outs):
            cut = slice(n * HEAD, (n + 1) * HEAD)
            out[:, h * HEAD : (h + 1) * HEAD] = sum(
                ref[:, cut].astype(jnp.float32) for ref in parts[SIDE * h : SIDE * (h + 1)]
            )


ANY = pl.BlockSpec(memory_space=pl.ANY)
VM = pl.BlockSpec(memory_space=pltpu.VMEM)


def stats_call(bias, z_parts, x_parts, known=()):
    span = z_parts[0].shape[0]
    near = not known
    rows = 2 * SIDE * SIDE
    out_shape = [jax.ShapeDtypeStruct((SIDE, 8, span), jnp.float32)] * 2
    scratch = [
        pltpu.VMEM((rows, span), jnp.float32),
        pltpu.VMEM((2, SIDE, span, 2 * HEAD), jnp.bfloat16),
        pltpu.VMEM((2, SIDE, span, 2 * HEAD), jnp.bfloat16),
        pltpu.VMEM((2, SIDE, span, HEAD), jnp.float32),
        pltpu.VMEM((2, SIDE, 8, span), jnp.float32),
        pltpu.SemaphoreType.DMA((24,)),
    ]
    if near:
        slots, pair_count, pair_of = NEAR, 9, near_pairs
        z_parts, x_parts = ([parts[r] for r in NEAR] for parts in (z_parts, x_parts))
        out_shape.append(jax.ShapeDtypeStruct((rows, span), jnp.float32))
        scratch.append(pltpu.VMEM(bias.shape, jnp.float32))
    else:
        slots, pair_count, pair_of = range(SIDE), 7, far_pairs
    pairs = pair_count * span * span
    return pl.pallas_call(
        functools.partial(stats_kernel, slots, pair_count, pair_of, near),
        out_shape=out_shape,
        in_specs=[ANY] * (1 + 2 * len(slots) + len(known)),
        out_specs=[ANY] * len(out_shape),
        scratch_shapes=scratch,
        compiler_params=pltpu.CompilerParams(vmem_limit_bytes=62 << 20),
        cost_estimate=pl.CostEstimate(
            flops=4 * HEAD * pairs, bytes_accessed=4 << 20, transcendentals=pairs
        ),
        name="stats",
    )(bias, *z_parts, *x_parts, *known)


def grads_call(bias, z_parts, x_parts, z_stats, x_stats):
    span = z_parts[0].shape[0]
    pairs = 17 * span * span

    def shapes(*shape):
        own = jax.ShapeDtypeStruct(shape, jnp.float32)
        send = jax.ShapeDtypeStruct(shape, jnp.bfloat16)
        return ([own] + [send] * 3) * 2

    outs = pl.pallas_call(
        grads_kernel,
        out_shape=shapes(HEAD, span) + shapes(span, 2 * HEAD),
        in_specs=[ANY] * 17,
        out_specs=[ANY] * 16,
        scratch_shapes=[
            pltpu.VMEM(bias.shape, jnp.float32),
            pltpu.VMEM((2, SIDE, span, 2 * HEAD), jnp.bfloat16),
            pltpu.VMEM((2, SIDE, span, 2 * HEAD), jnp.bfloat16),
            pltpu.VMEM((2, SIDE, span, HEAD), jnp.float32),
            pltpu.VMEM((2, SIDE, SIDE, 8, span), jnp.float32),
            pltpu.VMEM((2, SIDE, 8, span), jnp.float32),
            pltpu.VMEM((SIDE, HEAD, span), jnp.bfloat16),
            pltpu.VMEM((2, SIDE, HEAD, span), jnp.float32),
            pltpu.VMEM((2, SIDE, span, 2 * HEAD), jnp.float32),
            pltpu.VMEM((2, SIDE, HEAD, span), jnp.bfloat16),
            pltpu.VMEM((2, SIDE, span, 2 * HEAD), jnp.bfloat16),
            pltpu.SemaphoreType.DMA((48,)),
        ],
        compiler_params=pltpu.CompilerParams(vmem_limit_bytes=62 << 20),
        cost_estimate=pl.CostEstimate(
            flops=10 * HEAD * pairs, bytes_accessed=8 << 20, transcendentals=pairs
        ),
        name="grads",
    )(bias, *z_parts, *x_parts, *z_stats, *x_stats)
    return outs[:4], outs[4:8], outs[8:12], outs[12:]


def weight_call(query_grads, inputs):
    cols, rows = query_grads[0].shape
    width = inputs[0].shape[1]
    own = jax.ShapeDtypeStruct((cols, width // 2), jnp.float32)
    send = jax.ShapeDtypeStruct((cols, width // 2), jnp.bfloat16)
    return pl.pallas_call(
        weight_kernel,
        out_shape=[own] + [send] * 3,
        in_specs=[ANY] * 12,
        out_specs=[VM] * 4,
        scratch_shapes=[
            pltpu.VMEM((SIDE, cols, rows), jnp.bfloat16),
            pltpu.VMEM((2, SIDE, rows, width), jnp.bfloat16),
            pltpu.SemaphoreType.DMA((12,)),
        ],
        compiler_params=pltpu.CompilerParams(vmem_limit_bytes=16 << 20),
        cost_estimate=pl.CostEstimate(
            flops=16 * rows * width * cols, bytes_accessed=6 << 20, transcendentals=0
        ),
        name="weight",
    )(*query_grads, *inputs)


def query_call(parts_0, parts_1):
    rows, span = parts_0[0].shape
    return pl.pallas_call(
        query_kernel,
        out_shape=[
            jax.ShapeDtypeStruct((2 * rows, span), jnp.bfloat16),
            jax.ShapeDtypeStruct((span, 2 * rows), jnp.float32),
        ],
        in_specs=[VM] * 8,
        out_specs=[VM] * 2,
        compiler_params=pltpu.CompilerParams(vmem_limit_bytes=16 << 20),
        cost_estimate=pl.CostEstimate(flops=10**6, bytes_accessed=2 << 20, transcendentals=0),
        name="query_sums",
    )(*parts_0, *parts_1)


def keys_call(parts_0, parts_1):
    span, cols = parts_0[0].shape
    block = pl.BlockSpec((span // SIDE, cols), lambda n: (n, 0))
    return pl.pallas_call(
        keys_kernel,
        grid=(SIDE,),
        out_shape=[jax.ShapeDtypeStruct((span, cols), jnp.float32)] * 2,
        in_specs=[block] * 8,
        out_specs=[block] * 2,
        compiler_params=pltpu.CompilerParams(vmem_limit_bytes=16 << 20),
        cost_estimate=pl.CostEstimate(flops=10**6, bytes_accessed=4 << 20, transcendentals=0),
        name="key_sums",
    )(*parts_0, *parts_1)


def head_of(array, h):
    return array[:, h * HEAD : (h + 1) * HEAD]


def local(queries, keys, values, forget_logits, layer_input, out_grad):
    gates = jnp.broadcast_to(forget_logits.T, (SIDE * SIDE,) + forget_logits.shape[::-1])
    gates = lax.all_to_all(gates, "sp", 0, 0, tiled=True)

    for_z = jnp.concatenate(
        [head_of(queries, 0), head_of(out_grad, 0), head_of(keys, 1), head_of(values, 1)], axis=1
    )
    for_x = jnp.concatenate(
        [head_of(keys, 0), head_of(values, 0), head_of(queries, 1), head_of(out_grad, 1)], axis=1
    )
    z_parts = fetched(for_z, along_z)
    x_parts = fetched(for_x, along_x)

    def over_zy(target):
        pairs = []
        for n in range(SIDE**3 * 2):
            zxyc = (n // 32, n // 8 % SIDE, n // 2 % SIDE, n % 2)
            new_z, new_y = target(zxyc[0], zxyc[2])
            pairs.append((n, new_z % SIDE * 32 + zxyc[1] * 8 + new_y % SIDE * 2 + zxyc[3]))
        return pairs

    everywhere = ("sp", "tp")
    moved = lax.ppermute(layer_input, everywhere, over_zy(lambda a, b: (a, a + b)))
    moved = lax.ppermute(moved, everywhere, over_zy(lambda a, b: (b - a, b)))
    inputs = fetched(moved, lambda r: [(p, (p + 2 * r) % 8) for p in range(8)], "tp")
    for part in list(inputs):
        inputs.append(lax.ppermute(part, "tp", [(p, p ^ 1) for p in range(8)]))

    *known, bias = stats_call(gates, z_parts, x_parts)
    stats_z, stats_x = stats_call(bias, z_parts, x_parts, known)
    z_stats = fetched(stats_z, along_z)
    x_stats = fetched(stats_x, along_x)
    dq_0, dq_1, dkv_0, dkv_1 = grads_call(bias, z_parts, x_parts, z_stats, x_stats)

    def arrived(parts, axis_perm):
        return [parts[0]] + [
            lax.ppermute(parts[r], "sp", axis_perm(r)) for r in range(1, SIDE)
        ]

    dq_0, dq_1 = arrived(dq_0, along_z), arrived(dq_1, along_x)
    low, query_grad = query_call(dq_0, dq_1)
    low, dkv_0, dkv_1 = lax.optimization_barrier((low, dkv_0, dkv_1))
    low_parts = fetched(low, along_z)
    terms = weight_call(low_parts, inputs)
    terms = arrived(terms, along_x)
    weight_grad = sum(part.astype(jnp.float32) for part in terms).T
    dkv_0 = arrived(dkv_0, along_x)
    dkv_1 = arrived(dkv_1, along_z)
    key_grad, value_grad = keys_call(dkv_0, dkv_1)
    return (query_grad, key_grad, value_grad, weight_grad)


def solution(mesh):
    placed = P("sp", "tp")

    return jax.shard_map(
        local,
        mesh=mesh,
        in_specs=(placed,) * 6,
        out_specs=(placed,) * 4,
        check_vma=False,
    )
```

```python
import functools
import math

import jax
import jax.numpy as jnp
from jax import lax
from jax.experimental import pallas as pl
from jax.experimental.pallas import tpu as pltpu
from jax.sharding import PartitionSpec as P


HEAD = 128
SIDE = 4
SCALE = HEAD ** (-0.5)
LOG2E = math.log2(math.e)
NEG_BIG = -1e30
SUB = 256


def along_z(r):
    return [(4 * z + x, 4 * ((z + r) % SIDE) + x) for z in range(SIDE) for x in range(SIDE)]


def along_x(r):
    return [(4 * z + x, 4 * z + (x + r) % SIDE) for z in range(SIDE) for x in range(SIDE)]


def fetched(array, axis_perm, axis="sp"):
    after, before = (lax.ppermute(array, axis, axis_perm(-r)) for r in (1, SIDE - 1))
    across = lax.ppermute(after, axis, axis_perm(-1))
    return [array, after, across, before]


def fetched_direct(array, axis_perm):
    return [array] + [lax.ppermute(array, "sp", axis_perm(-r)) for r in range(1, SIDE)]


def dot_nt(a, b):
    return lax.dot_general(a, b, (((1,), (1,)), ((), ())), preferred_element_type=jnp.float32)


def dot_nn(a, b):
    return lax.dot_general(a, b, (((1,), (0,)), ((), ())), preferred_element_type=jnp.float32)


def copy_list(sems):
    made = []

    def begin(src, dst):
        copy = pltpu.make_async_copy(src, dst, sems.at[len(made)])
        made.append(copy)
        copy.start()
        return copy

    return begin


def wait_all(copies):
    for c in copies:
        c.wait()


def start_loads(begin, h, z_refs, x_refs, slots, qd, kv):
    cols = pl.ds(h * 2 * HEAD, 2 * HEAD)
    q_refs, k_refs = (z_refs, x_refs) if h == 0 else (x_refs, z_refs)
    copies = []
    for r, q_ref, k_ref in zip(slots, q_refs, k_refs):
        copies.append(begin(q_ref.at[:, cols], qd.at[h, r]))
        copies.append(begin(k_ref.at[:, cols], kv.at[h, r]))
    return copies


def span_at(h, keys, r):
    here = lax.axis_index("sp")
    z, x = here // SIDE, here % SIDE
    if (h == 0) != keys:
        return SIDE * ((z + r) % SIDE) + x
    return SIDE * z + (x + r) % SIDE


def gate_sums(gates, bias):
    spans, heads, width = gates.shape
    for n in range(spans):
        bias[heads * n : heads * (n + 1), :] = gates[n]
    sums = jax.nn.log_sigmoid(bias[...])
    rows = spans * heads
    lane = lax.broadcasted_iota(jnp.int32, sums.shape, 1)
    step = 1
    while step < width:
        sums = sums + jnp.where(lane >= step, pltpu.roll(sums, step, axis=1), 0.0)
        step *= 2
    shape = (rows, rows)
    mine, other = (lax.broadcasted_iota(jnp.int32, shape, d) for d in (0, 1))
    earlier = jnp.where((other < mine) & (other % heads == mine % heads), 1.0, 0.0)
    totals = jnp.broadcast_to(sums[:, width - 1 :], (rows, HEAD))
    before = jnp.dot(
        earlier, totals, preferred_element_type=jnp.float32, precision=lax.Precision.HIGHEST
    )
    bias[...] = (sums + wide(before, width)) * LOG2E


def fill_bias(bias, bcol, h):
    def one(r, _):
        row = bias[pl.ds(2 * span_at(h, True, r) + h, 1), :]
        for j in range(4):
            tile = jnp.broadcast_to(row[:, j * HEAD : (j + 1) * HEAD], (HEAD, HEAD))
            bcol[h, r, j * HEAD : (j + 1) * HEAD, :] = tile.T
        return 0

    lax.fori_loop(0, SIDE, one, 0)


def for_visible(h, qi, ki, block):
    q_span, k_span = span_at(h, False, qi), span_at(h, True, ki)

    @pl.when(k_span < q_span)
    def _():
        block(h, qi, ki, False)

    @pl.when(k_span == q_span)
    def _():
        block(h, qi, ki, True)


def visible_mask(shape, first_query):
    key_at = lax.broadcasted_iota(jnp.int32, shape, 0)
    query_at = lax.broadcasted_iota(jnp.int32, shape, 1) + first_query
    return key_at <= query_at


def wide(tile, width):
    return jnp.concatenate([tile] * (width // tile.shape[1]), axis=1)


NEAR = (0, 1, 3)


def near_slot(n):
    return n + n // 2


def near_pairs(n):
    return near_slot(n // 3), near_slot(n % 3)


def far_pairs(n):
    near = near_slot(jnp.maximum(n - SIDE, 0))
    return jnp.where(n < SIDE, 2, near), jnp.where(n < SIDE, n, 2)


def stats_kernel(slots, pair_count, pair_of, near, bias_ref, *rest):
    n_slots = len(slots)
    z_refs, x_refs = rest[:n_slots], rest[n_slots : 2 * n_slots]
    rest = rest[2 * n_slots :]
    n_scratch = 7 if near else 6
    n_outs = 3 if near else 2
    scratch, rest = rest[-n_scratch:], rest[:-n_scratch]
    outs, known = rest[-n_outs:], rest[:-n_outs]
    bias, qd, kv, bcol, stats, sems = scratch[:6]
    span = qd.shape[2]
    begin = copy_list(sems)
    bias_copy = begin(bias_ref, scratch[6] if near else bias)
    loads = []
    for h in range(2):
        loads.append(start_loads(begin, h, z_refs, x_refs, slots, qd, kv))
        if near:
            stats[h] = jnp.zeros((SIDE, 8, span), jnp.float32)
            stats[h, :, 0:1, :] = jnp.full((SIDE, 1, span), NEG_BIG, jnp.float32)
        else:
            loads[h].append(begin(known[h], stats.at[h]))

    def block(h, qi, ki, diagonal):
        for s in range(span // SUB):
            cols = slice(s * SUB, (s + 1) * SUB)
            q = qd[h, qi, cols, :HEAD]
            do = qd[h, qi, cols, HEAD:]
            seen = (s + 1) * SUB if diagonal else span
            k = kv[h, ki, :seen, :HEAD]
            v = kv[h, ki, :seen, HEAD:]
            x = dot_nt(k, q) * (SCALE * LOG2E) - wide(bcol[h, ki, :seen], SUB)
            if diagonal:
                x = jnp.where(visible_mask(x.shape, s * SUB), x, NEG_BIG)
            dp = dot_nt(v, do)
            old = stats[h, qi, 0:1, cols]
            new = jnp.maximum(old, jnp.max(x, axis=0, keepdims=True))
            p = jnp.exp2(x - new)
            shrink = jnp.exp2(old - new)
            stats[h, qi, 0:1, cols] = new
            stats[h, qi, 1:2, cols] = stats[h, qi, 1:2, cols] * shrink + jnp.sum(
                p, axis=0, keepdims=True
            )
            stats[h, qi, 2:3, cols] = stats[h, qi, 2:3, cols] * shrink + jnp.sum(
                p * dp, axis=0, keepdims=True
            )

    bias_copy.wait()
    stores = []
    if near:
        gate_sums(scratch[6], bias)
        stores.append(begin(bias, outs[2]))
    for h in range(2):
        fill_bias(bias, bcol, h)
    for h in range(2):
        wait_all(loads[h])

        def one_pair(n, _, h=h):
            qi, ki = pair_of(n)
            for_visible(h, qi, ki, block)
            return 0

        lax.fori_loop(0, pair_count, one_pair, 0)
        stores.append(begin(stats.at[h], outs[h]))
    wait_all(stores)


def grads_kernel(bias_ref, *rest):
    z_refs, x_refs = rest[:4], rest[4:8]
    stat_refs = (rest[8:12], rest[12:16])
    outs = rest[16:32]
    bias, qd, kv, bcol, parts, rows, kt, dqt, dkv, dq_send, dkv_send, sems = rest[32:]
    span = qd.shape[2]
    begin = copy_list(sems)
    bias_copy = begin(bias_ref, bias)
    loads = []
    for h in range(2):
        stat_copies = [begin(stat_refs[h][s], parts.at[h, s]) for s in range(SIDE)]
        loads.append(stat_copies + start_loads(begin, h, z_refs, x_refs, range(SIDE), qd, kv))

    def combine(h):
        for r in range(SIDE):
            found = [parts[h, s, (r - s) % SIDE] for s in range(SIDE)]
            top = functools.reduce(jnp.maximum, [p[0:1, :] for p in found])
            factors = [jnp.exp2(p[0:1, :] - top) for p in found]
            total = sum(p[1:2, :] * f for p, f in zip(found, factors))
            mixed = sum(p[2:3, :] * f for p, f in zip(found, factors))
            rows[h, r, 0:1, :] = top + jnp.log2(total)
            rows[h, r, 1:2, :] = mixed / total

    def block(h, qi, ki, diagonal):
        for s in range(span // SUB):
            cols = slice(s * SUB, (s + 1) * SUB)
            q = qd[h, qi, cols, :HEAD]
            do = qd[h, qi, cols, HEAD:]
            seen = (s + 1) * SUB if diagonal else span
            k = kv[h, ki, :seen, :HEAD]
            v = kv[h, ki, :seen, HEAD:]
            x = dot_nt(k, q) * (SCALE * LOG2E) - wide(bcol[h, ki, :seen], SUB)
            x = x - rows[h, qi, 0:1, cols]
            if diagonal:
                x = jnp.where(visible_mask(x.shape, s * SUB), x, NEG_BIG)
            p = jnp.exp2(x)
            ds = (p * (dot_nt(v, do) - rows[h, qi, 1:2, cols])).astype(jnp.bfloat16)
            dkv[h, ki, :seen, HEAD:] += dot_nn(p.astype(jnp.bfloat16), do)
            dkv[h, ki, :seen, :HEAD] += dot_nn(ds, q)
            dqt[h, qi, :, cols] += dot_nn(kt[ki, :, :seen], ds)

    dqt[...] = jnp.zeros_like(dqt)
    dkv[...] = jnp.zeros_like(dkv)
    bias_copy.wait()
    stores = []
    for h in range(2):
        fill_bias(bias, bcol, h)
    for h in range(2):
        wait_all(loads[h])
        combine(h)
        key_outs = outs[8 + SIDE * h : 8 + SIDE * (h + 1)]
        key_sources = [dkv.at[h, 0]] + [dkv_send.at[h, r] for r in range(1, SIDE)]
        key_stores = [
            pltpu.make_async_copy(source, out, sems.at[40 + SIDE * h + r])
            for r, (source, out) in enumerate(zip(key_sources, key_outs))
        ]

        def turn(r, _, h=h):
            kt[r] = kv[h, r, :, :HEAD].astype(jnp.float32).T.astype(jnp.bfloat16)
            return 0

        lax.fori_loop(0, SIDE, turn, 0)

        def one_key_span(ki, _, h=h, key_stores=key_stores):
            def one_query_span(qi, _):
                for_visible(h, qi, ki, block)
                return 0

            lax.fori_loop(0, SIDE, one_query_span, 0)
            scaled = dkv[h, ki, :, :HEAD] * SCALE
            dkv[h, ki, :, :HEAD] = scaled
            dkv_send[h, ki, :, :HEAD] = scaled.astype(jnp.bfloat16)
            dkv_send[h, ki, :, HEAD:] = dkv[h, ki, :, HEAD:].astype(jnp.bfloat16)
            for r in range(SIDE):
                pl.when(ki == r)(key_stores[r].start)
            return 0

        lax.fori_loop(0, SIDE, one_key_span, 0)
        stores += key_stores
        dqt[h, 0] = dqt[h, 0] * SCALE
        stores.append(begin(dqt.at[h, 0], outs[SIDE * h]))
        for r in range(1, SIDE):
            dq_send[h, r] = (dqt[h, r] * SCALE).astype(jnp.bfloat16)
            stores.append(begin(dq_send.at[h, r], outs[SIDE * h + r]))
    wait_all(stores)


def weight_kernel(*rest):
    dq_refs, in_refs, outs = rest[:4], rest[4:12], rest[12:16]
    dqs, inputs, sems = rest[16:]
    here, part = lax.axis_index("sp"), lax.axis_index("tp")
    z, x, y, core = here // SIDE, here % SIDE, part // 2, part % 2
    begin = copy_list(sems)
    copies = []
    for r in range(SIDE):
        of_span = (y - z + r + SIDE) % SIDE
        for other in range(2):
            held_by = core if other == 0 else 1 - core
            copies.append(begin(in_refs[SIDE * other + r], inputs.at[held_by, of_span]))
        copies.append(begin(dq_refs[r], dqs.at[(z + r) % SIDE]))
    wait_all(copies)
    width = outs[0].shape[1]
    for r in (1, 2, 3, 0):
        block = (x + r) % SIDE
        cols = pl.ds(pl.multiple_of((block % 2) * width, width), width)
        total = sum(dot_nn(dqs[a], inputs[block // 2, a, :, cols]) for a in range(SIDE))
        outs[r][...] = total.astype(outs[r].dtype)


def query_kernel(*refs):
    parts, (low_ref, grad_ref, own, sems) = refs[:8], refs[8:]
    begin = copy_list(sems)
    wait_all([begin(parts[SIDE * h], own.at[h]) for h in range(2)])
    for h in range(2):
        total = own[h]
        for ref in parts[SIDE * h + 1 : SIDE * (h + 1)]:
            total = total + ref[...].astype(jnp.float32)
        cut = slice(h * HEAD, (h + 1) * HEAD)
        low_ref[cut, :] = total.astype(jnp.bfloat16)
        grad_ref[:, cut] = total.T


def keys_kernel(*refs):
    parts, outs = refs[:8], refs[8:]
    for h in range(2):
        for n, out in enumerate(outs):
            cut = slice(n * HEAD, (n + 1) * HEAD)
            out[:, h * HEAD : (h + 1) * HEAD] = sum(
                ref[:, cut].astype(jnp.float32) for ref in parts[SIDE * h : SIDE * (h + 1)]
            )


ANY = pl.BlockSpec(memory_space=pl.ANY)
VM = pl.BlockSpec(memory_space=pltpu.VMEM)


def stats_call(bias, z_parts, x_parts, known=()):
    span = z_parts[0].shape[0]
    near = not known
    rows = 2 * SIDE * SIDE
    out_shape = [jax.ShapeDtypeStruct((SIDE, 8, span), jnp.float32)] * 2
    scratch = [
        pltpu.VMEM((rows, span), jnp.float32),
        pltpu.VMEM((2, SIDE, span, 2 * HEAD), jnp.bfloat16),
        pltpu.VMEM((2, SIDE, span, 2 * HEAD), jnp.bfloat16),
        pltpu.VMEM((2, SIDE, span, HEAD), jnp.float32),
        pltpu.VMEM((2, SIDE, 8, span), jnp.float32),
        pltpu.SemaphoreType.DMA((24,)),
    ]
    if near:
        slots, pair_count, pair_of = NEAR, 9, near_pairs
        z_parts, x_parts = ([parts[r] for r in NEAR] for parts in (z_parts, x_parts))
        out_shape.append(jax.ShapeDtypeStruct((rows, span), jnp.float32))
        scratch.append(pltpu.VMEM(bias.shape, jnp.float32))
    else:
        slots, pair_count, pair_of = range(SIDE), 7, far_pairs
    pairs = pair_count * span * span
    return pl.pallas_call(
        functools.partial(stats_kernel, slots, pair_count, pair_of, near),
        out_shape=out_shape,
        in_specs=[ANY] * (1 + 2 * len(slots) + len(known)),
        out_specs=[ANY] * len(out_shape),
        scratch_shapes=scratch,
        compiler_params=pltpu.CompilerParams(vmem_limit_bytes=62 << 20),
        cost_estimate=pl.CostEstimate(
            flops=4 * HEAD * pairs, bytes_accessed=4 << 20, transcendentals=pairs
        ),
        name="stats",
    )(bias, *z_parts, *x_parts, *known)


def grads_call(bias, z_parts, x_parts, z_stats, x_stats):
    span = z_parts[0].shape[0]
    pairs = 17 * span * span

    def shapes(*shape):
        own = jax.ShapeDtypeStruct(shape, jnp.float32)
        send = jax.ShapeDtypeStruct(shape, jnp.bfloat16)
        return ([own] + [send] * 3) * 2

    outs = pl.pallas_call(
        grads_kernel,
        out_shape=shapes(HEAD, span) + shapes(span, 2 * HEAD),
        in_specs=[ANY] * 17,
        out_specs=[ANY] * 16,
        scratch_shapes=[
            pltpu.VMEM(bias.shape, jnp.float32),
            pltpu.VMEM((2, SIDE, span, 2 * HEAD), jnp.bfloat16),
            pltpu.VMEM((2, SIDE, span, 2 * HEAD), jnp.bfloat16),
            pltpu.VMEM((2, SIDE, span, HEAD), jnp.float32),
            pltpu.VMEM((2, SIDE, SIDE, 8, span), jnp.float32),
            pltpu.VMEM((2, SIDE, 8, span), jnp.float32),
            pltpu.VMEM((SIDE, HEAD, span), jnp.bfloat16),
            pltpu.VMEM((2, SIDE, HEAD, span), jnp.float32),
            pltpu.VMEM((2, SIDE, span, 2 * HEAD), jnp.float32),
            pltpu.VMEM((2, SIDE, HEAD, span), jnp.bfloat16),
            pltpu.VMEM((2, SIDE, span, 2 * HEAD), jnp.bfloat16),
            pltpu.SemaphoreType.DMA((48,)),
        ],
        compiler_params=pltpu.CompilerParams(vmem_limit_bytes=62 << 20),
        cost_estimate=pl.CostEstimate(
            flops=10 * HEAD * pairs, bytes_accessed=8 << 20, transcendentals=pairs
        ),
        name="grads",
    )(bias, *z_parts, *x_parts, *z_stats, *x_stats)
    return outs[:4], outs[4:8], outs[8:12], outs[12:]


def weight_call(query_grads, inputs):
    cols, rows = query_grads[0].shape
    width = inputs[0].shape[1]
    own = jax.ShapeDtypeStruct((cols, width // 2), jnp.float32)
    send = jax.ShapeDtypeStruct((cols, width // 2), jnp.bfloat16)
    return pl.pallas_call(
        weight_kernel,
        out_shape=[own] + [send] * 3,
        in_specs=[ANY] * 12,
        out_specs=[VM] * 4,
        scratch_shapes=[
            pltpu.VMEM((SIDE, cols, rows), jnp.bfloat16),
            pltpu.VMEM((2, SIDE, rows, width), jnp.bfloat16),
            pltpu.SemaphoreType.DMA((12,)),
        ],
        compiler_params=pltpu.CompilerParams(vmem_limit_bytes=16 << 20),
        cost_estimate=pl.CostEstimate(
            flops=16 * rows * width * cols, bytes_accessed=6 << 20, transcendentals=0
        ),
        name="weight",
    )(*query_grads, *inputs)


def query_call(parts_0, parts_1):
    rows, span = parts_0[0].shape
    return pl.pallas_call(
        query_kernel,
        out_shape=[
            jax.ShapeDtypeStruct((2 * rows, span), jnp.bfloat16),
            jax.ShapeDtypeStruct((span, 2 * rows), jnp.float32),
        ],
        in_specs=[ANY, VM, VM, VM] * 2,
        out_specs=[VM] * 2,
        scratch_shapes=[
            pltpu.VMEM((2, rows, span), jnp.float32),
            pltpu.SemaphoreType.DMA((2,)),
        ],
        compiler_params=pltpu.CompilerParams(vmem_limit_bytes=16 << 20),
        cost_estimate=pl.CostEstimate(flops=10**6, bytes_accessed=2 << 20, transcendentals=0),
        name="query_sums",
    )(*parts_0, *parts_1)


def keys_call(parts_0, parts_1):
    span, cols = parts_0[0].shape
    block = pl.BlockSpec((span // SIDE, cols), lambda n: (n, 0))
    return pl.pallas_call(
        keys_kernel,
        grid=(SIDE,),
        out_shape=[jax.ShapeDtypeStruct((span, cols), jnp.float32)] * 2,
        in_specs=[block] * 8,
        out_specs=[block] * 2,
        compiler_params=pltpu.CompilerParams(vmem_limit_bytes=16 << 20),
        cost_estimate=pl.CostEstimate(flops=10**6, bytes_accessed=4 << 20, transcendentals=0),
        name="key_sums",
    )(*parts_0, *parts_1)


def head_of(array, h):
    return array[:, h * HEAD : (h + 1) * HEAD]


def local(queries, keys, values, forget_logits, layer_input, out_grad):
    gates = jnp.broadcast_to(forget_logits.T, (SIDE * SIDE,) + forget_logits.shape[::-1])
    gates = lax.all_to_all(gates, "sp", 0, 0, tiled=True)

    for_z = jnp.concatenate(
        [head_of(queries, 0), head_of(out_grad, 0), head_of(keys, 1), head_of(values, 1)], axis=1
    )
    for_x = jnp.concatenate(
        [head_of(keys, 0), head_of(values, 0), head_of(queries, 1), head_of(out_grad, 1)], axis=1
    )
    z_parts = fetched(for_z, along_z)
    x_parts = fetched(for_x, along_x)

    def over_zy(target):
        pairs = []
        for n in range(SIDE**3 * 2):
            zxyc = (n // 32, n // 8 % SIDE, n // 2 % SIDE, n % 2)
            new_z, new_y = target(zxyc[0], zxyc[2])
            pairs.append((n, new_z % SIDE * 32 + zxyc[1] * 8 + new_y % SIDE * 2 + zxyc[3]))
        return pairs

    everywhere = ("sp", "tp")
    moved = lax.ppermute(layer_input, everywhere, over_zy(lambda a, b: (a, a + b)))
    moved = lax.ppermute(moved, everywhere, over_zy(lambda a, b: (b - a, b)))
    inputs = fetched(moved, lambda r: [(p, (p + 2 * r) % 8) for p in range(8)], "tp")
    for part in list(inputs):
        inputs.append(lax.ppermute(part, "tp", [(p, p ^ 1) for p in range(8)]))

    *known, bias = stats_call(gates, z_parts, x_parts)
    stats_z, stats_x = stats_call(bias, z_parts, x_parts, known)
    z_stats = fetched(stats_z, along_z)
    x_stats = fetched(stats_x, along_x)
    dq_0, dq_1, dkv_0, dkv_1 = grads_call(bias, z_parts, x_parts, z_stats, x_stats)

    def arrived(parts, axis_perm):
        return [parts[0]] + [
            lax.ppermute(parts[r], "sp", axis_perm(r)) for r in range(1, SIDE)
        ]

    dq_0, dq_1 = arrived(dq_0, along_z), arrived(dq_1, along_x)
    low, query_grad = query_call(dq_0, dq_1)
    low, dkv_0, dkv_1 = lax.optimization_barrier((low, dkv_0, dkv_1))
    low_parts = fetched_direct(low, along_z)
    terms = weight_call(low_parts, inputs)
    terms = arrived(terms, along_x)
    weight_grad = sum(part.astype(jnp.float32) for part in terms).T
    dkv_0 = arrived(dkv_0, along_x)
    dkv_1 = arrived(dkv_1, along_z)
    key_grad, value_grad = keys_call(dkv_0, dkv_1)
    return (query_grad, key_grad, value_grad, weight_grad)


def solution(mesh):
    placed = P("sp", "tp")

    return jax.shard_map(
        local,
        mesh=mesh,
        in_specs=(placed,) * 6,
        out_specs=(placed,) * 4,
        check_vma=False,
    )
```

```python
import functools
import math

import jax
import jax.numpy as jnp
from jax import lax
from jax.experimental import pallas as pl
from jax.experimental.pallas import tpu as pltpu
from jax.sharding import PartitionSpec as P


HEAD = 128
SIDE = 4
SCALE = HEAD ** (-0.5)
LOG2E = math.log2(math.e)
NEG_BIG = -1e30
SUB = 256


def along_z(r):
    return [(4 * z + x, 4 * ((z + r) % SIDE) + x) for z in range(SIDE) for x in range(SIDE)]


def along_x(r):
    return [(4 * z + x, 4 * z + (x + r) % SIDE) for z in range(SIDE) for x in range(SIDE)]


def fetched(array, axis_perm, axis="sp"):
    after, before = (lax.ppermute(array, axis, axis_perm(-r)) for r in (1, SIDE - 1))
    across = lax.ppermute(after, axis, axis_perm(-1))
    return [array, after, across, before]


def fetched_direct(array, axis_perm):
    return [array] + [lax.ppermute(array, "sp", axis_perm(-r)) for r in range(1, SIDE)]


def dot_nt(a, b):
    return lax.dot_general(a, b, (((1,), (1,)), ((), ())), preferred_element_type=jnp.float32)


def dot_nn(a, b):
    return lax.dot_general(a, b, (((1,), (0,)), ((), ())), preferred_element_type=jnp.float32)


def copy_list(sems):
    made = []

    def begin(src, dst):
        copy = pltpu.make_async_copy(src, dst, sems.at[len(made)])
        made.append(copy)
        copy.start()
        return copy

    return begin


def wait_all(copies):
    for c in copies:
        c.wait()


def start_loads(begin, h, z_refs, x_refs, slots, qd, kv):
    cols = pl.ds(h * 2 * HEAD, 2 * HEAD)
    q_refs, k_refs = (z_refs, x_refs) if h == 0 else (x_refs, z_refs)
    copies = []
    for r, q_ref, k_ref in zip(slots, q_refs, k_refs):
        copies.append(begin(q_ref.at[:, cols], qd.at[h, r]))
        copies.append(begin(k_ref.at[:, cols], kv.at[h, r]))
    return copies


def span_at(h, keys, r):
    here = lax.axis_index("sp")
    z, x = here // SIDE, here % SIDE
    if (h == 0) != keys:
        return SIDE * ((z + r) % SIDE) + x
    return SIDE * z + (x + r) % SIDE


def gate_sums(gates, bias):
    spans, heads, width = gates.shape
    for n in range(spans):
        bias[heads * n : heads * (n + 1), :] = gates[n]
    sums = jax.nn.log_sigmoid(bias[...])
    rows = spans * heads
    lane = lax.broadcasted_iota(jnp.int32, sums.shape, 1)
    step = 1
    while step < width:
        sums = sums + jnp.where(lane >= step, pltpu.roll(sums, step, axis=1), 0.0)
        step *= 2
    shape = (rows, rows)
    mine, other = (lax.broadcasted_iota(jnp.int32, shape, d) for d in (0, 1))
    earlier = jnp.where((other < mine) & (other % heads == mine % heads), 1.0, 0.0)
    totals = jnp.broadcast_to(sums[:, width - 1 :], (rows, HEAD))
    before = jnp.dot(
        earlier, totals, preferred_element_type=jnp.float32, precision=lax.Precision.HIGHEST
    )
    bias[...] = (sums + wide(before, width)) * LOG2E


def fill_bias(bias, bcol, h):
    def one(r, _):
        row = bias[pl.ds(2 * span_at(h, True, r) + h, 1), :]
        for j in range(4):
            tile = jnp.broadcast_to(row[:, j * HEAD : (j + 1) * HEAD], (HEAD, HEAD))
            bcol[h, r, j * HEAD : (j + 1) * HEAD, :] = tile.T
        return 0

    lax.fori_loop(0, SIDE, one, 0)


def for_visible(h, qi, ki, block):
    q_span, k_span = span_at(h, False, qi), span_at(h, True, ki)

    @pl.when(k_span < q_span)
    def _():
        block(h, qi, ki, False)

    @pl.when(k_span == q_span)
    def _():
        block(h, qi, ki, True)


def visible_mask(shape, first_query):
    key_at = lax.broadcasted_iota(jnp.int32, shape, 0)
    query_at = lax.broadcasted_iota(jnp.int32, shape, 1) + first_query
    return key_at <= query_at


def wide(tile, width):
    return jnp.concatenate([tile] * (width // tile.shape[1]), axis=1)


NEAR = (0, 1, 3)


def near_slot(n):
    return n + n // 2


def near_pairs(n):
    return near_slot(n // 3), near_slot(n % 3)


def far_pairs(n):
    near = near_slot(jnp.maximum(n - SIDE, 0))
    return jnp.where(n < SIDE, 2, near), jnp.where(n < SIDE, n, 2)


def stats_kernel(slots, pair_count, pair_of, near, bias_ref, *rest):
    n_slots = len(slots)
    z_refs, x_refs = rest[:n_slots], rest[n_slots : 2 * n_slots]
    rest = rest[2 * n_slots :]
    n_scratch = 7 if near else 6
    n_outs = 3 if near else 2
    scratch, rest = rest[-n_scratch:], rest[:-n_scratch]
    outs, known = rest[-n_outs:], rest[:-n_outs]
    bias, qd, kv, bcol, stats, sems = scratch[:6]
    span = qd.shape[2]
    begin = copy_list(sems)
    bias_copy = begin(bias_ref, scratch[6] if near else bias)
    loads = []
    for h in range(2):
        loads.append(start_loads(begin, h, z_refs, x_refs, slots, qd, kv))
        if near:
            stats[h] = jnp.zeros((SIDE, 8, span), jnp.float32)
            stats[h, :, 0:1, :] = jnp.full((SIDE, 1, span), NEG_BIG, jnp.float32)
        else:
            loads[h].append(begin(known[h], stats.at[h]))

    def block(h, qi, ki, diagonal):
        for s in range(span // SUB):
            cols = slice(s * SUB, (s + 1) * SUB)
            q = qd[h, qi, cols, :HEAD]
            do = qd[h, qi, cols, HEAD:]
            seen = (s + 1) * SUB if diagonal else span
            k = kv[h, ki, :seen, :HEAD]
            v = kv[h, ki, :seen, HEAD:]
            x = dot_nt(k, q) * (SCALE * LOG2E) - wide(bcol[h, ki, :seen], SUB)
            if diagonal:
                x = jnp.where(visible_mask(x.shape, s * SUB), x, NEG_BIG)
            dp = dot_nt(v, do)
            old = stats[h, qi, 0:1, cols]
            new = jnp.maximum(old, jnp.max(x, axis=0, keepdims=True))
            p = jnp.exp2(x - new)
            shrink = jnp.exp2(old - new)
            stats[h, qi, 0:1, cols] = new
            stats[h, qi, 1:2, cols] = stats[h, qi, 1:2, cols] * shrink + jnp.sum(
                p, axis=0, keepdims=True
            )
            stats[h, qi, 2:3, cols] = stats[h, qi, 2:3, cols] * shrink + jnp.sum(
                p * dp, axis=0, keepdims=True
            )

    bias_copy.wait()
    stores = []
    if near:
        gate_sums(scratch[6], bias)
        stores.append(begin(bias, outs[2]))
    for h in range(2):
        fill_bias(bias, bcol, h)
    for h in range(2):
        wait_all(loads[h])

        def one_pair(n, _, h=h):
            qi, ki = pair_of(n)
            for_visible(h, qi, ki, block)
            return 0

        lax.fori_loop(0, pair_count, one_pair, 0)
        stores.append(begin(stats.at[h], outs[h]))
    wait_all(stores)


def grads_kernel(bias_ref, *rest):
    z_refs, x_refs = rest[:4], rest[4:8]
    stat_refs = (rest[8:12], rest[12:16])
    own_dq, dq_outs, dkv_outs = rest[16], rest[17:23], rest[23:31]
    bias, qd, kv, bcol, parts, rows, kt, dqt, dkv, dq_send, dkv_send, sems = rest[31:]
    span = qd.shape[2]
    begin = copy_list(sems)
    bias_copy = begin(bias_ref, bias)
    loads = []
    for h in range(2):
        stat_copies = [begin(stat_refs[h][s], parts.at[h, s]) for s in range(SIDE)]
        loads.append(stat_copies + start_loads(begin, h, z_refs, x_refs, range(SIDE), qd, kv))

    def combine(h):
        for r in range(SIDE):
            found = [parts[h, s, (r - s) % SIDE] for s in range(SIDE)]
            top = functools.reduce(jnp.maximum, [p[0:1, :] for p in found])
            factors = [jnp.exp2(p[0:1, :] - top) for p in found]
            total = sum(p[1:2, :] * f for p, f in zip(found, factors))
            mixed = sum(p[2:3, :] * f for p, f in zip(found, factors))
            rows[h, r, 0:1, :] = top + jnp.log2(total)
            rows[h, r, 1:2, :] = mixed / total

    def block(h, qi, ki, diagonal):
        for s in range(span // SUB):
            cols = slice(s * SUB, (s + 1) * SUB)
            q = qd[h, qi, cols, :HEAD]
            do = qd[h, qi, cols, HEAD:]
            seen = (s + 1) * SUB if diagonal else span
            k = kv[h, ki, :seen, :HEAD]
            v = kv[h, ki, :seen, HEAD:]
            x = dot_nt(k, q) * (SCALE * LOG2E) - wide(bcol[h, ki, :seen], SUB)
            x = x - rows[h, qi, 0:1, cols]
            if diagonal:
                x = jnp.where(visible_mask(x.shape, s * SUB), x, NEG_BIG)
            p = jnp.exp2(x)
            ds = (p * (dot_nt(v, do) - rows[h, qi, 1:2, cols])).astype(jnp.bfloat16)
            dkv[h, ki, :seen, HEAD:] += dot_nn(p.astype(jnp.bfloat16), do)
            dkv[h, ki, :seen, :HEAD] += dot_nn(ds, q)
            dqt[h, qi, :, cols] += dot_nn(kt[ki, :, :seen], ds)

    dqt[...] = jnp.zeros_like(dqt)
    dkv[...] = jnp.zeros_like(dkv)
    bias_copy.wait()
    stores = []
    for h in range(2):
        fill_bias(bias, bcol, h)
    for h in range(2):
        wait_all(loads[h])
        combine(h)
        key_outs = dkv_outs[SIDE * h : SIDE * (h + 1)]
        key_sources = [dkv.at[h, 0]] + [dkv_send.at[h, r] for r in range(1, SIDE)]
        key_stores = [
            pltpu.make_async_copy(source, out, sems.at[40 + SIDE * h + r])
            for r, (source, out) in enumerate(zip(key_sources, key_outs))
        ]

        def turn(r, _, h=h):
            kt[r] = kv[h, r, :, :HEAD].astype(jnp.float32).T.astype(jnp.bfloat16)
            return 0

        lax.fori_loop(0, SIDE, turn, 0)

        def one_key_span(ki, _, h=h, key_stores=key_stores):
            def one_query_span(qi, _):
                for_visible(h, qi, ki, block)
                return 0

            lax.fori_loop(0, SIDE, one_query_span, 0)
            scaled = dkv[h, ki, :, :HEAD] * SCALE
            dkv[h, ki, :, :HEAD] = scaled
            dkv_send[h, ki, :, :HEAD] = scaled.astype(jnp.bfloat16)
            dkv_send[h, ki, :, HEAD:] = dkv[h, ki, :, HEAD:].astype(jnp.bfloat16)
            for r in range(SIDE):
                pl.when(ki == r)(key_stores[r].start)
            return 0

        lax.fori_loop(0, SIDE, one_key_span, 0)
        stores += key_stores
        dqt[h, 0] = dqt[h, 0] * SCALE
        stores.append(begin(dqt.at[h, 0], own_dq.at[pl.ds(h * HEAD, HEAD), :]))
        for r in range(1, SIDE):
            dq_send[h, r] = (dqt[h, r] * SCALE).astype(jnp.bfloat16)
            stores.append(begin(dq_send.at[h, r], dq_outs[3 * h + r - 1]))
    wait_all(stores)


def weight_kernel(*rest):
    dq_refs, in_refs, outs = rest[:4], rest[4:12], rest[12:16]
    dqs, inputs, sems = rest[16:]
    here, part = lax.axis_index("sp"), lax.axis_index("tp")
    z, x, y, core = here // SIDE, here % SIDE, part // 2, part % 2
    begin = copy_list(sems)
    copies = []
    for r in range(SIDE):
        of_span = (y - z + r + SIDE) % SIDE
        for other in range(2):
            held_by = core if other == 0 else 1 - core
            copies.append(begin(in_refs[SIDE * other + r], inputs.at[held_by, of_span]))
        copies.append(begin(dq_refs[r], dqs.at[(z + r) % SIDE]))
    wait_all(copies)
    width = outs[0].shape[1]
    for r in (1, 2, 3, 0):
        block = (x + r) % SIDE
        cols = pl.ds(pl.multiple_of((block % 2) * width, width), width)
        total = sum(dot_nn(dqs[a], inputs[block // 2, a, :, cols]) for a in range(SIDE))
        outs[r][...] = total.astype(outs[r].dtype)


def query_kernel(own_ref, *refs):
    parts, (low_ref, grad_ref) = refs[:6], refs[6:]
    for h in range(2):
        cut = slice(h * HEAD, (h + 1) * HEAD)
        total = own_ref[cut, :]
        for ref in parts[3 * h : 3 * (h + 1)]:
            total = total + ref[...].astype(jnp.float32)
        low_ref[cut, :] = total.astype(jnp.bfloat16)
        grad_ref[:, cut] = total.T


def keys_kernel(*refs):
    parts, outs = refs[:8], refs[8:]
    for h in range(2):
        for n, out in enumerate(outs):
            cut = slice(n * HEAD, (n + 1) * HEAD)
            out[:, h * HEAD : (h + 1) * HEAD] = sum(
                ref[:, cut].astype(jnp.float32) for ref in parts[SIDE * h : SIDE * (h + 1)]
            )


ANY = pl.BlockSpec(memory_space=pl.ANY)
VM = pl.BlockSpec(memory_space=pltpu.VMEM)


def stats_call(bias, z_parts, x_parts, known=()):
    span = z_parts[0].shape[0]
    near = not known
    rows = 2 * SIDE * SIDE
    out_shape = [jax.ShapeDtypeStruct((SIDE, 8, span), jnp.float32)] * 2
    scratch = [
        pltpu.VMEM((rows, span), jnp.float32),
        pltpu.VMEM((2, SIDE, span, 2 * HEAD), jnp.bfloat16),
        pltpu.VMEM((2, SIDE, span, 2 * HEAD), jnp.bfloat16),
        pltpu.VMEM((2, SIDE, span, HEAD), jnp.float32),
        pltpu.VMEM((2, SIDE, 8, span), jnp.float32),
        pltpu.SemaphoreType.DMA((24,)),
    ]
    if near:
        slots, pair_count, pair_of = NEAR, 9, near_pairs
        z_parts, x_parts = ([parts[r] for r in NEAR] for parts in (z_parts, x_parts))
        out_shape.append(jax.ShapeDtypeStruct((rows, span), jnp.float32))
        scratch.append(pltpu.VMEM(bias.shape, jnp.float32))
    else:
        slots, pair_count, pair_of = range(SIDE), 7, far_pairs
    pairs = pair_count * span * span
    return pl.pallas_call(
        functools.partial(stats_kernel, slots, pair_count, pair_of, near),
        out_shape=out_shape,
        in_specs=[ANY] * (1 + 2 * len(slots) + len(known)),
        out_specs=[ANY] * len(out_shape),
        scratch_shapes=scratch,
        compiler_params=pltpu.CompilerParams(vmem_limit_bytes=62 << 20),
        cost_estimate=pl.CostEstimate(
            flops=4 * HEAD * pairs, bytes_accessed=4 << 20, transcendentals=pairs
        ),
        name="stats",
    )(bias, *z_parts, *x_parts, *known)


def grads_call(bias, z_parts, x_parts, z_stats, x_stats):
    span = z_parts[0].shape[0]
    pairs = 17 * span * span

    own_dq = jax.ShapeDtypeStruct((2 * HEAD, span), jnp.float32)
    send_dq = jax.ShapeDtypeStruct((HEAD, span), jnp.bfloat16)
    own_dkv = jax.ShapeDtypeStruct((span, 2 * HEAD), jnp.float32)
    send_dkv = jax.ShapeDtypeStruct((span, 2 * HEAD), jnp.bfloat16)
    outs = pl.pallas_call(
        grads_kernel,
        out_shape=[own_dq] + [send_dq] * 6 + ([own_dkv] + [send_dkv] * 3) * 2,
        in_specs=[ANY] * 17,
        out_specs=[ANY] * 15,
        scratch_shapes=[
            pltpu.VMEM(bias.shape, jnp.float32),
            pltpu.VMEM((2, SIDE, span, 2 * HEAD), jnp.bfloat16),
            pltpu.VMEM((2, SIDE, span, 2 * HEAD), jnp.bfloat16),
            pltpu.VMEM((2, SIDE, span, HEAD), jnp.float32),
            pltpu.VMEM((2, SIDE, SIDE, 8, span), jnp.float32),
            pltpu.VMEM((2, SIDE, 8, span), jnp.float32),
            pltpu.VMEM((SIDE, HEAD, span), jnp.bfloat16),
            pltpu.VMEM((2, SIDE, HEAD, span), jnp.float32),
            pltpu.VMEM((2, SIDE, span, 2 * HEAD), jnp.float32),
            pltpu.VMEM((2, SIDE, HEAD, span), jnp.bfloat16),
            pltpu.VMEM((2, SIDE, span, 2 * HEAD), jnp.bfloat16),
            pltpu.SemaphoreType.DMA((48,)),
        ],
        compiler_params=pltpu.CompilerParams(vmem_limit_bytes=62 << 20),
        cost_estimate=pl.CostEstimate(
            flops=10 * HEAD * pairs, bytes_accessed=8 << 20, transcendentals=pairs
        ),
        name="grads",
    )(bias, *z_parts, *x_parts, *z_stats, *x_stats)
    return outs[0], outs[1:4], outs[4:7], outs[7:11], outs[11:]


def weight_call(query_grads, inputs):
    cols, rows = query_grads[0].shape
    width = inputs[0].shape[1]
    own = jax.ShapeDtypeStruct((cols, width // 2), jnp.float32)
    send = jax.ShapeDtypeStruct((cols, width // 2), jnp.bfloat16)
    return pl.pallas_call(
        weight_kernel,
        out_shape=[own] + [send] * 3,
        in_specs=[ANY] * 12,
        out_specs=[VM] * 4,
        scratch_shapes=[
            pltpu.VMEM((SIDE, cols, rows), jnp.bfloat16),
            pltpu.VMEM((2, SIDE, rows, width), jnp.bfloat16),
            pltpu.SemaphoreType.DMA((12,)),
        ],
        compiler_params=pltpu.CompilerParams(vmem_limit_bytes=16 << 20),
        cost_estimate=pl.CostEstimate(
            flops=16 * rows * width * cols, bytes_accessed=6 << 20, transcendentals=0
        ),
        name="weight",
    )(*query_grads, *inputs)


def query_call(own, parts_0, parts_1):
    rows, span = own.shape
    return pl.pallas_call(
        query_kernel,
        out_shape=[
            jax.ShapeDtypeStruct((rows, span), jnp.bfloat16),
            jax.ShapeDtypeStruct((span, rows), jnp.float32),
        ],
        in_specs=[VM] * 7,
        out_specs=[VM] * 2,
        compiler_params=pltpu.CompilerParams(vmem_limit_bytes=16 << 20),
        cost_estimate=pl.CostEstimate(flops=10**6, bytes_accessed=2 << 20, transcendentals=0),
        name="query_sums",
    )(own, *parts_0, *parts_1)


def keys_call(parts_0, parts_1):
    span, cols = parts_0[0].shape
    block = pl.BlockSpec((span // SIDE, cols), lambda n: (n, 0))
    return pl.pallas_call(
        keys_kernel,
        grid=(SIDE,),
        out_shape=[jax.ShapeDtypeStruct((span, cols), jnp.float32)] * 2,
        in_specs=[block] * 8,
        out_specs=[block] * 2,
        compiler_params=pltpu.CompilerParams(vmem_limit_bytes=16 << 20),
        cost_estimate=pl.CostEstimate(flops=10**6, bytes_accessed=4 << 20, transcendentals=0),
        name="key_sums",
    )(*parts_0, *parts_1)


def head_of(array, h):
    return array[:, h * HEAD : (h + 1) * HEAD]


def local(queries, keys, values, forget_logits, layer_input, out_grad):
    gates = jnp.broadcast_to(forget_logits.T, (SIDE * SIDE,) + forget_logits.shape[::-1])
    gates = lax.all_to_all(gates, "sp", 0, 0, tiled=True)

    for_z = jnp.concatenate(
        [head_of(queries, 0), head_of(out_grad, 0), head_of(keys, 1), head_of(values, 1)], axis=1
    )
    for_x = jnp.concatenate(
        [head_of(keys, 0), head_of(values, 0), head_of(queries, 1), head_of(out_grad, 1)], axis=1
    )
    z_parts = fetched(for_z, along_z)
    x_parts = fetched(for_x, along_x)

    def over_zy(target):
        pairs = []
        for n in range(SIDE**3 * 2):
            zxyc = (n // 32, n // 8 % SIDE, n // 2 % SIDE, n % 2)
            new_z, new_y = target(zxyc[0], zxyc[2])
            pairs.append((n, new_z % SIDE * 32 + zxyc[1] * 8 + new_y % SIDE * 2 + zxyc[3]))
        return pairs

    everywhere = ("sp", "tp")
    moved = lax.ppermute(layer_input, everywhere, over_zy(lambda a, b: (a, a + b)))
    moved = lax.ppermute(moved, everywhere, over_zy(lambda a, b: (b - a, b)))
    inputs = fetched(moved, lambda r: [(p, (p + 2 * r) % 8) for p in range(8)], "tp")
    for part in list(inputs):
        inputs.append(lax.ppermute(part, "tp", [(p, p ^ 1) for p in range(8)]))

    *known, bias = stats_call(gates, z_parts, x_parts)
    stats_z, stats_x = stats_call(bias, z_parts, x_parts, known)
    z_stats = fetched_direct(stats_z, along_z)
    x_stats = fetched_direct(stats_x, along_x)
    own_dq, dq_0, dq_1, dkv_0, dkv_1 = grads_call(bias, z_parts, x_parts, z_stats, x_stats)

    def sent(parts, axis_perm):
        return [lax.ppermute(part, "sp", axis_perm(r + 1)) for r, part in enumerate(parts)]

    def arrived(parts, axis_perm):
        return [parts[0]] + sent(parts[1:], axis_perm)

    dq_0, dq_1 = sent(dq_0, along_z), sent(dq_1, along_x)
    low, query_grad = query_call(own_dq, dq_0, dq_1)
    low, dkv_0, dkv_1 = lax.optimization_barrier((low, dkv_0, dkv_1))
    low_parts = fetched_direct(low, along_z)
    terms = weight_call(low_parts, inputs)
    terms = arrived(terms, along_x)
    weight_grad = sum(part.astype(jnp.float32) for part in terms).T
    dkv_0 = arrived(dkv_0, along_x)
    dkv_1 = arrived(dkv_1, along_z)
    key_grad, value_grad = keys_call(dkv_0, dkv_1)
    return (query_grad, key_grad, value_grad, weight_grad)


def solution(mesh):
    placed = P("sp", "tp")

    return jax.shard_map(
        local,
        mesh=mesh,
        in_specs=(placed,) * 6,
        out_specs=(placed,) * 4,
        check_vma=False,
    )
```
